32 devices in a mesh: sp: 8 (over z, y), tp: 4 (over x, core).
Axes of the slice: x: 2, y: 2, z: 4, core: 2. Of those that a mesh axis runs over, the one named last changes fastest.
Arguments:
- queries: bfloat16 [8192, 1024], P('sp', 'tp'), may hold values from -6 to 6
- cell_key_rows: bfloat16 [8192, 1024], P('sp', 'tp'), may hold values from -6 to 6
- cell_value_rows: bfloat16 [8192, 2048], P('sp', 'tp'), may hold values from -6 to 6
- output_gate_logits: bfloat16 [8192, 2048], P('sp', 'tp'), may hold values from -6 to 6
- input_gate_logits: bfloat16 [8, 8192], P('tp', 'sp'), may hold values from -4 to 216
- forget_gate_logits: bfloat16 [8, 8192], P('tp', 'sp'), may hold values from 0.5 to 14
- forget_extra_term: float32 [8, 8192], P('tp', 'sp'), may hold values from -1.4 to 0
- residual: bfloat16 [8192, 2048], P('sp', 'tp'), may hold values from -13 to 13
- head_norm_gain: bfloat16 [2048], P('tp'), may hold values from 0.099609375 to 1.8984375
- cell_output_weight: bfloat16 [2048, 2048], P('tp'), may hold values from -0.25 to 0.25
- feedforward_norm_gain: bfloat16 [2048], replicated, may hold values from 0.099609375 to 1.8984375
- gate_projection_weight: bfloat16 [2048, 5632], P('sp', 'tp'), may hold values from -0.125 to 0.125
- up_projection_weight: bfloat16 [2048, 5632], P('sp', 'tp'), may hold values from -0.125 to 0.125
- down_projection_weight: bfloat16 [5632, 2048], P('tp', 'sp'), may hold values from -0.15625 to 0.15625
Outputs:
- mixed: bfloat16 [8192, 2048], P('sp', 'tp')
The draws below stay inside these ranges and needn't reach their ends.
All inputs are finite; a program needn't handle non-finite values.
Results may differ from the reference program's by a relative error of at most 0.017.
Values may be sent and summed in bfloat16 or wider, within the bound.
A program may use at most 128 MiB of HBM per device.

```python
import jax
import jax.numpy as jnp
from jax import lax

D = 2048
HEADS = 8
DK = 128
DV = 256
FF = 5632
TOK_DEV = 1024
TOKENS = 8192
N_TP = 4


def draw_input_gate_logits(key, part):
    base_key = jax.random.fold_in(key, 11)
    values = jnp.clip(jax.random.normal(base_key, (HEADS, TOKENS), jnp.float32), -4.0, 4.0)
    return values.astype(jnp.bfloat16)


def draw_forget_gate_logits(key, part):
    order = jax.random.permutation(jax.random.fold_in(key, 21), HEADS)
    noise_key = jax.random.fold_in(key, 22)
    slow_count = HEADS // 2
    jitter = 0.6 * jnp.clip(jax.random.normal(noise_key, (HEADS, TOKENS), jnp.float32), -4.0, 4.0)
    slow_heads = order < slow_count
    quick = jnp.log(jax.random.uniform(jax.random.fold_in(key, 23), (HEADS,), jnp.float32, 30.0, 60.0))
    level = jnp.where(slow_heads, jnp.log(TOKENS / 0.8), quick)
    block_shift = jax.random.uniform(jax.random.fold_in(key, 24), (HEADS, TOKENS // TOK_DEV), jnp.float32, -0.4, 0.4)
    shifts = jnp.repeat(block_shift, TOK_DEV, axis=1)
    return (level[:, None] + shifts + jitter).astype(jnp.bfloat16)


def draw_forget_extra_term(key, part):
    spots = jax.random.randint(jax.random.fold_in(key, 31), (HEADS, 2, 1), 0, TOKENS)
    fraction = jax.random.uniform(jax.random.fold_in(key, 32), (HEADS, 2, 1), jnp.float32, 0.2, 0.5)
    depth = jnp.log(1.0 - fraction)
    places = jnp.arange(TOKENS)[None, None, :]
    return jnp.sum(jnp.where(places == spots, depth, 0.0), axis=1).astype(jnp.float32)


def draw_residual(key, part):
    column_scale = 0.4 * 6.0 ** (jnp.arange(D, dtype=jnp.float32) / D)
    values = jnp.clip(jax.random.normal(jax.random.fold_in(key, 41), (TOKENS, D), jnp.float32), -4.0, 4.0)
    return (values * column_scale[None, :]).astype(jnp.bfloat16)


def block_levels(rng, dims, shards, low, largest):
    factor_of, own = 1.0, jax.random.fold_in(rng, 6)
    for position, parts in shards:
        steps = jnp.exp(jax.random.uniform(jax.random.fold_in(own, position), (parts,), jnp.float32, low / len(shards), largest / len(shards)))
        factor_of = factor_of * jnp.repeat(steps, dims[position] // parts).reshape([-1 if axis == position else 1 for axis in range(len(dims))])
    return factor_of


def normal_values(rng, shape, spread, most, split=(), held_as=jnp.bfloat16):
    loudness = block_levels(rng, shape, split, -0.22, 0.18) if split else 1.0
    result = jax.random.normal(rng, shape, jnp.float32) * spread * loudness
    return jnp.minimum(jnp.maximum(result, -most), most).astype(held_as)


def setup_inputs(seed: int = 0) -> dict:
    arg_keys = jax.random.split(jax.random.key(seed), 15)
    return {
        "queries": normal_values(arg_keys[0], (TOKENS, HEADS * DK), 1.0, 6.0, ((0, 8), (1, 4))),
        "cell_key_rows": normal_values(arg_keys[1], (TOKENS, HEADS * DK), 1.0, 6.0, ((0, 8), (1, 4))),
        "cell_value_rows": normal_values(arg_keys[2], (TOKENS, HEADS * DV), 1.0, 6.0, ((0, 8), (1, 4))),
        "output_gate_logits": normal_values(arg_keys[3], (TOKENS, HEADS * DV), 1.0, 6.0, ((0, 8), (1, 4))),
        "input_gate_logits": draw_input_gate_logits(jax.random.fold_in(arg_keys[14], 71), 0),
        "forget_gate_logits": draw_forget_gate_logits(jax.random.fold_in(arg_keys[14], 71), 0),
        "forget_extra_term": draw_forget_extra_term(jax.random.fold_in(arg_keys[14], 71), 0),
        "residual": draw_residual(jax.random.fold_in(arg_keys[14], 71), 0),
        "head_norm_gain": jnp.clip(1.0 + 0.18 * jax.random.normal(arg_keys[8], (HEADS * DV,), jnp.float32), 0.099609375, 1.8984375).astype(jnp.bfloat16),
        "cell_output_weight": normal_values(arg_keys[9], (HEADS * DV, D), (HEADS * DV // 4) ** -0.5, 0.25, ((0, 4),)),
        "feedforward_norm_gain": jnp.clip(1.0 + 0.18 * jax.random.normal(arg_keys[10], (D,), jnp.float32), 0.099609375, 1.8984375).astype(jnp.bfloat16),
        "gate_projection_weight": normal_values(arg_keys[11], (D, FF), D ** -0.5, 0.125, ((0, 8), (1, 4))),
        "up_projection_weight": normal_values(arg_keys[12], (D, FF), D ** -0.5, 0.125, ((0, 8), (1, 4))),
        "down_projection_weight": normal_values(arg_keys[13], (FF, D), (FF // 4) ** -0.5, 0.15625, ((0, 4), (1, 8))),
    }


PRECISE = lax.Precision.HIGHEST
LOWEST_LOG = -1e+30
EPSILON = 1e-06

def to_blocks(array, block_count, block_size):
    shaped = array.reshape((array.shape[0], block_count, block_size) + array.shape[2:])
    return jnp.moveaxis(shaped, 1, 0)

def from_blocks(array):
    moved = jnp.moveaxis(array, 0, 1)
    return moved.reshape((moved.shape[0], moved.shape[1] * moved.shape[2]) + moved.shape[3:])

def memory_blocks(query_heads, key_heads, value_heads, in_gates, forget_log_value, block_size):
    head_count, length, key_width = query_heads.shape
    value_width = value_heads.shape[2]
    block_count = length // block_size
    causal = jnp.tril(jnp.ones((block_size, block_size), bool))

    def advance(carried, pieces):
        memory_state, top_log, offset = carried
        query_block, key_block, value_block, gate_block, forget_block = pieces
        running = jnp.cumsum(forget_block, axis=-1)
        log_weight = jnp.where(causal, running[:, :, None] - running[:, None, :] + gate_block[:, None, :], -jnp.inf)
        log_start = running + top_log[:, None]
        row_max = jnp.maximum(lax.optimization_barrier(jnp.max(log_weight, axis=-1)), log_start)
        scores = jnp.einsum('htd,hsd->hts', query_block, key_block, precision=PRECISE)
        scores = scores * jnp.exp(log_weight - row_max[:, :, None])
        earlier = jnp.einsum('htd,hde->hte', query_block, memory_state, precision=PRECISE)
        numerator = jnp.exp(log_start - row_max)[:, :, None] * earlier
        numerator = numerator + jnp.einsum('hts,hse->hte', scores, value_block, precision=PRECISE)
        last_cum = running[:, -1]
        log_end = last_cum[:, None] - running + gate_block
        new_top = jnp.maximum(last_cum + top_log, lax.optimization_barrier(jnp.max(log_end, axis=-1)))
        scaled = key_block * jnp.exp(log_end - new_top[:, None])[:, :, None]
        memory_state = jnp.exp(last_cum + top_log - new_top)[:, None, None] * memory_state
        memory_state = memory_state + jnp.einsum('hsd,hse->hde', scaled, value_block, precision=PRECISE)
        return ((memory_state, new_top, offset + last_cum), (numerator, row_max, offset[:, None] + running))
    initial = (jnp.zeros((head_count, key_width, value_width), jnp.float32), jnp.full((head_count,), LOWEST_LOG, jnp.float32), jnp.zeros((head_count,), jnp.float32))
    pieces = tuple((to_blocks(array, block_count, block_size) for array in (query_heads, key_heads, value_heads, in_gates, forget_log_value)))
    ending, outputs = lax.scan(advance, initial, pieces)
    return (tuple((from_blocks(output) for output in outputs)), ending)

def reference(queries, cell_key_rows, cell_value_rows, output_gate_logits, input_gate_logits, forget_gate_logits, forget_extra_term, residual, head_norm_gain, cell_output_weight, feedforward_norm_gain, gate_projection_weight, up_projection_weight, down_projection_weight):
    length = queries.shape[0]

    def heads_first(array, width):
        return jnp.transpose(array.reshape(length, HEADS, width), (1, 0, 2)).astype(jnp.float32)
    query_heads = heads_first(queries, DK) * DK ** (-0.5)
    key_heads = heads_first(cell_key_rows, DK)
    value_heads = heads_first(cell_value_rows, DV)
    forget_log_value = jax.nn.log_sigmoid(forget_gate_logits.astype(jnp.float32)) + forget_extra_term
    results, _ = memory_blocks(query_heads, key_heads, value_heads, input_gate_logits.astype(jnp.float32), forget_log_value, min(length, 256))
    memory = jnp.transpose(results[0], (1, 0, 2))
    normal = memory * lax.rsqrt(lax.optimization_barrier(jnp.mean(memory * memory, axis=-1, keepdims=True)) + EPSILON)
    gate_open = jax.nn.sigmoid(output_gate_logits.astype(jnp.float32).reshape(length, HEADS, DV))
    gated_heads = normal * head_norm_gain.astype(jnp.float32).reshape(HEADS, DV) * gate_open
    gated_heads = gated_heads.reshape(length, HEADS * DV).astype(jnp.bfloat16)
    head_width = HEADS * DV // N_TP
    stream_sum = residual.astype(jnp.float32)
    for head_part in range(N_TP):
        head_lower = head_part * head_width
        head_term = jnp.dot(gated_heads[:, head_lower:head_lower + head_width], cell_output_weight[head_lower:head_lower + head_width], preferred_element_type=jnp.float32)
        head_rounded = lax.optimization_barrier(head_term.astype(jnp.bfloat16))
        stream_sum = stream_sum + head_rounded.astype(jnp.float32)
    stream = stream_sum.astype(jnp.bfloat16)
    stream_wide = stream.astype(jnp.float32)
    scale = lax.rsqrt(lax.optimization_barrier(jnp.mean(stream_wide * stream_wide, axis=-1, keepdims=True)) + EPSILON)
    normed = (stream_wide * scale * feedforward_norm_gain.astype(jnp.float32)).astype(jnp.bfloat16)
    gate_value = jnp.dot(normed, gate_projection_weight, preferred_element_type=jnp.float32)
    lifted = jnp.dot(normed, up_projection_weight, preferred_element_type=jnp.float32)
    hidden = (jax.nn.silu(gate_value) * lifted).astype(jnp.bfloat16)
    part_width = FF // N_TP
    summed = jnp.zeros(stream_wide.shape, jnp.float32)
    for part_index in range(N_TP):
        lower = part_index * part_width
        partial_value = jnp.dot(hidden[:, lower:lower + part_width], down_projection_weight[lower:lower + part_width], preferred_element_type=jnp.float32)
        rounded = lax.optimization_barrier(partial_value.astype(jnp.bfloat16))
        summed = summed + rounded.astype(jnp.float32)
    return (stream_wide + 0.5 * summed).astype(jnp.bfloat16)
```

```python
import functools

import jax
import jax.numpy as jnp
from jax import lax
from jax.experimental import pallas as pl
from jax.experimental.pallas import tpu as pltpu
from jax.sharding import PartitionSpec as P

LOWEST_LOG = -1e30
EPSILON = 1e-06


def shift_pairs(length, step):
    return [(source, source + step) for source in range(length - step)]


def entering_state(state, top, total):
    length, index = lax.axis_size("sp"), lax.axis_index("sp")
    heads, key_width, value_width = state.shape

    def pack(s, t, f):
        tail = jnp.zeros((heads, 8, value_width), jnp.float32)
        tail = tail.at[:, 0, :].set(t[:, None]).at[:, 1, :].set(f[:, None])
        return jnp.concatenate([s, tail], axis=1)

    def unpack(p, valid):
        s = p[:, :key_width, :]
        t = jnp.where(valid, p[:, key_width, 0], LOWEST_LOG)
        f = jnp.where(valid, p[:, key_width + 1, 0], 0.0)
        return jnp.where(valid, s, 0.0), t, f

    moved = lax.ppermute(pack(state, top, total), "sp", shift_pairs(length, 1))
    s, t, f = unpack(moved, index >= 1)
    step = 1
    while step < length - 1:
        moved = lax.ppermute(pack(s, t, f), "sp", shift_pairs(length, step))
        s0, t0, f0 = unpack(moved, index >= step)
        from_top = t0 + f
        new_top = jnp.maximum(from_top, t)
        s = (
            jnp.exp(from_top - new_top)[:, None, None] * s0
            + jnp.exp(t - new_top)[:, None, None] * s
        )
        t, f = new_top, f0 + f
        step *= 2
    return s, t


def cell_kernel(q_ref, k_ref, v_ref, a_ref, m_ref, c_ref, state_ref, open_ref, gain_ref, o_ref, *, scale):
    block = q_ref.shape[0]
    length = k_ref.shape[0]
    q = q_ref[...]
    first = pl.program_id(1) * block
    scores = lax.dot_general(
        q, k_ref[...], (((1,), (1,)), ((), ())), preferred_element_type=jnp.float32
    )
    rows = first + lax.broadcasted_iota(jnp.int32, (block, length), 0)
    cols = lax.broadcasted_iota(jnp.int32, (block, length), 1)
    weight = jnp.where(cols <= rows, jnp.exp(jnp.minimum(a_ref[0] - m_ref[0], 0.0)), 0.0)
    numer = jnp.dot(
        (scores * weight).astype(jnp.bfloat16), v_ref[...], preferred_element_type=jnp.float32
    )
    before = jnp.dot(q, state_ref[0].astype(jnp.bfloat16), preferred_element_type=jnp.float32)
    memory = (numer + c_ref[0] * before) * scale
    normal = memory * lax.rsqrt(jnp.mean(memory * memory, axis=-1, keepdims=True) + EPSILON)
    gate_open = jax.nn.sigmoid(open_ref[...].astype(jnp.float32))
    o_ref[...] = (normal * gain_ref[...].astype(jnp.float32) * gate_open).astype(o_ref.dtype)


def cell(queries, keys, values, a_log, m_col, c_col, state, open_logits, gain):
    heads, length = a_log.shape
    dk, dv = queries.shape[1] // heads, values.shape[1] // heads
    block = min(length, 256)
    return pl.pallas_call(
        lambda *refs: cell_kernel(*refs, scale=dk ** (-0.5)),
        grid=(heads, length // block),
        in_specs=[
            pl.BlockSpec((block, dk), lambda h, i: (i, h)),
            pl.BlockSpec((length, dk), lambda h, i: (0, h)),
            pl.BlockSpec((length, dv), lambda h, i: (0, h)),
            pl.BlockSpec((1, 1, length), lambda h, i: (h, 0, 0)),
            pl.BlockSpec((1, block, 1), lambda h, i: (h, i, 0)),
            pl.BlockSpec((1, block, 1), lambda h, i: (h, i, 0)),
            pl.BlockSpec((1, dk, dv), lambda h, i: (h, 0, 0)),
            pl.BlockSpec((block, dv), lambda h, i: (i, h)),
            pl.BlockSpec((1, dv), lambda h, i: (0, h)),
        ],
        out_specs=pl.BlockSpec((block, dv), lambda h, i: (i, h)),
        out_shape=jax.ShapeDtypeStruct((length, heads * dv), jnp.bfloat16),
        cost_estimate=pl.CostEstimate(
            flops=8 * heads * length * length * dv, bytes_accessed=6 * length * heads * dv, transcendentals=0
        ),
        name="cell",
    )(queries, keys, values, a_log[:, None, :], m_col[:, :, None], c_col[:, :, None], state, open_logits, gain)


def partner_pairs(count):
    return [(i, i ^ 1) for i in range(count)]


def ring_pairs(count, step):
    return [(i, (i + 2 * step) % count) for i in range(count)]


def product_scattered(rows, weight):
    count, index = lax.axis_size("tp"), lax.axis_index("tp")
    chips, core, chip = count // 2, index % 2, index // 2
    width = weight.shape[1] // count

    def product(block):
        columns = lax.dynamic_slice_in_dim(weight, block * width, width, 1)
        return jnp.dot(rows, columns, preferred_element_type=jnp.float32)

    def chip_sum(to):
        given = product(2 * to + 1 - core).astype(jnp.bfloat16)
        got = lax.ppermute(given, "tp", partner_pairs(count))
        return product(2 * to + core) + got.astype(jnp.float32)

    moved = []
    for step in range(1, chips):
        sent = chip_sum((chip + step) % chips).astype(jnp.bfloat16)
        moved.append(lax.ppermute(sent, "tp", ring_pairs(count, step)))
    total = chip_sum(chip)
    for part in moved:
        total = total + part.astype(jnp.float32)
    return total


def columns_gathered(block):
    count, index = lax.axis_size("tp"), lax.axis_index("tp")
    chips, core, chip = count // 2, index % 2, index // 2
    width = block.shape[1]
    whole = jnp.zeros((block.shape[0], count * width), block.dtype)
    held = [(chip, block)]
    for step in range(1, chips):
        moved = lax.ppermute(block, "tp", ring_pairs(count, step))
        held.append(((chip - step) % chips, moved))
    for place, piece in held:
        other = lax.ppermute(piece, "tp", partner_pairs(count))
        whole = lax.dynamic_update_slice(whole, piece, (0, (2 * place + core) * width))
        whole = lax.dynamic_update_slice(whole, other, (0, (2 * place + 1 - core) * width))
    return whole


def general(
    queries,
    cell_key_rows,
    cell_value_rows,
    output_gate_logits,
    input_gate_logits,
    forget_gate_logits,
    forget_extra_term,
    residual,
    head_norm_gain,
    cell_output_weight,
    feedforward_norm_gain,
    gate_projection_weight,
    up_projection_weight,
    down_projection_weight,
):
    whole_gate = lax.all_gather(gate_projection_weight, "sp", axis=0, tiled=True)
    whole_up = lax.all_gather(up_projection_weight, "sp", axis=0, tiled=True)
    length = queries.shape[0]
    heads = input_gate_logits.shape[0]
    dk, dv = queries.shape[1] // heads, cell_value_rows.shape[1] // heads
    log_forget = jax.nn.log_sigmoid(forget_gate_logits.astype(jnp.float32)) + forget_extra_term
    running = jnp.cumsum(log_forget, axis=-1)
    a_log = input_gate_logits.astype(jnp.float32) - running
    m_log = lax.cummax(a_log, axis=1)
    a_top, total = m_log[:, -1], running[:, -1]
    decay = jnp.exp(a_log - a_top[:, None])
    weighed = (
        cell_key_rows.reshape(length, heads, dk).astype(jnp.float32) * decay.T[:, :, None]
    ).astype(jnp.bfloat16)
    state = jnp.stack(
        [
            lax.dot_general(
                weighed[:, h],
                cell_value_rows[:, h * dv : (h + 1) * dv],
                (((0,), (0,)), ((), ())),
                preferred_element_type=jnp.float32,
            )
            for h in range(heads)
        ]
    )
    carried, carried_top = entering_state(state, a_top + total, total)
    m_all = jnp.maximum(m_log, carried_top[:, None])
    coefficient = jnp.exp(carried_top[:, None] - m_all)
    gated = cell(
        queries,
        cell_key_rows,
        cell_value_rows,
        a_log,
        m_all,
        coefficient,
        carried,
        output_gate_logits,
        head_norm_gain[None, :],
    )
    summed = product_scattered(gated, cell_output_weight)
    stream = (residual.astype(jnp.float32) + summed).astype(jnp.bfloat16)
    down_late, stream = lax.optimization_barrier((down_projection_weight, stream))
    whole_down = lax.all_gather(down_late, "sp", axis=1, tiled=True)
    wide = columns_gathered(stream).astype(jnp.float32)
    scale = lax.rsqrt(jnp.mean(wide * wide, axis=-1, keepdims=True) + EPSILON)
    normed = (wide * scale * feedforward_norm_gain.astype(jnp.float32)[None, :]).astype(jnp.bfloat16)
    gate_value = jnp.dot(normed, whole_gate, preferred_element_type=jnp.float32)
    lifted = jnp.dot(normed, whole_up, preferred_element_type=jnp.float32)
    hidden = (jax.nn.silu(gate_value) * lifted).astype(jnp.bfloat16)
    channel_total = product_scattered(hidden, whole_down)
    return (stream.astype(jnp.float32) + 0.5 * channel_total).astype(jnp.bfloat16)


NX, NY = 2, 2
BY_NAME = pl.DeviceIdType.MESH


def block_body(
    planes,
    q_ref,
    k_ref,
    v_ref,
    open_ref,
    a_ref,
    cols_ref,
    meta_ref,
    resid_ref,
    gain_ref,
    wo_ref,
    fgain_ref,
    gate_ref,
    up_ref,
    down_ref,
    out_ref,
    gu,
    dn,
    rows_all,
    hid,
    gu_out,
    num,
    ent,
    st_own,
    st_y,
    st_sum,
    st_z,
    meta_y,
    meta_sum,
    meta_z,
    lw_ref,
    pool,
    core_in,
    x_in,
    normed,
    core_back,
    y_back,
    x_back,
    zs,
    zr,
    ysem,
    ssem,
    fsem,
    gsem,
    bsem,
    lsem,
):
    sp, tp = lax.axis_index("sp"), lax.axis_index("tp")
    z, y, x, c = sp // NY, sp % NY, tp // 2, tp % 2
    tokens, heads = q_ref.shape[0], a_ref.shape[0]
    dk, dv = q_ref.shape[1] // heads, v_ref.shape[1] // heads
    width = resid_ref.shape[1]
    depth, hidden = gate_ref.shape
    half = hidden // NY
    count = 2 * NX
    last = planes - 1
    strip = tokens // 4
    wide = width // 2
    part_rows = depth // 2

    partner = {"tp": tp + 1 - 2 * c}
    x_next = {"tp": (1 - x) * 2 + c}
    y_next = {"sp": z * NY + 1 - y}

    def on_plane(at):
        return {"sp": at * NY + y}

    def remote(src, dst, sems, to):
        return pltpu.make_async_remote_copy(
            src_ref=src, dst_ref=dst, send_sem=sems[0], recv_sem=sems[1], device_id=to, device_id_type=BY_NAME
        )

    barrier = pltpu.get_barrier_semaphore()
    for to in (partner, x_next, y_next):
        pl.semaphore_signal(barrier, inc=1, device_id=to, device_id_type=BY_NAME)
    for step in range(1, planes):
        pl.semaphore_signal(
            barrier, inc=1, device_id=on_plane((z + step) % planes), device_id_type=BY_NAME
        )
    pl.semaphore_wait(barrier, planes + 2)

    for mine in range(NY):

        @pl.when(y == mine)
        def _():
            own = pl.ds(pl.multiple_of(sp * depth, depth), depth)
            here, there = mine * half, (1 - mine) * half
            gu_out[:, 0:half] = gate_ref[:, there : there + half]
            gu_out[:, half : 2 * half] = up_ref[:, there : there + half]
            gu[own, 0:half] = gate_ref[:, here : here + half]
            gu[own, half : 2 * half] = up_ref[:, here : here + half]

    def gu_rows(at, chunk):
        side = (y + chunk // 2) % 2
        start = (at * NY + side) * depth + (chunk % 2) * part_rows
        return pl.ds(pl.multiple_of(start, part_rows), part_rows)

    def z_copy(way, dist, chunk):
        at = z - dist if way == 0 else z + dist
        to = z + 1 if way == 0 else z - 1
        sems = (zs.at[way, dist, chunk], zr.at[way, dist + 1, chunk])
        if chunk < 4:
            part = gu.at[gu_rows(at, chunk), :]
        else:
            part = dn.at[at * NY + chunk - 4]
        return remote(part, part, sems, on_plane(to))

    def z_arrival(way, dist, chunk):
        at = z - dist if way == 0 else z + dist
        sems = (zs.at[way, dist, chunk], zr.at[way, dist, chunk])
        if chunk < 4:
            part = gu.at[gu_rows(at, chunk), :]
        else:
            part = dn.at[at * NY + chunk - 4]
        return remote(part, part, sems, on_plane(z))

    def has_next(way):
        return z < last if way == 0 else z > 0

    def has_origin(way, dist):
        return z >= dist if way == 0 else z + dist <= last

    def z_send(chunk):
        for way in range(2):

            @pl.when(has_next(way))
            def _():
                z_copy(way, 0, chunk).start()

    def z_forward(dist, chunk):
        for way in range(2):

            @pl.when(jnp.logical_and(has_origin(way, dist), has_next(way)))
            def _():
                z_arrival(way, dist, chunk).wait_recv()
                z_copy(way, dist, chunk).start()

    def y_rows(owner, chunk):
        start = (z * NY + owner) * depth + chunk * part_rows
        return pl.ds(pl.multiple_of(start, part_rows), part_rows)

    def y_weight(chunk):
        sems = (ysem.at[0, chunk], ysem.at[1, chunk])
        if chunk < 2:
            return remote(
                gu_out.at[pl.ds(chunk * part_rows, part_rows), :], gu.at[y_rows(y, chunk), :], sems, y_next
            )
        start = pl.multiple_of((1 - y) * half, half)
        return remote(down_ref.at[pl.ds(start, half), :], dn.at[sp], sems, y_next)

    own_down = pltpu.make_async_copy(
        down_ref.at[pl.ds(pl.multiple_of(y * half, half), half), :], dn.at[sp], lsem.at[0]
    )
    own_down.start()
    y_weight(0).start()
    z_send(0)

    for h in range(heads):
        weighed = (
            k_ref[:, h * dk : (h + 1) * dk].astype(jnp.float32) * cols_ref[:, h : h + 1]
        ).astype(jnp.bfloat16)
        st_own[h] = lax.dot_general(
            weighed,
            v_ref[:, h * dv : (h + 1) * dv],
            (((0,), (0,)), ((), ())),
            preferred_element_type=jnp.float32,
        ).astype(jnp.bfloat16)

    state_y = [
        remote(st_own, st_y, (ssem.at[0, 0], ssem.at[0, 1]), y_next),
        remote(meta_ref, meta_y, (ssem.at[1, 0], ssem.at[1, 1]), y_next),
    ]
    for copy in state_y:
        copy.start()
    y_weight(1).start()
    y_weight(2).start()
    z_send(1)

    def attend(h, i):
        span = (i + 1) * strip
        at = pl.ds(i * strip, strip)
        scores = lax.dot_general(
            q_ref[at, h * dk : (h + 1) * dk],
            k_ref[0:span, h * dk : (h + 1) * dk],
            (((1,), (1,)), ((), ())),
            preferred_element_type=jnp.float32,
        )
        log_weight = a_ref[h : h + 1, 0:span] - cols_ref[at, heads + h : heads + h + 1]
        row = i * strip + lax.broadcasted_iota(jnp.int32, (strip, span), 0)
        col = lax.broadcasted_iota(jnp.int32, (strip, span), 1)
        weight = jnp.where(col <= row, jnp.exp(jnp.minimum(log_weight, 0.0)), 0.0)
        num[at, h * dv : (h + 1) * dv] = jnp.dot(
            (scores * weight).astype(jnp.bfloat16),
            v_ref[0:span, h * dv : (h + 1) * dv],
            preferred_element_type=jnp.float32,
        )

    for h in range(heads):
        attend(h, 0)

    for copy in state_y:
        copy.wait_recv()
    first = y == 0
    meta_own, meta_other = meta_ref[...], meta_y[...]
    meta_0 = jnp.where(first, meta_own, meta_other)
    meta_1 = jnp.where(first, meta_other, meta_own)
    top_0 = meta_0[0:heads] + meta_1[heads : 2 * heads]
    top_1 = meta_1[0:heads]
    top = jnp.maximum(top_0, top_1)
    scale_0, scale_1 = jnp.exp(top_0 - top), jnp.exp(top_1 - top)
    scale_own = jnp.where(first, scale_0, scale_1)
    scale_other = jnp.where(first, scale_1, scale_0)
    meta_sum[...] = jnp.zeros_like(meta_sum)
    meta_sum[0:heads, :] = top
    meta_sum[heads : 2 * heads, :] = meta_0[heads : 2 * heads] + meta_1[heads : 2 * heads]
    for h in range(heads):
        st_sum[h] = (
            st_own[h].astype(jnp.float32) * scale_own[h : h + 1]
            + st_y[h].astype(jnp.float32) * scale_other[h : h + 1]
        ).astype(jnp.bfloat16)

    def state_z(step, source):
        kept = st_z.at[source], meta_z.at[source]
        to = on_plane(z + step)
        return [
            remote(st_sum, kept[0], (ssem.at[2, step], ssem.at[3, source]), to),
            remote(meta_sum, kept[1], (ssem.at[4, step], ssem.at[5, source]), to),
        ]

    for step in range(1, planes):

        @pl.when(z + step <= last)
        def _():
            for copy in state_z(step, z):
                copy.start()

    for chunk in range(2):
        y_weight(chunk).wait_recv()
        z_send(2 + chunk)

    for h in range(heads):
        for i in range(1, 4):
            attend(h, i)

    low = jnp.full((heads, meta_ref.shape[1]), LOWEST_LOG, jnp.float32)
    later = jnp.where(y == 1, meta_y[heads : 2 * heads, :], 0.0)
    lw_ref[planes - 1, 0:heads, :] = jnp.where(y == 1, meta_y[0:heads, :], low)
    ctop = lw_ref[planes - 1, 0:heads, :]
    for source in range(planes - 2, -1, -1):
        valid = z > source

        @pl.when(valid)
        def _():
            for copy in state_z(0, source):
                copy.wait_recv()

        here = jnp.where(valid, meta_z[source, 0:heads, :] + later, low)
        lw_ref[source, 0:heads, :] = here
        ctop = jnp.maximum(ctop, here)
        later = later + jnp.where(valid, meta_z[source, heads : 2 * heads, :], 0.0)
    ent[...] = jnp.zeros_like(ent)
    for source in range(planes):
        valid = z > source if source < planes - 1 else y == 1

        @pl.when(valid)
        def _():
            scale = jnp.exp(lw_ref[source, 0:heads, :] - ctop)
            for h in range(heads):
                part = st_z[source, h] if source < planes - 1 else st_y[h]
                ent[h] += part.astype(jnp.float32) * scale[h : h + 1]

    z_forward(1, 0)
    z_forward(1, 1)
    z_forward(1, 2)

    def front_core(i):
        at = pl.ds(pl.multiple_of(i * strip, strip), strip)
        return remote(
            pool.at[0:4, at, :], core_in.at[:, at, :], (fsem.at[0, i], fsem.at[1, i]), partner
        )

    def front_x(i):
        at = pl.ds(pl.multiple_of(i * strip, strip), strip)
        return remote(
            pool.at[8:10, at, :], x_in.at[:, at, :], (fsem.at[2, i], fsem.at[3, i]), x_next
        )

    def gate_strip(i):
        at = pl.ds(pl.multiple_of(i * strip, strip), strip)
        gated = []
        for h in range(heads):
            lanes = slice(h * dv, (h + 1) * dv)
            before = jnp.dot(
                q_ref[at, h * dk : (h + 1) * dk],
                ent[h].astype(jnp.bfloat16),
                preferred_element_type=jnp.float32,
            )
            m_log = cols_ref[at, heads + h : heads + h + 1]
            m_all = jnp.maximum(m_log, ctop[h : h + 1, 0:1])
            memory = (
                num[at, lanes] * jnp.exp(m_log - m_all)
                + jnp.exp(ctop[h : h + 1, 0:1] - m_all) * before
            ) * dk ** (-0.5)
            normal = memory * lax.rsqrt(jnp.mean(memory * memory, axis=-1, keepdims=True) + EPSILON)
            opened = jax.nn.sigmoid(open_ref[at, lanes].astype(jnp.float32))
            gated.append((normal * gain_ref[0:1, lanes].astype(jnp.float32) * opened).astype(jnp.bfloat16))
        gated = jnp.concatenate(gated, axis=1)
        for chip in range(NX):
            for part in range(2):
                for mine in range(2):
                    core = c if mine else 1 - c
                    lanes = pl.ds(
                        pl.multiple_of((chip * 2 + core) * width + part * wide, wide), wide
                    )
                    pool[mine * 4 + chip * 2 + part, at, :] = jnp.dot(
                        gated, wo_ref[:, lanes], preferred_element_type=jnp.float32
                    ).astype(jnp.bfloat16)
        front_core(i).start()

    def core_sum(i):
        at = pl.ds(pl.multiple_of(i * strip, strip), strip)
        front_core(i).wait_recv()
        for part in range(2):
            far, near = (1 - x) * 2 + part, x * 2 + part
            pool[8 + part, at, :] = (
                pool[4 + far, at, :].astype(jnp.float32) + core_in[far, at, :].astype(jnp.float32)
            ).astype(jnp.bfloat16)
        front_x(i).start()

    @pl.loop(0, 5)
    def _(i):
        @pl.when(i < 4)
        def _():
            gate_strip(i)

        @pl.when(i >= 1)
        def _():
            core_sum(i - 1)

    z_forward(1, 3)
    z_forward(2, 0)
    y_weight(2).wait_recv()
    own_down.wait()

    def piece(owner_x, owner_c, owner_y, i):
        at = pl.multiple_of(owner_y * tokens + i * strip, strip)
        return rows_all.at[owner_x * 2 + owner_c, pl.ds(at, strip), :]

    def to_x(i):
        part = piece(x, c, y, i)
        return remote(part, part, (gsem.at[0, i], gsem.at[1, i]), x_next)

    def to_y(kind, i):
        part = piece(x if kind == 0 else 1 - x, c, y, i)
        return remote(part, part, (gsem.at[2 + kind, i], gsem.at[4 + kind, i]), y_next)

    def to_core(kind, i):
        part = piece(
            x if kind % 2 == 0 else 1 - x, c, y if kind // 2 == 0 else 1 - y, i
        )
        return remote(part, part, (gsem.at[6 + kind, i], gsem.at[10 + kind, i]), partner)

    @pl.loop(0, 4)
    def _(i):
        at = pl.ds(pl.multiple_of(i * strip, strip), strip)
        front_x(i).wait_recv()
        start = pl.multiple_of(y * tokens + i * strip, strip)
        for part in range(2):
            lanes = slice(part * wide, (part + 1) * wide)
            near = x * 2 + part
            total = (
                pool[4 + near, at, :].astype(jnp.float32)
                + core_in[near, at, :].astype(jnp.float32)
                + x_in[part, at, :].astype(jnp.float32)
            )
            rows_all[tp, pl.ds(start, strip), lanes] = (
                resid_ref[at, lanes].astype(jnp.float32) + total
            ).astype(jnp.bfloat16)
        to_x(i).start()
        to_y(0, i).start()
        to_core(0, i).start()

    z_forward(2, 1)

    @pl.loop(0, 4)
    def _(i):
        to_x(i).wait_recv()
        to_y(1, i).start()
        to_core(1, i).start()

    z_forward(2, 2)
    z_forward(2, 3)
    z_send(4)
    z_send(5)

    @pl.loop(0, 4)
    def _(i):
        to_y(0, i).wait_recv()
        to_core(2, i).start()

    @pl.loop(0, 4)
    def _(i):
        to_y(1, i).wait_recv()
        to_core(3, i).start()

    for dist in range(1, planes - 1):
        for chunk in (4, 5):
            z_forward(dist, chunk)

    for way in range(2):
        for dist in range(1, planes):

            @pl.when(jnp.logical_and(has_origin(way, dist), jnp.logical_not(has_next(way))))
            def _():
                for chunk in range(4):
                    z_arrival(way, dist, chunk).wait_recv()

    @pl.loop(0, 4)
    def _(i):
        for kind in range(4):
            to_core(kind, i).wait_recv()

    @pl.loop(0, 4)
    def _(i):
        for copy in (front_core(i), front_x(i), to_x(i), to_y(0, i), to_y(1, i)):
            copy.wait_send()
        for kind in range(4):
            to_core(kind, i).wait_send()

    tall = normed.shape[0]

    @pl.loop(0, NY * tokens // tall)
    def _(i):
        base = pl.multiple_of(i * tall, tall)

        @pl.loop(0, tall // 64)
        def _(r):
            at = pl.ds(pl.multiple_of(base + r * 64, 64), 64)
            parts = [rows_all[j, at, :].astype(jnp.float32) for j in range(count)]
            square = sum(jnp.sum(p * p, axis=-1, keepdims=True) for p in parts)
            scale = lax.rsqrt(square / (count * width) + EPSILON)
            to = pl.ds(pl.multiple_of(r * 64, 64), 64)
            for j in range(count):
                lanes = slice(j * width, (j + 1) * width)
                normed[to, lanes] = (parts[j] * scale * fgain_ref[0:1, lanes].astype(jnp.float32)).astype(
                    jnp.bfloat16
                )

        both = jnp.dot(normed[...], gu[...], preferred_element_type=jnp.float32)
        hid[pl.ds(base, tall), :] = (jax.nn.silu(both[:, :half]) * both[:, half:]).astype(jnp.bfloat16)

    units = planes * NY

    def place(unit):
        step = unit // NY
        low_bit = (z % 2 + step % 2) % 2
        high = (z // 2 + step // 2) % 2
        return high * 2 + low_bit

    def slot(unit):
        return unit // 4 * 2 + unit % 2

    def back_core(unit):
        return remote(
            pool.at[pl.ds(unit * 2, 2)], core_back.at[slot(unit)], (bsem.at[0, unit], bsem.at[1, unit]), partner
        )

    def back_y(unit):
        return remote(
            pool.at[unit * 2 + 1 - y], y_back.at[slot(unit)], (bsem.at[2, unit], bsem.at[3, unit]), y_next
        )

    def back_x(unit):
        return remote(
            pool.at[unit * 2 + y], x_back.at[unit % 2], (bsem.at[4, unit], bsem.at[5, unit]), x_next
        )

    def keeps(unit):
        return place(unit) % 2 == c

    def owns(unit):
        return place(unit) == tp

    def passes(unit):
        return jnp.logical_and(keeps(unit), place(unit) // 2 != x)

    def down_part(unit):
        step, side = unit // NY, unit % NY

        @pl.when(jnp.logical_and(step > 0, jnp.logical_or(z == 0, z == last)))
        def _():
            at = place(unit) * NY + side
            way = jnp.where(z == 0, 1, 0)
            part = dn.at[at]
            remote(part, part, (zs.at[way, step, 4 + side], zr.at[way, step, 4 + side]), on_plane(z)).wait_recv()

        weight = dn[place(unit) * NY + side]
        for top_row in range(NY):
            for quarter in range(2):
                rows = tokens // 2
                start = top_row * tokens + quarter * rows
                pool[unit * 2 + top_row, pl.ds(quarter * rows, rows), :] = jnp.dot(
                    hid[pl.ds(start, rows), :], weight, preferred_element_type=jnp.float32
                ).astype(jnp.bfloat16)

        @pl.when(jnp.logical_not(keeps(unit)))
        def _():
            back_core(unit).start()

    def after_core(unit):
        @pl.when(keeps(unit))
        def _():
            back_core(unit).wait_recv()
            for side in (1 - y, y):
                pool[unit * 2 + side] = (
                    pool[unit * 2 + side].astype(jnp.float32)
                    + core_back[slot(unit), side].astype(jnp.float32)
                ).astype(jnp.bfloat16)
            back_y(unit).start()

    def after_y(unit):
        @pl.when(keeps(unit))
        def _():
            back_y(unit).wait_recv()
            pool[unit * 2 + y] = (
                pool[unit * 2 + y].astype(jnp.float32) + y_back[slot(unit)].astype(jnp.float32)
            ).astype(jnp.bfloat16)

        @pl.when(passes(unit))
        def _():
            back_x(unit).start()

    def after_x(unit):
        @pl.when(owns(unit))
        def _():
            back_x(unit).wait_recv()
            total = pool[unit * 2 + y].astype(jnp.float32) + x_back[unit % 2].astype(jnp.float32)
            lanes = pl.ds(pl.multiple_of((unit % 2) * wide, wide), wide)
            mine = pl.ds(pl.multiple_of(y * tokens, tokens), tokens)
            out_ref[:, lanes] = (
                rows_all[tp, mine, lanes].astype(jnp.float32) + 0.5 * total
            ).astype(out_ref.dtype)

    @pl.loop(0, units + 3)
    def _(i):
        @pl.when(i < units)
        def _():
            down_part(i)

        @pl.when(jnp.logical_and(i >= 1, i < units + 1))
        def _():
            after_core(i - 1)

        @pl.when(jnp.logical_and(i >= 2, i < units + 2))
        def _():
            after_y(i - 2)

        @pl.when(i >= 3)
        def _():
            after_x(i - 3)

    @pl.loop(0, units)
    def _(i):
        @pl.when(jnp.logical_not(keeps(i)))
        def _():
            back_core(i).wait_send()

        @pl.when(keeps(i))
        def _():
            back_y(i).wait_send()

        @pl.when(passes(i))
        def _():
            back_x(i).wait_send()

    for chunk in range(3):
        y_weight(chunk).wait_send()
    for copy in state_y:
        copy.wait_send()
    for step in range(1, planes):

        @pl.when(z + step <= last)
        def _():
            for copy in state_z(step, z):
                copy.wait_send()

    for way in range(2):
        for dist in range(planes - 1):

            @pl.when(jnp.logical_and(has_origin(way, dist), has_next(way)))
            def _():
                for chunk in range(6):
                    z_copy(way, dist, chunk).wait_send()


def plane_layer(
    planes,
    queries,
    cell_key_rows,
    cell_value_rows,
    output_gate_logits,
    input_gate_logits,
    forget_gate_logits,
    forget_extra_term,
    residual,
    head_norm_gain,
    cell_output_weight,
    feedforward_norm_gain,
    gate_projection_weight,
    up_projection_weight,
    down_projection_weight,
):
    tokens, heads = queries.shape[0], input_gate_logits.shape[0]
    width = residual.shape[1]
    model = cell_output_weight.shape[1]
    depth, hidden = gate_projection_weight.shape
    half = hidden // NY
    dk, dv = queries.shape[1] // heads, cell_value_rows.shape[1] // heads
    log_forget = jax.nn.log_sigmoid(forget_gate_logits.astype(jnp.float32)) + forget_extra_term
    running = jnp.cumsum(log_forget, axis=-1)
    a_log = input_gate_logits.astype(jnp.float32) - running
    m_log = lax.cummax(a_log, axis=1)
    a_top, total = m_log[:, -1], running[:, -1]
    decay = jnp.exp(a_log - a_top[:, None])
    cols = jnp.concatenate([decay, m_log], axis=0).T
    meta = jnp.concatenate([a_top + total, total, jnp.zeros((8 - 2 * heads,), jnp.float32)])
    meta = jnp.broadcast_to(meta[:, None], (8, dv))
    bf16, f32 = jnp.bfloat16, jnp.float32
    vmem, dma = pltpu.VMEM, pltpu.SemaphoreType.DMA
    scratch = [
        vmem((model, hidden), bf16),
        vmem((planes * NY, half, depth), bf16),
        vmem((2 * NX, NY * tokens, width), bf16),
        vmem((NY * tokens, half), bf16),
        vmem((depth, hidden), bf16),
        vmem((tokens, heads * dv), f32),
        vmem((heads, dk, dv), f32),
        vmem((heads, dk, dv), bf16),
        vmem((heads, dk, dv), bf16),
        vmem((heads, dk, dv), bf16),
        vmem((planes - 1, heads, dk, dv), bf16),
        vmem((8, dv), f32),
        vmem((8, dv), f32),
        vmem((planes - 1, 8, dv), f32),
        vmem((planes, 8, dv), f32),
        vmem((2 * planes * NY, tokens, width // 2), bf16),
        vmem((4, tokens, width // 2), bf16),
        vmem((2, tokens, width // 2), bf16),
        vmem((512, model), bf16),
        vmem((planes * NY // 2, 2, tokens, width // 2), bf16),
        vmem((planes * NY // 2, tokens, width // 2), bf16),
        vmem((2, tokens, width // 2), bf16),
        dma((2, planes, 6)),
        dma((2, planes, 6)),
        dma((2, 3)),
        dma((6, planes)),
        dma((4, 4)),
        dma((14, 4)),
        dma((6, planes * NY)),
        dma((1,)),
    ]
    whole = pl.BlockSpec(memory_space=pltpu.VMEM)
    return pl.pallas_call(
        functools.partial(block_body, planes),
        out_shape=jax.ShapeDtypeStruct((tokens, width), bf16),
        in_specs=[whole] * 14,
        out_specs=whole,
        scratch_shapes=scratch,
        compiler_params=pltpu.CompilerParams(
            collective_id=0, has_side_effects=True, vmem_limit_bytes=67043328
        ),
        cost_estimate=pl.CostEstimate(flops=22 * 10**9, bytes_accessed=10**7, transcendentals=0),
        name="block",
    )(
        queries,
        cell_key_rows,
        cell_value_rows,
        output_gate_logits,
        a_log,
        cols,
        meta,
        residual,
        head_norm_gain[None, :],
        cell_output_weight,
        feedforward_norm_gain[None, :],
        gate_projection_weight,
        up_projection_weight,
        down_projection_weight,
    )


def layer(rows, columns, *arrays):
    if columns == 2 * NX and rows == 4 * NY:
        return plane_layer(rows // NY, *arrays)
    return general(*arrays)


def solution(mesh):
    placed = (
        P("sp", "tp"),
        P("sp", "tp"),
        P("sp", "tp"),
        P("sp", "tp"),
        P("tp", "sp"),
        P("tp", "sp"),
        P("tp", "sp"),
        P("sp", "tp"),
        P("tp"),
        P("tp", None),
        P(),
        P("sp", "tp"),
        P("sp", "tp"),
        P("tp", "sp"),
    )
    return jax.shard_map(
        functools.partial(layer, mesh.shape["sp"], mesh.shape["tp"]), mesh=mesh, in_specs=placed, out_specs=P("sp", "tp"), check_vma=False
    )
```

```python
import functools

import jax
import jax.numpy as jnp
from jax import lax
from jax.experimental import pallas as pl
from jax.experimental.pallas import tpu as pltpu
from jax.sharding import PartitionSpec as P

LOWEST_LOG = -1e30
EPSILON = 1e-06


def shift_pairs(length, step):
    return [(source, source + step) for source in range(length - step)]


def entering_state(state, top, total):
    length, index = lax.axis_size("sp"), lax.axis_index("sp")
    heads, key_width, value_width = state.shape

    def pack(s, t, f):
        tail = jnp.zeros((heads, 8, value_width), jnp.float32)
        tail = tail.at[:, 0, :].set(t[:, None]).at[:, 1, :].set(f[:, None])
        return jnp.concatenate([s, tail], axis=1)

    def unpack(p, valid):
        s = p[:, :key_width, :]
        t = jnp.where(valid, p[:, key_width, 0], LOWEST_LOG)
        f = jnp.where(valid, p[:, key_width + 1, 0], 0.0)
        return jnp.where(valid, s, 0.0), t, f

    moved = lax.ppermute(pack(state, top, total), "sp", shift_pairs(length, 1))
    s, t, f = unpack(moved, index >= 1)
    step = 1
    while step < length - 1:
        moved = lax.ppermute(pack(s, t, f), "sp", shift_pairs(length, step))
        s0, t0, f0 = unpack(moved, index >= step)
        from_top = t0 + f
        new_top = jnp.maximum(from_top, t)
        s = (
            jnp.exp(from_top - new_top)[:, None, None] * s0
            + jnp.exp(t - new_top)[:, None, None] * s
        )
        t, f = new_top, f0 + f
        step *= 2
    return s, t


def cell_kernel(q_ref, k_ref, v_ref, a_ref, m_ref, c_ref, state_ref, open_ref, gain_ref, o_ref, *, scale):
    block = q_ref.shape[0]
    length = k_ref.shape[0]
    q = q_ref[...]
    first = pl.program_id(1) * block
    scores = lax.dot_general(
        q, k_ref[...], (((1,), (1,)), ((), ())), preferred_element_type=jnp.float32
    )
    rows = first + lax.broadcasted_iota(jnp.int32, (block, length), 0)
    cols = lax.broadcasted_iota(jnp.int32, (block, length), 1)
    weight = jnp.where(cols <= rows, jnp.exp(jnp.minimum(a_ref[0] - m_ref[0], 0.0)), 0.0)
    numer = jnp.dot(
        (scores * weight).astype(jnp.bfloat16), v_ref[...], preferred_element_type=jnp.float32
    )
    before = jnp.dot(q, state_ref[0].astype(jnp.bfloat16), preferred_element_type=jnp.float32)
    memory = (numer + c_ref[0] * before) * scale
    normal = memory * lax.rsqrt(jnp.mean(memory * memory, axis=-1, keepdims=True) + EPSILON)
    gate_open = jax.nn.sigmoid(open_ref[...].astype(jnp.float32))
    o_ref[...] = (normal * gain_ref[...].astype(jnp.float32) * gate_open).astype(o_ref.dtype)


def cell(queries, keys, values, a_log, m_col, c_col, state, open_logits, gain):
    heads, length = a_log.shape
    dk, dv = queries.shape[1] // heads, values.shape[1] // heads
    block = min(length, 256)
    return pl.pallas_call(
        lambda *refs: cell_kernel(*refs, scale=dk ** (-0.5)),
        grid=(heads, length // block),
        in_specs=[
            pl.BlockSpec((block, dk), lambda h, i: (i, h)),
            pl.BlockSpec((length, dk), lambda h, i: (0, h)),
            pl.BlockSpec((length, dv), lambda h, i: (0, h)),
            pl.BlockSpec((1, 1, length), lambda h, i: (h, 0, 0)),
            pl.BlockSpec((1, block, 1), lambda h, i: (h, i, 0)),
            pl.BlockSpec((1, block, 1), lambda h, i: (h, i, 0)),
            pl.BlockSpec((1, dk, dv), lambda h, i: (h, 0, 0)),
            pl.BlockSpec((block, dv), lambda h, i: (i, h)),
            pl.BlockSpec((1, dv), lambda h, i: (0, h)),
        ],
        out_specs=pl.BlockSpec((block, dv), lambda h, i: (i, h)),
        out_shape=jax.ShapeDtypeStruct((length, heads * dv), jnp.bfloat16),
        cost_estimate=pl.CostEstimate(
            flops=8 * heads * length * length * dv, bytes_accessed=6 * length * heads * dv, transcendentals=0
        ),
        name="cell",
    )(queries, keys, values, a_log[:, None, :], m_col[:, :, None], c_col[:, :, None], state, open_logits, gain)


def partner_pairs(count):
    return [(i, i ^ 1) for i in range(count)]


def ring_pairs(count, step):
    return [(i, (i + 2 * step) % count) for i in range(count)]


def product_scattered(rows, weight):
    count, index = lax.axis_size("tp"), lax.axis_index("tp")
    chips, core, chip = count // 2, index % 2, index // 2
    width = weight.shape[1] // count

    def product(block):
        columns = lax.dynamic_slice_in_dim(weight, block * width, width, 1)
        return jnp.dot(rows, columns, preferred_element_type=jnp.float32)

    def chip_sum(to):
        given = product(2 * to + 1 - core).astype(jnp.bfloat16)
        got = lax.ppermute(given, "tp", partner_pairs(count))
        return product(2 * to + core) + got.astype(jnp.float32)

    moved = []
    for step in range(1, chips):
        sent = chip_sum((chip + step) % chips).astype(jnp.bfloat16)
        moved.append(lax.ppermute(sent, "tp", ring_pairs(count, step)))
    total = chip_sum(chip)
    for part in moved:
        total = total + part.astype(jnp.float32)
    return total


def columns_gathered(block):
    count, index = lax.axis_size("tp"), lax.axis_index("tp")
    chips, core, chip = count // 2, index % 2, index // 2
    width = block.shape[1]
    whole = jnp.zeros((block.shape[0], count * width), block.dtype)
    held = [(chip, block)]
    for step in range(1, chips):
        moved = lax.ppermute(block, "tp", ring_pairs(count, step))
        held.append(((chip - step) % chips, moved))
    for place, piece in held:
        other = lax.ppermute(piece, "tp", partner_pairs(count))
        whole = lax.dynamic_update_slice(whole, piece, (0, (2 * place + core) * width))
        whole = lax.dynamic_update_slice(whole, other, (0, (2 * place + 1 - core) * width))
    return whole


def general(
    queries,
    cell_key_rows,
    cell_value_rows,
    output_gate_logits,
    input_gate_logits,
    forget_gate_logits,
    forget_extra_term,
    residual,
    head_norm_gain,
    cell_output_weight,
    feedforward_norm_gain,
    gate_projection_weight,
    up_projection_weight,
    down_projection_weight,
):
    whole_gate = lax.all_gather(gate_projection_weight, "sp", axis=0, tiled=True)
    whole_up = lax.all_gather(up_projection_weight, "sp", axis=0, tiled=True)
    length = queries.shape[0]
    heads = input_gate_logits.shape[0]
    dk, dv = queries.shape[1] // heads, cell_value_rows.shape[1] // heads
    log_forget = jax.nn.log_sigmoid(forget_gate_logits.astype(jnp.float32)) + forget_extra_term
    running = jnp.cumsum(log_forget, axis=-1)
    a_log = input_gate_logits.astype(jnp.float32) - running
    m_log = lax.cummax(a_log, axis=1)
    a_top, total = m_log[:, -1], running[:, -1]
    decay = jnp.exp(a_log - a_top[:, None])
    weighed = (
        cell_key_rows.reshape(length, heads, dk).astype(jnp.float32) * decay.T[:, :, None]
    ).astype(jnp.bfloat16)
    state = jnp.stack(
        [
            lax.dot_general(
                weighed[:, h],
                cell_value_rows[:, h * dv : (h + 1) * dv],
                (((0,), (0,)), ((), ())),
                preferred_element_type=jnp.float32,
            )
            for h in range(heads)
        ]
    )
    carried, carried_top = entering_state(state, a_top + total, total)
    m_all = jnp.maximum(m_log, carried_top[:, None])
    coefficient = jnp.exp(carried_top[:, None] - m_all)
    gated = cell(
        queries,
        cell_key_rows,
        cell_value_rows,
        a_log,
        m_all,
        coefficient,
        carried,
        output_gate_logits,
        head_norm_gain[None, :],
    )
    summed = product_scattered(gated, cell_output_weight)
    stream = (residual.astype(jnp.float32) + summed).astype(jnp.bfloat16)
    down_late, stream = lax.optimization_barrier((down_projection_weight, stream))
    whole_down = lax.all_gather(down_late, "sp", axis=1, tiled=True)
    wide = columns_gathered(stream).astype(jnp.float32)
    scale = lax.rsqrt(jnp.mean(wide * wide, axis=-1, keepdims=True) + EPSILON)
    normed = (wide * scale * feedforward_norm_gain.astype(jnp.float32)[None, :]).astype(jnp.bfloat16)
    gate_value = jnp.dot(normed, whole_gate, preferred_element_type=jnp.float32)
    lifted = jnp.dot(normed, whole_up, preferred_element_type=jnp.float32)
    hidden = (jax.nn.silu(gate_value) * lifted).astype(jnp.bfloat16)
    channel_total = product_scattered(hidden, whole_down)
    return (stream.astype(jnp.float32) + 0.5 * channel_total).astype(jnp.bfloat16)


NX, NY = 2, 2
BY_NAME = pl.DeviceIdType.MESH


def block_body(
    planes,
    q_in,
    k_in,
    v_in,
    open_in,
    input_in,
    forget_in,
    extra_in,
    resid_in,
    gain_ref,
    wo_in,
    fgain_ref,
    gate_in,
    up_in,
    down_ref,
    out_ref,
    gate_ref,
    up_ref,
    wo_ref,
    a_ref,
    cols_ref,
    meta_ref,
    gu,
    dn,
    rows_all,
    hid,
    sums,
    gu_out,
    num,
    ent,
    st_own,
    st_y,
    st_sum,
    st_z,
    meta_y,
    meta_sum,
    meta_z,
    lw_ref,
    pool,
    core_in,
    x_in,
    core_back,
    y_back,
    x_back,
    zs,
    zr,
    ysem,
    ssem,
    fsem,
    gsem,
    bsem,
    lsem,
):
    sp, tp = lax.axis_index("sp"), lax.axis_index("tp")
    z, y, x, c = sp // NY, sp % NY, tp // 2, tp % 2
    tokens, heads = q_in.shape[0], input_in.shape[0]
    dk, dv = q_in.shape[1] // heads, v_in.shape[1] // heads
    width = resid_in.shape[1]
    depth, hidden = gate_ref.shape
    half = hidden // NY
    count = 2 * NX
    last = planes - 1
    strip = tokens // 4
    wide = width // 2
    part_rows = depth // 2

    partner = {"tp": tp + 1 - 2 * c}
    x_next = {"tp": (1 - x) * 2 + c}
    y_next = {"sp": z * NY + 1 - y}

    def on_plane(at):
        return {"sp": at * NY + y}

    def remote(src, dst, sems, to):
        return pltpu.make_async_remote_copy(
            src_ref=src, dst_ref=dst, send_sem=sems[0], recv_sem=sems[1], device_id=to, device_id_type=BY_NAME
        )

    q_ref, k_ref = core_back.at[0, 0], core_back.at[0, 1]
    v_ref, open_ref, resid_ref = core_back.at[1], core_back.at[2], core_back.at[3]
    loads = {}
    wanted = [("gate", gate_in, gate_ref), ("up", up_in, up_ref), ("k", k_in, k_ref)]
    for name, source, kept in (("v", v_in, v_ref), ("q", q_in, q_ref), ("open", open_in, open_ref)):
        if name == "q":
            wanted.append((name, source, kept))
        else:
            for part in range(2):
                wanted.append((name + str(part), source.at[:, part * wide : (part + 1) * wide], kept.at[part]))
    wanted.append(("wo", wo_in, wo_ref))
    for part in range(2):
        wanted.append(("resid" + str(part), resid_in.at[:, part * wide : (part + 1) * wide], resid_ref.at[part]))
    for index, (name, source, kept) in enumerate(wanted):
        loads[name] = pltpu.make_async_copy(source, kept, lsem.at[index + 1])
        loads[name].start()

    barrier = pltpu.get_barrier_semaphore()
    for to in (partner, x_next, y_next):
        pl.semaphore_signal(barrier, inc=1, device_id=to, device_id_type=BY_NAME)
    for step in range(1, planes):
        pl.semaphore_signal(
            barrier, inc=1, device_id=on_plane((z + step) % planes), device_id_type=BY_NAME
        )
    pl.semaphore_wait(barrier, planes + 2)

    loads["gate"].wait()
    loads["up"].wait()

    for mine in range(NY):

        @pl.when(y == mine)
        def _():
            own = pl.ds(pl.multiple_of(sp * depth, depth), depth)
            here, there = mine * half, (1 - mine) * half
            gu_out[:, 0:half] = gate_ref[:, there : there + half]
            gu_out[:, half : 2 * half] = up_ref[:, there : there + half]
            gu[own, 0:half] = gate_ref[:, here : here + half]
            gu[own, half : 2 * half] = up_ref[:, here : here + half]

    def gu_rows(at, chunk):
        side = (y + chunk // 2) % 2
        start = (at * NY + side) * depth + (chunk % 2) * part_rows
        return pl.ds(pl.multiple_of(start, part_rows), part_rows)

    def z_copy(way, dist, chunk):
        at = z - dist if way == 0 else z + dist
        to = z + 1 if way == 0 else z - 1
        sems = (zs.at[way, dist, chunk], zr.at[way, dist + 1, chunk])
        if chunk < 4:
            part = gu.at[gu_rows(at, chunk), :]
        else:
            part = dn.at[at * NY + chunk - 4]
        return remote(part, part, sems, on_plane(to))

    def z_arrival(way, dist, chunk):
        at = z - dist if way == 0 else z + dist
        sems = (zs.at[way, dist, chunk], zr.at[way, dist, chunk])
        if chunk < 4:
            part = gu.at[gu_rows(at, chunk), :]
        else:
            part = dn.at[at * NY + chunk - 4]
        return remote(part, part, sems, on_plane(z))

    def has_next(way):
        return z < last if way == 0 else z > 0

    def has_origin(way, dist):
        return z >= dist if way == 0 else z + dist <= last

    def z_send(chunk):
        for way in range(2):

            @pl.when(has_next(way))
            def _():
                z_copy(way, 0, chunk).start()

    def z_forward(dist, chunk):
        for way in range(2):

            @pl.when(jnp.logical_and(has_origin(way, dist), has_next(way)))
            def _():
                z_arrival(way, dist, chunk).wait_recv()
                z_copy(way, dist, chunk).start()

    def z_down(rank, dist):
        for way in range(2):

            @pl.when(z == (rank if way == 0 else last - rank))
            def _():
                for chunk in (4, 5):
                    if dist:
                        z_arrival(way, dist, chunk).wait_recv()
                    z_copy(way, dist, chunk).start()

    def y_rows(owner, chunk):
        start = (z * NY + owner) * depth + chunk * part_rows
        return pl.ds(pl.multiple_of(start, part_rows), part_rows)

    def y_weight(chunk):
        sems = (ysem.at[0, chunk], ysem.at[1, chunk])
        if chunk < 2:
            return remote(
                gu_out.at[pl.ds(chunk * part_rows, part_rows), :], gu.at[y_rows(y, chunk), :], sems, y_next
            )
        start = pl.multiple_of((1 - y) * half, half)
        return remote(down_ref.at[pl.ds(start, half), :], dn.at[sp], sems, y_next)

    own_down = pltpu.make_async_copy(
        down_ref.at[pl.ds(pl.multiple_of(y * half, half), half), :], dn.at[sp], lsem.at[0]
    )
    z_send(0)

    def padded(rows):
        return jnp.concatenate([rows, jnp.zeros((8 - heads, tokens), jnp.float32)], axis=0)

    lane = lax.broadcasted_iota(jnp.int32, (8, tokens), 1)
    logits = forget_in[...].astype(jnp.float32)
    running = padded(
        jnp.minimum(logits, 0.0) - jnp.log1p(jnp.exp(-jnp.abs(logits))) + extra_in[...]
    )
    step = 1
    while step < tokens:
        running = running + jnp.where(lane >= step, pltpu.roll(running, step, 1), 0.0)
        step *= 2
    a_log = padded(input_in[...].astype(jnp.float32)) - running
    m_log = a_log
    step = 1
    while step < tokens:
        m_log = jnp.maximum(m_log, jnp.where(lane >= step, pltpu.roll(m_log, step, 1), LOWEST_LOG))
        step *= 2
    a_ref[...] = a_log
    a_top, total = m_log[:, tokens - 1 :], running[:, tokens - 1 :]
    decay = jnp.exp(a_log - a_top)
    cols_ref[...] = jnp.concatenate(
        [decay[0:heads], m_log[0:heads], jnp.zeros((8 - 2 * heads, tokens), jnp.float32)], axis=0
    ).T
    meta_ref[...] = jnp.zeros_like(meta_ref)
    meta_ref[0:heads, :] = jnp.broadcast_to((a_top + total)[0:heads], (heads, meta_ref.shape[1]))
    meta_ref[heads : 2 * heads, :] = jnp.broadcast_to(total[0:heads], (heads, meta_ref.shape[1]))
    for name in ("k", "v0", "v1"):
        loads[name].wait()

    for h in range(heads):
        weighed = (
            k_ref[:, h * dk : (h + 1) * dk].astype(jnp.float32) * cols_ref[:, h : h + 1]
        ).astype(jnp.bfloat16)
        st_own[h] = lax.dot_general(
            weighed,
            v_ref[h],
            (((0,), (0,)), ((), ())),
            preferred_element_type=jnp.float32,
        ).astype(jnp.bfloat16)

    state_y = [
        remote(st_own, st_y, (ssem.at[0, 0], ssem.at[0, 1]), y_next),
        remote(meta_ref, meta_y, (ssem.at[1, 0], ssem.at[1, 1]), y_next),
    ]
    for copy in state_y:
        copy.start()
    for chunk in range(3):
        y_weight(chunk).start()
    own_down.start()
    loads["q"].wait()

    def attend(h, i):
        span = (i + 1) * strip
        at = pl.ds(i * strip, strip)
        scores = lax.dot_general(
            q_ref[at, h * dk : (h + 1) * dk],
            k_ref[0:span, h * dk : (h + 1) * dk],
            (((1,), (1,)), ((), ())),
            preferred_element_type=jnp.float32,
        )
        log_weight = a_ref[h : h + 1, 0:span] - cols_ref[at, heads + h : heads + h + 1]
        row = i * strip + lax.broadcasted_iota(jnp.int32, (strip, span), 0)
        col = lax.broadcasted_iota(jnp.int32, (strip, span), 1)
        weight = jnp.where(col <= row, jnp.exp(jnp.minimum(log_weight, 0.0)), 0.0)
        num[at, h * dv : (h + 1) * dv] = jnp.dot(
            (scores * weight).astype(jnp.bfloat16),
            v_ref[h, 0:span, :],
            preferred_element_type=jnp.float32,
        )

    for h in range(heads):
        attend(h, 0)

    for copy in state_y:
        copy.wait_recv()
    first = y == 0
    meta_own, meta_other = meta_ref[...], meta_y[...]
    meta_0 = jnp.where(first, meta_own, meta_other)
    meta_1 = jnp.where(first, meta_other, meta_own)
    top_0 = meta_0[0:heads] + meta_1[heads : 2 * heads]
    top_1 = meta_1[0:heads]
    top = jnp.maximum(top_0, top_1)
    scale_0, scale_1 = jnp.exp(top_0 - top), jnp.exp(top_1 - top)
    scale_own = jnp.where(first, scale_0, scale_1)
    scale_other = jnp.where(first, scale_1, scale_0)
    meta_sum[...] = jnp.zeros_like(meta_sum)
    meta_sum[0:heads, :] = top
    meta_sum[heads : 2 * heads, :] = meta_0[heads : 2 * heads] + meta_1[heads : 2 * heads]
    for h in range(heads):
        st_sum[h] = (
            st_own[h].astype(jnp.float32) * scale_own[h : h + 1]
            + st_y[h].astype(jnp.float32) * scale_other[h : h + 1]
        ).astype(jnp.bfloat16)

    def state_z(step, source):
        kept = st_z.at[source], meta_z.at[source]
        to = on_plane(z + step)
        return [
            remote(st_sum, kept[0], (ssem.at[2, step], ssem.at[3, source]), to),
            remote(meta_sum, kept[1], (ssem.at[4, step], ssem.at[5, source]), to),
        ]

    for step in range(1, planes):

        @pl.when(z + step <= last)
        def _():
            for copy in state_z(step, z):
                copy.start()

    z_send(1)
    for h in range(heads):
        for i in range(1, 4):
            attend(h, i)
    y_weight(0).wait_recv()
    z_send(2)

    low = jnp.full((heads, meta_ref.shape[1]), LOWEST_LOG, jnp.float32)
    later = jnp.where(y == 1, meta_y[heads : 2 * heads, :], 0.0)
    lw_ref[planes - 1, 0:heads, :] = jnp.where(y == 1, meta_y[0:heads, :], low)
    ctop = lw_ref[planes - 1, 0:heads, :]
    for source in range(planes - 2, -1, -1):
        valid = z > source

        @pl.when(valid)
        def _():
            for copy in state_z(0, source):
                copy.wait_recv()

        here = jnp.where(valid, meta_z[source, 0:heads, :] + later, low)
        lw_ref[source, 0:heads, :] = here
        ctop = jnp.maximum(ctop, here)
        later = later + jnp.where(valid, meta_z[source, heads : 2 * heads, :], 0.0)
    ent[...] = jnp.zeros_like(ent)
    for source in range(planes):
        valid = z > source if source < planes - 1 else y == 1

        @pl.when(valid)
        def _():
            scale = jnp.exp(lw_ref[source, 0:heads, :] - ctop)
            for h in range(heads):
                part = st_z[source, h] if source < planes - 1 else st_y[h]
                ent[h] += part.astype(jnp.float32) * scale[h : h + 1]

    for name in ("open0", "open1", "wo"):
        loads[name].wait()

    def front_core(i):
        at = pl.ds(pl.multiple_of(i * strip, strip), strip)
        return remote(
            pool.at[0:4, at, :], core_in.at[:, at, :], (fsem.at[0, i], fsem.at[1, i]), partner
        )

    def front_x(i):
        at = pl.ds(pl.multiple_of(i * strip, strip), strip)
        return remote(
            pool.at[8:10, at, :], x_in.at[:, at, :], (fsem.at[2, i], fsem.at[3, i]), x_next
        )

    def gate_strip(i):
        at = pl.ds(pl.multiple_of(i * strip, strip), strip)
        gated = []
        for h in range(heads):
            lanes = slice(h * dv, (h + 1) * dv)
            before = jnp.dot(
                q_ref[at, h * dk : (h + 1) * dk],
                ent[h].astype(jnp.bfloat16),
                preferred_element_type=jnp.float32,
            )
            m_log = cols_ref[at, heads + h : heads + h + 1]
            m_all = jnp.maximum(m_log, ctop[h : h + 1, 0:1])
            memory = (
                num[at, lanes] * jnp.exp(m_log - m_all)
                + jnp.exp(ctop[h : h + 1, 0:1] - m_all) * before
            ) * dk ** (-0.5)
            normal = memory * lax.rsqrt(jnp.mean(memory * memory, axis=-1, keepdims=True) + EPSILON)
            opened = jax.nn.sigmoid(open_ref[h, at, :].astype(jnp.float32))
            gated.append((normal * gain_ref[lanes][None, :].astype(jnp.float32) * opened).astype(jnp.bfloat16))
        gated = jnp.concatenate(gated, axis=1)
        for chip in range(NX):
            for part in range(2):
                for mine in range(2):
                    core = c if mine else 1 - c
                    lanes = pl.ds(
                        pl.multiple_of((chip * 2 + core) * width + part * wide, wide), wide
                    )
                    pool[mine * 4 + chip * 2 + part, at, :] = jnp.dot(
                        gated, wo_ref[:, lanes], preferred_element_type=jnp.float32
                    ).astype(jnp.bfloat16)
        front_core(i).start()

    def core_sum(i):
        at = pl.ds(pl.multiple_of(i * strip, strip), strip)
        front_core(i).wait_recv()
        for part in range(2):
            far, near = (1 - x) * 2 + part, x * 2 + part
            pool[8 + part, at, :] = (
                pool[4 + far, at, :].astype(jnp.float32) + core_in[far, at, :].astype(jnp.float32)
            ).astype(jnp.bfloat16)
        front_x(i).start()

    @pl.loop(0, 5)
    def _(i):
        @pl.when(i < 4)
        def _():
            gate_strip(i)

        @pl.when(i == 2)
        def _():
            y_weight(1).wait_recv()
            z_send(3)

        @pl.when(i >= 1)
        def _():
            core_sum(i - 1)

    z_forward(1, 0)
    z_forward(1, 1)
    y_weight(2).wait_recv()
    own_down.wait()
    z_down(0, 0)
    for part in range(2):
        loads["resid" + str(part)].wait()

    def piece(owner_x, owner_c, owner_y, i):
        at = pl.multiple_of(owner_y * tokens + i * strip, strip)
        lanes = pl.multiple_of((owner_x * 2 + owner_c) * width, width)
        return rows_all.at[pl.ds(at, strip), pl.ds(lanes, width)]

    def to_x(i):
        part = piece(x, c, y, i)
        return remote(part, part, (gsem.at[0, i], gsem.at[1, i]), x_next)

    def to_y(kind, i):
        part = piece(x if kind == 0 else 1 - x, c, y, i)
        return remote(part, part, (gsem.at[2 + kind, i], gsem.at[4 + kind, i]), y_next)

    def to_core(kind, i):
        part = piece(
            x if kind % 2 == 0 else 1 - x, c, y if kind // 2 == 0 else 1 - y, i
        )
        return remote(part, part, (gsem.at[6 + kind, i], gsem.at[10 + kind, i]), partner)

    @pl.loop(0, 4)
    def _(i):
        at = pl.ds(pl.multiple_of(i * strip, strip), strip)
        front_x(i).wait_recv()
        start = pl.multiple_of(y * tokens + i * strip, strip)
        for part in range(2):
            lanes = slice(part * wide, (part + 1) * wide)
            near = x * 2 + part
            total = (
                pool[4 + near, at, :].astype(jnp.float32)
                + core_in[near, at, :].astype(jnp.float32)
                + x_in[part, at, :].astype(jnp.float32)
            )
            fresh = (resid_ref[part, at, :].astype(jnp.float32) + total).astype(jnp.bfloat16)
            out_ref[at, lanes] = fresh
            columns = pl.ds(pl.multiple_of(tp * width + part * wide, wide), wide)
            rows_all[pl.ds(start, strip), columns] = fresh
        to_x(i).start()
        to_y(0, i).start()
        to_core(0, i).start()

        @pl.when(i == 1)
        def _():
            z_forward(1, 2)

    z_forward(1, 3)
    z_down(1, 0)

    @pl.loop(0, 4)
    def _(i):
        to_x(i).wait_recv()
        to_y(1, i).start()
        to_core(1, i).start()

        @pl.when(i == 1)
        def _():
            z_forward(2, 0)
            z_forward(2, 1)

    z_forward(2, 2)
    z_down(1, 1)

    @pl.loop(0, 4)
    def _(i):
        to_y(0, i).wait_recv()
        to_core(2, i).start()

    @pl.loop(0, 4)
    def _(i):
        to_y(1, i).wait_recv()
        to_core(3, i).start()

    z_forward(2, 3)
    z_down(2, 0)

    @pl.loop(0, 4)
    def _(i):
        for kind in range(4):
            to_core(kind, i).wait_recv()

    @pl.loop(0, 4)
    def _(i):
        for copy in (front_core(i), front_x(i), to_x(i), to_y(0, i), to_y(1, i)):
            copy.wait_send()
        for kind in range(4):
            to_core(kind, i).wait_send()

    short = 32

    @pl.loop(0, NY * tokens // short)
    def _(i):
        at = pl.ds(pl.multiple_of(i * short, short), short)
        wide_rows = rows_all[at, :].astype(jnp.float32)
        scale = lax.rsqrt(jnp.mean(wide_rows * wide_rows, axis=-1, keepdims=True) + EPSILON)
        rows_all[at, :] = (wide_rows * scale * fgain_ref[...][None, :].astype(jnp.float32)).astype(
            jnp.bfloat16
        )

    tall = 512
    plane_rows = NY * depth
    early = last * plane_rows
    early_at = jnp.where(z == last, plane_rows, 0)
    late_at = jnp.where(z == last, 0, early)

    def gate_up(i, start, size):
        at = pl.ds(pl.multiple_of(i * tall, tall), tall)
        taken = pl.ds(pl.multiple_of(start, plane_rows), size)
        return at, jnp.dot(rows_all[at, taken], gu[taken, :], preferred_element_type=jnp.float32)

    def gu_arrived(dist):
        for way in range(2):

            @pl.when(jnp.logical_and(has_origin(way, dist), jnp.logical_not(has_next(way))))
            def _():
                for chunk in range(4):
                    z_arrival(way, dist, chunk).wait_recv()

    for dist in range(1, last):
        gu_arrived(dist)

    @pl.loop(0, NY * tokens // tall)
    def _(i):
        at, product = gate_up(i, early_at, early)
        sums[at, :] = product

    gu_arrived(last)

    @pl.loop(0, NY * tokens // tall)
    def _(i):
        at, product = gate_up(i, late_at, plane_rows)
        both = sums[at, :] + product
        hid[at, :] = (jax.nn.silu(both[:, :half]) * both[:, half:]).astype(jnp.bfloat16)

    z_down(2, 1)
    z_down(2, 2)

    units = planes * NY * 2
    rows = tokens // 2

    def side_of(unit):
        return unit // 2 % NY

    def place(unit):
        step = unit // (2 * NY)
        inner = jnp.where(step < planes - 1, (step + 1) % (planes - 1), step)
        base = jnp.where(jnp.logical_or(z == 0, z == last), step, inner)
        return jnp.where(z < planes // 2, base, last - base)

    def slot(unit):
        return unit // 8 * 2 + side_of(unit)

    def strip_of(unit):
        return pl.ds(pl.multiple_of(unit % 2 * rows, rows), rows)

    def held(unit, top_row):
        return unit // 2 * 2 + top_row, strip_of(unit)

    def both_of(unit):
        return pool.at[pl.ds(unit // 2 * 2, 2), strip_of(unit)]

    def back_core(unit):
        kept = core_back.at[slot(unit), :, strip_of(unit)]
        return remote(both_of(unit), kept, (bsem.at[0, unit], bsem.at[1, unit]), partner)

    def back_y(unit):
        kept = y_back.at[slot(unit), strip_of(unit)]
        return remote(pool.at[held(unit, 1 - y)], kept, (bsem.at[2, unit], bsem.at[3, unit]), y_next)

    def back_x(unit):
        kept = x_back.at[side_of(unit), strip_of(unit)]
        return remote(pool.at[held(unit, y)], kept, (bsem.at[4, unit], bsem.at[5, unit]), x_next)

    def keeps(unit):
        return place(unit) % 2 == c

    def owns(unit):
        return place(unit) == tp

    def passes(unit):
        return jnp.logical_and(keeps(unit), place(unit) // 2 != x)

    def add(unit, top_row, other):
        at = held(unit, top_row)
        pool[at] = (pool[at].astype(jnp.float32) + other.astype(jnp.float32)).astype(jnp.bfloat16)

    def down_part(unit):
        step, side = unit // (2 * NY), side_of(unit)
        ends = jnp.logical_or(z == 0, z == last)

        @pl.when(jnp.logical_and(jnp.logical_and(step > 0, unit % 2 == 0), ends))
        def _():
            way = jnp.where(z == 0, 1, 0)
            part = dn.at[place(unit) * NY + side]
            remote(part, part, (zs.at[way, 0, 4 + side], zr.at[way, step, 4 + side]), on_plane(z)).wait_recv()

        weight = dn[place(unit) * NY + side]
        for top_row in (1 - y, y):
            start = pl.multiple_of(top_row * tokens + unit % 2 * rows, rows)
            pool[held(unit, top_row)] = jnp.dot(
                hid[pl.ds(start, rows), :], weight, preferred_element_type=jnp.float32
            ).astype(jnp.bfloat16)

        @pl.when(jnp.logical_not(keeps(unit)))
        def _():
            back_core(unit).start()

    def after_core(unit):
        @pl.when(keeps(unit))
        def _():
            back_core(unit).wait_recv()
            for top_row in (1 - y, y):
                add(unit, top_row, core_back[slot(unit), top_row, strip_of(unit)])
            back_y(unit).start()

    def after_y(unit):
        @pl.when(keeps(unit))
        def _():
            back_y(unit).wait_recv()
            add(unit, y, y_back[slot(unit), strip_of(unit)])

        @pl.when(passes(unit))
        def _():
            back_x(unit).start()

    def after_x(unit):
        @pl.when(owns(unit))
        def _():
            back_x(unit).wait_recv()
            at = strip_of(unit)
            lanes = pl.ds(pl.multiple_of(side_of(unit) * wide, wide), wide)
            total = pool[held(unit, y)].astype(jnp.float32) + x_back[side_of(unit), at].astype(jnp.float32)
            out_ref[at, lanes] = (out_ref[at, lanes].astype(jnp.float32) + 0.5 * total).astype(out_ref.dtype)

    def run(low, high):
        @pl.loop(low, high + 1)
        def _(i):
            @pl.when(i < high)
            def _():
                down_part(i)

            @pl.when(i > low)
            def _():
                after_core(i - 1)

    def each(stage, low, high):
        @pl.loop(low, high)
        def _(i):
            stage(i)

    run(0, 8)
    each(after_y, 0, 4)
    run(8, 12)
    each(after_y, 4, 8)
    run(12, 14)
    each(after_y, 8, 12)
    run(14, units)
    each(after_y, 12, units)
    each(after_x, 0, units)

    @pl.loop(0, units)
    def _(i):
        @pl.when(jnp.logical_not(keeps(i)))
        def _():
            back_core(i).wait_send()

        @pl.when(keeps(i))
        def _():
            back_y(i).wait_send()

        @pl.when(passes(i))
        def _():
            back_x(i).wait_send()

    for chunk in range(3):
        y_weight(chunk).wait_send()
    for copy in state_y:
        copy.wait_send()
    for step in range(1, planes):

        @pl.when(z + step <= last)
        def _():
            for copy in state_z(step, z):
                copy.wait_send()

    for way in range(2):
        for dist in range(planes - 1):

            @pl.when(jnp.logical_and(has_origin(way, dist), has_next(way)))
            def _():
                for chunk in range(6):
                    z_copy(way, dist, chunk).wait_send()


def plane_layer(
    planes,
    queries,
    cell_key_rows,
    cell_value_rows,
    output_gate_logits,
    input_gate_logits,
    forget_gate_logits,
    forget_extra_term,
    residual,
    head_norm_gain,
    cell_output_weight,
    feedforward_norm_gain,
    gate_projection_weight,
    up_projection_weight,
    down_projection_weight,
):
    tokens, heads = queries.shape[0], input_gate_logits.shape[0]
    width = residual.shape[1]
    model = cell_output_weight.shape[1]
    depth, hidden = gate_projection_weight.shape
    half = hidden // NY
    dk, dv = queries.shape[1] // heads, cell_value_rows.shape[1] // heads
    bf16, f32 = jnp.bfloat16, jnp.float32
    vmem, dma = pltpu.VMEM, pltpu.SemaphoreType.DMA
    scratch = [
        vmem((depth, hidden), bf16),
        vmem((depth, hidden), bf16),
        vmem((heads * dv, model), bf16),
        vmem((8, tokens), f32),
        vmem((tokens, 8), f32),
        vmem((8, dv), f32),
        vmem((model, hidden), bf16),
        vmem((planes * NY, half, depth), bf16),
        vmem((NY * tokens, 2 * NX * width), bf16),
        vmem((NY * tokens, half), bf16),
        vmem((NY * tokens, hidden), f32),
        vmem((depth, hidden), bf16),
        vmem((tokens, heads * dv), f32),
        vmem((heads, dk, dv), f32),
        vmem((heads, dk, dv), bf16),
        vmem((heads, dk, dv), bf16),
        vmem((heads, dk, dv), bf16),
        vmem((planes - 1, heads, dk, dv), bf16),
        vmem((8, dv), f32),
        vmem((8, dv), f32),
        vmem((planes - 1, 8, dv), f32),
        vmem((planes, 8, dv), f32),
        vmem((2 * planes * NY, tokens, width // 2), bf16),
        vmem((4, tokens, width // 2), bf16),
        vmem((2, tokens, width // 2), bf16),
        vmem((planes * NY // 2, 2, tokens, width // 2), bf16),
        vmem((planes * NY // 2, tokens, width // 2), bf16),
        vmem((2, tokens, width // 2), bf16),
        dma((2, planes, 6)),
        dma((2, planes, 6)),
        dma((2, 3)),
        dma((6, planes)),
        dma((4, 4)),
        dma((14, 4)),
        dma((6, planes * NY * 2)),
        dma((12,)),
    ]
    whole = pl.BlockSpec(memory_space=pltpu.VMEM)
    far = pl.BlockSpec(memory_space=pl.ANY)
    return pl.pallas_call(
        functools.partial(block_body, planes),
        out_shape=jax.ShapeDtypeStruct((tokens, width), bf16),
        in_specs=[far] * 4 + [whole] * 3 + [far, whole, far, whole] + [far] * 3,
        out_specs=whole,
        scratch_shapes=scratch,
        compiler_params=pltpu.CompilerParams(
            collective_id=0, has_side_effects=True, vmem_limit_bytes=67043328
        ),
        cost_estimate=pl.CostEstimate(flops=22 * 10**9, bytes_accessed=10**7, transcendentals=0),
        name="block",
    )(
        queries,
        cell_key_rows,
        cell_value_rows,
        output_gate_logits,
        input_gate_logits,
        forget_gate_logits,
        forget_extra_term,
        residual,
        head_norm_gain,
        cell_output_weight,
        feedforward_norm_gain,
        gate_projection_weight,
        up_projection_weight,
        down_projection_weight,
    )


def layer(rows, columns, *arrays):
    if columns == 2 * NX and rows == 4 * NY:
        return plane_layer(rows // NY, *arrays)
    return general(*arrays)


def solution(mesh):
    placed = (
        P("sp", "tp"),
        P("sp", "tp"),
        P("sp", "tp"),
        P("sp", "tp"),
        P("tp", "sp"),
        P("tp", "sp"),
        P("tp", "sp"),
        P("sp", "tp"),
        P("tp"),
        P("tp", None),
        P(),
        P("sp", "tp"),
        P("sp", "tp"),
        P("tp", "sp"),
    )
    return jax.shard_map(
        functools.partial(layer, mesh.shape["sp"], mesh.shape["tp"]), mesh=mesh, in_specs=placed, out_specs=P("sp", "tp"), check_vma=False
    )
```

```python
import functools

import jax
import jax.numpy as jnp
from jax import lax
from jax.experimental import pallas as pl
from jax.experimental.pallas import tpu as pltpu
from jax.sharding import PartitionSpec as P

LOWEST_LOG = -1e30
EPSILON = 1e-06


def shift_pairs(length, step):
    return [(source, source + step) for source in range(length - step)]


def entering_state(state, top, total):
    length, index = lax.axis_size("sp"), lax.axis_index("sp")
    heads, key_width, value_width = state.shape

    def pack(s, t, f):
        tail = jnp.zeros((heads, 8, value_width), jnp.float32)
        tail = tail.at[:, 0, :].set(t[:, None]).at[:, 1, :].set(f[:, None])
        return jnp.concatenate([s, tail], axis=1)

    def unpack(p, valid):
        s = p[:, :key_width, :]
        t = jnp.where(valid, p[:, key_width, 0], LOWEST_LOG)
        f = jnp.where(valid, p[:, key_width + 1, 0], 0.0)
        return jnp.where(valid, s, 0.0), t, f

    moved = lax.ppermute(pack(state, top, total), "sp", shift_pairs(length, 1))
    s, t, f = unpack(moved, index >= 1)
    step = 1
    while step < length - 1:
        moved = lax.ppermute(pack(s, t, f), "sp", shift_pairs(length, step))
        s0, t0, f0 = unpack(moved, index >= step)
        from_top = t0 + f
        new_top = jnp.maximum(from_top, t)
        s = (
            jnp.exp(from_top - new_top)[:, None, None] * s0
            + jnp.exp(t - new_top)[:, None, None] * s
        )
        t, f = new_top, f0 + f
        step *= 2
    return s, t


def cell_kernel(q_ref, k_ref, v_ref, a_ref, m_ref, c_ref, state_ref, open_ref, gain_ref, o_ref, *, scale):
    block = q_ref.shape[0]
    length = k_ref.shape[0]
    q = q_ref[...]
    first = pl.program_id(1) * block
    scores = lax.dot_general(
        q, k_ref[...], (((1,), (1,)), ((), ())), preferred_element_type=jnp.float32
    )
    rows = first + lax.broadcasted_iota(jnp.int32, (block, length), 0)
    cols = lax.broadcasted_iota(jnp.int32, (block, length), 1)
    weight = jnp.where(cols <= rows, jnp.exp(jnp.minimum(a_ref[0] - m_ref[0], 0.0)), 0.0)
    numer = jnp.dot(
        (scores * weight).astype(jnp.bfloat16), v_ref[...], preferred_element_type=jnp.float32
    )
    before = jnp.dot(q, state_ref[0].astype(jnp.bfloat16), preferred_element_type=jnp.float32)
    memory = (numer + c_ref[0] * before) * scale
    normal = memory * lax.rsqrt(jnp.mean(memory * memory, axis=-1, keepdims=True) + EPSILON)
    gate_open = jax.nn.sigmoid(open_ref[...].astype(jnp.float32))
    o_ref[...] = (normal * gain_ref[...].astype(jnp.float32) * gate_open).astype(o_ref.dtype)


def cell(queries, keys, values, a_log, m_col, c_col, state, open_logits, gain):
    heads, length = a_log.shape
    dk, dv = queries.shape[1] // heads, values.shape[1] // heads
    block = min(length, 256)
    return pl.pallas_call(
        lambda *refs: cell_kernel(*refs, scale=dk ** (-0.5)),
        grid=(heads, length // block),
        in_specs=[
            pl.BlockSpec((block, dk), lambda h, i: (i, h)),
            pl.BlockSpec((length, dk), lambda h, i: (0, h)),
            pl.BlockSpec((length, dv), lambda h, i: (0, h)),
            pl.BlockSpec((1, 1, length), lambda h, i: (h, 0, 0)),
            pl.BlockSpec((1, block, 1), lambda h, i: (h, i, 0)),
            pl.BlockSpec((1, block, 1), lambda h, i: (h, i, 0)),
            pl.BlockSpec((1, dk, dv), lambda h, i: (h, 0, 0)),
            pl.BlockSpec((block, dv), lambda h, i: (i, h)),
            pl.BlockSpec((1, dv), lambda h, i: (0, h)),
        ],
        out_specs=pl.BlockSpec((block, dv), lambda h, i: (i, h)),
        out_shape=jax.ShapeDtypeStruct((length, heads * dv), jnp.bfloat16),
        cost_estimate=pl.CostEstimate(
            flops=8 * heads * length * length * dv, bytes_accessed=6 * length * heads * dv, transcendentals=0
        ),
        name="cell",
    )(queries, keys, values, a_log[:, None, :], m_col[:, :, None], c_col[:, :, None], state, open_logits, gain)


def partner_pairs(count):
    return [(i, i ^ 1) for i in range(count)]


def ring_pairs(count, step):
    return [(i, (i + 2 * step) % count) for i in range(count)]


def product_scattered(rows, weight):
    count, index = lax.axis_size("tp"), lax.axis_index("tp")
    chips, core, chip = count // 2, index % 2, index // 2
    width = weight.shape[1] // count

    def product(block):
        columns = lax.dynamic_slice_in_dim(weight, block * width, width, 1)
        return jnp.dot(rows, columns, preferred_element_type=jnp.float32)

    def chip_sum(to):
        given = product(2 * to + 1 - core).astype(jnp.bfloat16)
        got = lax.ppermute(given, "tp", partner_pairs(count))
        return product(2 * to + core) + got.astype(jnp.float32)

    moved = []
    for step in range(1, chips):
        sent = chip_sum((chip + step) % chips).astype(jnp.bfloat16)
        moved.append(lax.ppermute(sent, "tp", ring_pairs(count, step)))
    total = chip_sum(chip)
    for part in moved:
        total = total + part.astype(jnp.float32)
    return total


def columns_gathered(block):
    count, index = lax.axis_size("tp"), lax.axis_index("tp")
    chips, core, chip = count // 2, index % 2, index // 2
    width = block.shape[1]
    whole = jnp.zeros((block.shape[0], count * width), block.dtype)
    held = [(chip, block)]
    for step in range(1, chips):
        moved = lax.ppermute(block, "tp", ring_pairs(count, step))
        held.append(((chip - step) % chips, moved))
    for place, piece in held:
        other = lax.ppermute(piece, "tp", partner_pairs(count))
        whole = lax.dynamic_update_slice(whole, piece, (0, (2 * place + core) * width))
        whole = lax.dynamic_update_slice(whole, other, (0, (2 * place + 1 - core) * width))
    return whole


def general(
    queries,
    cell_key_rows,
    cell_value_rows,
    output_gate_logits,
    input_gate_logits,
    forget_gate_logits,
    forget_extra_term,
    residual,
    head_norm_gain,
    cell_output_weight,
    feedforward_norm_gain,
    gate_projection_weight,
    up_projection_weight,
    down_projection_weight,
):
    whole_gate = lax.all_gather(gate_projection_weight, "sp", axis=0, tiled=True)
    whole_up = lax.all_gather(up_projection_weight, "sp", axis=0, tiled=True)
    length = queries.shape[0]
    heads = input_gate_logits.shape[0]
    dk, dv = queries.shape[1] // heads, cell_value_rows.shape[1] // heads
    log_forget = jax.nn.log_sigmoid(forget_gate_logits.astype(jnp.float32)) + forget_extra_term
    running = jnp.cumsum(log_forget, axis=-1)
    a_log = input_gate_logits.astype(jnp.float32) - running
    m_log = lax.cummax(a_log, axis=1)
    a_top, total = m_log[:, -1], running[:, -1]
    decay = jnp.exp(a_log - a_top[:, None])
    weighed = (
        cell_key_rows.reshape(length, heads, dk).astype(jnp.float32) * decay.T[:, :, None]
    ).astype(jnp.bfloat16)
    state = jnp.stack(
        [
            lax.dot_general(
                weighed[:, h],
                cell_value_rows[:, h * dv : (h + 1) * dv],
                (((0,), (0,)), ((), ())),
                preferred_element_type=jnp.float32,
            )
            for h in range(heads)
        ]
    )
    carried, carried_top = entering_state(state, a_top + total, total)
    m_all = jnp.maximum(m_log, carried_top[:, None])
    coefficient = jnp.exp(carried_top[:, None] - m_all)
    gated = cell(
        queries,
        cell_key_rows,
        cell_value_rows,
        a_log,
        m_all,
        coefficient,
        carried,
        output_gate_logits,
        head_norm_gain[None, :],
    )
    summed = product_scattered(gated, cell_output_weight)
    stream = (residual.astype(jnp.float32) + summed).astype(jnp.bfloat16)
    down_late, stream = lax.optimization_barrier((down_projection_weight, stream))
    whole_down = lax.all_gather(down_late, "sp", axis=1, tiled=True)
    wide = columns_gathered(stream).astype(jnp.float32)
    scale = lax.rsqrt(jnp.mean(wide * wide, axis=-1, keepdims=True) + EPSILON)
    normed = (wide * scale * feedforward_norm_gain.astype(jnp.float32)[None, :]).astype(jnp.bfloat16)
    gate_value = jnp.dot(normed, whole_gate, preferred_element_type=jnp.float32)
    lifted = jnp.dot(normed, whole_up, preferred_element_type=jnp.float32)
    hidden = (jax.nn.silu(gate_value) * lifted).astype(jnp.bfloat16)
    channel_total = product_scattered(hidden, whole_down)
    return (stream.astype(jnp.float32) + 0.5 * channel_total).astype(jnp.bfloat16)


NX, NY = 2, 2
BY_NAME = pl.DeviceIdType.MESH


def block_body(
    planes,
    q_in,
    k_in,
    v_in,
    open_in,
    input_in,
    forget_in,
    extra_in,
    resid_in,
    gain_ref,
    wo_in,
    fgain_ref,
    gate_in,
    up_in,
    down_ref,
    out_ref,
    gate_ref,
    up_ref,
    wo_ref,
    a_ref,
    cols_ref,
    meta_ref,
    gu,
    dn,
    rows_all,
    hid,
    sums,
    gu_out,
    num,
    ent,
    st_own,
    st_y,
    st_sum,
    st_pre,
    st_z,
    meta_y,
    meta_sum,
    meta_pre,
    meta_z,
    lw_ref,
    pool,
    core_in,
    x_in,
    core_back,
    y_back,
    x_back,
    zs,
    zr,
    ysem,
    ssem,
    fsem,
    gsem,
    bsem,
    lsem,
):
    sp, tp = lax.axis_index("sp"), lax.axis_index("tp")
    z, y, x, c = sp // NY, sp % NY, tp // 2, tp % 2
    tokens, heads = q_in.shape[0], input_in.shape[0]
    dk, dv = q_in.shape[1] // heads, v_in.shape[1] // heads
    width = resid_in.shape[1]
    depth, hidden = gate_ref.shape
    half = hidden // NY
    count = 2 * NX
    last = planes - 1
    strip = tokens // 4
    wide = width // 2
    part_rows = depth // 2

    partner = {"tp": tp + 1 - 2 * c}
    x_next = {"tp": (1 - x) * 2 + c}
    y_next = {"sp": z * NY + 1 - y}

    def on_plane(at):
        return {"sp": at * NY + y}

    def remote(src, dst, sems, to):
        return pltpu.make_async_remote_copy(
            src_ref=src, dst_ref=dst, send_sem=sems[0], recv_sem=sems[1], device_id=to, device_id_type=BY_NAME
        )

    q_ref, k_ref = core_back.at[0, 0], core_back.at[0, 1]
    v_ref, open_ref, resid_ref = core_back.at[1], core_back.at[2], core_back.at[3]
    loads = {}
    wanted = [("gate", gate_in, gate_ref), ("up", up_in, up_ref), ("k", k_in, k_ref)]
    for name, source, kept in (("v", v_in, v_ref), ("q", q_in, q_ref), ("open", open_in, open_ref)):
        if name == "q":
            wanted.append((name, source, kept))
        else:
            for part in range(2):
                wanted.append((name + str(part), source.at[:, part * wide : (part + 1) * wide], kept.at[part]))
    wanted.append(("wo", wo_in, wo_ref))
    for part in range(2):
        wanted.append(("resid" + str(part), resid_in.at[:, part * wide : (part + 1) * wide], resid_ref.at[part]))
    for index, (name, source, kept) in enumerate(wanted):
        loads[name] = pltpu.make_async_copy(source, kept, lsem.at[index + 1])
        loads[name].start()

    barrier = pltpu.get_barrier_semaphore()
    for to in (partner, x_next, y_next):
        pl.semaphore_signal(barrier, inc=1, device_id=to, device_id_type=BY_NAME)
    for ok, at in ((z > 0, z - 1), (z < last, z + 1)):

        @pl.when(ok)
        def _():
            pl.semaphore_signal(barrier, inc=1, device_id=on_plane(at), device_id_type=BY_NAME)

    ends = jnp.logical_or(z == 0, z == last)
    pl.semaphore_wait(barrier, 5 - jnp.where(ends, 1, 0))

    loads["gate"].wait()
    loads["up"].wait()

    for mine in range(NY):

        @pl.when(y == mine)
        def _():
            own = pl.ds(pl.multiple_of(sp * depth, depth), depth)
            here, there = mine * half, (1 - mine) * half
            gu_out[:, 0:half] = gate_ref[:, there : there + half]
            gu_out[:, half : 2 * half] = up_ref[:, there : there + half]
            gu[own, 0:half] = gate_ref[:, here : here + half]
            gu[own, half : 2 * half] = up_ref[:, here : here + half]

    def gu_rows(at, chunk):
        side = (y + chunk // 2) % 2
        start = (at * NY + side) * depth + (chunk % 2) * part_rows
        return pl.ds(pl.multiple_of(start, part_rows), part_rows)

    def z_copy(way, dist, chunk):
        at = z - dist if way == 0 else z + dist
        to = z + 1 if way == 0 else z - 1
        sems = (zs.at[way, dist, chunk], zr.at[way, dist, chunk])
        if chunk < 4:
            part = gu.at[gu_rows(at, chunk), :]
        else:
            part = dn.at[at * NY + chunk - 4]
        return remote(part, part, sems, on_plane(to))

    def z_arrival(way, dist, chunk):
        at = z - dist if way == 0 else z + dist
        sems = (zs.at[way, 0, chunk], zr.at[way, dist - 1, chunk])
        if chunk < 4:
            part = gu.at[gu_rows(at, chunk), :]
        else:
            part = dn.at[at * NY + chunk - 4]
        return remote(part, part, sems, on_plane(z))

    def has_next(way):
        return z < last if way == 0 else z > 0

    def has_origin(way, dist):
        return z >= dist if way == 0 else z + dist <= last

    def z_send(chunk, ways=((0, True), (1, True))):
        for way, also in ways:

            @pl.when(jnp.logical_and(has_next(way), also))
            def _():
                z_copy(way, 0, chunk).start()

    def z_forward(dist, chunk):
        for way in range(2):

            @pl.when(jnp.logical_and(has_origin(way, dist), has_next(way)))
            def _():
                z_arrival(way, dist, chunk).wait_recv()
                z_copy(way, dist, chunk).start()

    def z_down(rank, dist):
        for way in range(2):

            @pl.when(z == (rank if way == 0 else last - rank))
            def _():
                for chunk in (4, 5):
                    if dist:
                        z_arrival(way, dist, chunk).wait_recv()
                    z_copy(way, dist, chunk).start()

    def y_rows(owner, chunk):
        start = (z * NY + owner) * depth + chunk * part_rows
        return pl.ds(pl.multiple_of(start, part_rows), part_rows)

    def y_weight(chunk):
        sems = (ysem.at[0, chunk], ysem.at[1, chunk])
        if chunk < 2:
            return remote(
                gu_out.at[pl.ds(chunk * part_rows, part_rows), :], gu.at[y_rows(y, chunk), :], sems, y_next
            )
        start = pl.multiple_of((1 - y) * half, half)
        return remote(down_ref.at[pl.ds(start, half), :], dn.at[sp], sems, y_next)

    own_down = pltpu.make_async_copy(
        down_ref.at[pl.ds(pl.multiple_of(y * half, half), half), :], dn.at[sp], lsem.at[0]
    )
    z_send(0)

    def padded(rows):
        return jnp.concatenate([rows, jnp.zeros((8 - heads, tokens), jnp.float32)], axis=0)

    lane = lax.broadcasted_iota(jnp.int32, (8, tokens), 1)
    logits = forget_in[...].astype(jnp.float32)
    running = padded(
        jnp.minimum(logits, 0.0) - jnp.log1p(jnp.exp(-jnp.abs(logits))) + extra_in[...]
    )
    step = 1
    while step < tokens:
        running = running + jnp.where(lane >= step, pltpu.roll(running, step, 1), 0.0)
        step *= 2
    a_log = padded(input_in[...].astype(jnp.float32)) - running
    m_log = a_log
    step = 1
    while step < tokens:
        m_log = jnp.maximum(m_log, jnp.where(lane >= step, pltpu.roll(m_log, step, 1), LOWEST_LOG))
        step *= 2
    a_ref[...] = a_log
    a_top, total = m_log[:, tokens - 1 :], running[:, tokens - 1 :]
    decay = jnp.exp(a_log - a_top)
    cols_ref[...] = jnp.concatenate(
        [decay[0:heads], m_log[0:heads], jnp.zeros((8 - 2 * heads, tokens), jnp.float32)], axis=0
    ).T
    meta_ref[...] = jnp.zeros_like(meta_ref)
    meta_ref[0:heads, :] = jnp.broadcast_to((a_top + total)[0:heads], (heads, meta_ref.shape[1]))
    meta_ref[heads : 2 * heads, :] = jnp.broadcast_to(total[0:heads], (heads, meta_ref.shape[1]))
    for name in ("k", "v0", "v1"):
        loads[name].wait()

    for h in range(heads):
        weighed = (
            k_ref[:, h * dk : (h + 1) * dk].astype(jnp.float32) * cols_ref[:, h : h + 1]
        ).astype(jnp.bfloat16)
        st_own[h] = lax.dot_general(
            weighed,
            v_ref[h],
            (((0,), (0,)), ((), ())),
            preferred_element_type=jnp.float32,
        ).astype(jnp.bfloat16)

    state_y = [
        remote(st_own, st_y, (ssem.at[0], ssem.at[1]), y_next),
        remote(meta_ref, meta_y, (ssem.at[2], ssem.at[3]), y_next),
    ]
    for copy in state_y:
        copy.start()
    for chunk in range(3):
        y_weight(chunk).start()
    own_down.start()
    loads["q"].wait()

    def attend(h, i):
        span = (i + 1) * strip
        at = pl.ds(i * strip, strip)
        scores = lax.dot_general(
            q_ref[at, h * dk : (h + 1) * dk],
            k_ref[0:span, h * dk : (h + 1) * dk],
            (((1,), (1,)), ((), ())),
            preferred_element_type=jnp.float32,
        )
        log_weight = a_ref[h : h + 1, 0:span] - cols_ref[at, heads + h : heads + h + 1]
        row = i * strip + lax.broadcasted_iota(jnp.int32, (strip, span), 0)
        col = lax.broadcasted_iota(jnp.int32, (strip, span), 1)
        weight = jnp.where(col <= row, jnp.exp(jnp.minimum(log_weight, 0.0)), 0.0)
        num[at, h * dv : (h + 1) * dv] = jnp.dot(
            (scores * weight).astype(jnp.bfloat16),
            v_ref[h, 0:span, :],
            preferred_element_type=jnp.float32,
        )

    for h in range(heads):
        attend(h, 0)

    for copy in state_y:
        copy.wait_recv()
    first = y == 0
    meta_own, meta_other = meta_ref[...], meta_y[...]
    meta_0 = jnp.where(first, meta_own, meta_other)
    meta_1 = jnp.where(first, meta_other, meta_own)
    top_0 = meta_0[0:heads] + meta_1[heads : 2 * heads]
    top_1 = meta_1[0:heads]
    top = jnp.maximum(top_0, top_1)
    scale_0, scale_1 = jnp.exp(top_0 - top), jnp.exp(top_1 - top)
    scale_own = jnp.where(first, scale_0, scale_1)
    scale_other = jnp.where(first, scale_1, scale_0)
    meta_sum[...] = jnp.zeros_like(meta_sum)
    meta_sum[0:heads, :] = top
    meta_sum[heads : 2 * heads, :] = meta_0[heads : 2 * heads] + meta_1[heads : 2 * heads]
    for h in range(heads):
        st_sum[h] = (
            st_own[h].astype(jnp.float32) * scale_own[h : h + 1]
            + st_y[h].astype(jnp.float32) * scale_other[h : h + 1]
        ).astype(jnp.bfloat16)

    def state_z(step, summed):
        state, meta = (st_pre, meta_pre) if summed else (st_sum, meta_sum)
        to = on_plane(z + step)
        return [
            remote(state, st_z, (ssem.at[4], ssem.at[5]), to),
            remote(meta, meta_z, (ssem.at[6], ssem.at[7]), to),
        ]

    @pl.when(z == 0)
    def _():
        for copy in state_z(1, 0):
            copy.start()

    def hop():
        for copy in state_z(0, 0):
            copy.wait_recv()
        before, own = meta_z[0:heads, :] + meta_sum[heads : 2 * heads, :], meta_sum[0:heads, :]
        joint = jnp.maximum(before, own)
        meta_pre[...] = jnp.zeros_like(meta_pre)
        meta_pre[0:heads, :] = joint
        meta_pre[heads : 2 * heads, :] = meta_z[heads : 2 * heads, :] + meta_sum[heads : 2 * heads, :]
        scale_before, scale_own = jnp.exp(before - joint), jnp.exp(own - joint)
        for h in range(heads):
            st_pre[h] = (
                st_z[h].astype(jnp.float32) * scale_before[h : h + 1]
                + st_sum[h].astype(jnp.float32) * scale_own[h : h + 1]
            ).astype(jnp.bfloat16)
        for copy in state_z(1, 1):
            copy.start()

    z_send(1, ((0, z != 1), (1, True)))
    for h in range(heads):
        for i in range(1, 4):
            attend(h, i)

    pl.when(z == 1)(hop)
    z_send(1, ((0, z == 1),))

    def z_half(part):
        short_part = part_rows // 2
        start = pl.multiple_of((z * NY + 1 - y) * depth + part * short_part, short_part)
        piece = gu.at[pl.ds(start, short_part), :]
        return remote(piece, piece, (zs.at[0, 0, 2], zr.at[0, 0, 2]), on_plane(z + 1))

    y_weight(0).wait_recv()
    z_send(2, ((0, z < 2), (1, True)))

    @pl.when(z == 2)
    def _():
        z_half(0).start()
        hop()
        z_half(1).start()

    low = jnp.full((heads, meta_ref.shape[1]), LOWEST_LOG, jnp.float32)
    later = jnp.where(y == 1, meta_y[heads : 2 * heads, :], 0.0)
    lw_ref[1, 0:heads, :] = jnp.where(y == 1, meta_y[0:heads, :], low)

    @pl.when(z == last)
    def _():
        for copy in state_z(0, 0):
            copy.wait_recv()

    lw_ref[0, 0:heads, :] = jnp.where(z > 0, meta_z[0:heads, :] + later, low)
    ctop = jnp.maximum(lw_ref[0, 0:heads, :], lw_ref[1, 0:heads, :])
    ent[...] = jnp.zeros_like(ent)
    for source, valid in ((0, z > 0), (1, y == 1)):

        @pl.when(valid)
        def _():
            scale = jnp.exp(lw_ref[source, 0:heads, :] - ctop)
            for h in range(heads):
                part = st_y[h] if source else st_z[h]
                ent[h] += part.astype(jnp.float32) * scale[h : h + 1]

    for name in ("open0", "open1", "wo"):
        loads[name].wait()

    def front_core(i):
        at = pl.ds(pl.multiple_of(i * strip, strip), strip)
        return remote(
            pool.at[0:4, at, :], core_in.at[:, at, :], (fsem.at[0, i], fsem.at[1, i]), partner
        )

    def front_x(i):
        at = pl.ds(pl.multiple_of(i * strip, strip), strip)
        return remote(
            pool.at[8:10, at, :], x_in.at[:, at, :], (fsem.at[2, i], fsem.at[3, i]), x_next
        )

    def gate_strip(i):
        at = pl.ds(pl.multiple_of(i * strip, strip), strip)
        gated = []
        for h in range(heads):
            lanes = slice(h * dv, (h + 1) * dv)
            before = jnp.dot(
                q_ref[at, h * dk : (h + 1) * dk],
                ent[h].astype(jnp.bfloat16),
                preferred_element_type=jnp.float32,
            )
            m_log = cols_ref[at, heads + h : heads + h + 1]
            m_all = jnp.maximum(m_log, ctop[h : h + 1, 0:1])
            memory = (
                num[at, lanes] * jnp.exp(m_log - m_all)
                + jnp.exp(ctop[h : h + 1, 0:1] - m_all) * before
            ) * dk ** (-0.5)
            normal = memory * lax.rsqrt(jnp.mean(memory * memory, axis=-1, keepdims=True) + EPSILON)
            opened = jax.nn.sigmoid(open_ref[h, at, :].astype(jnp.float32))
            gated.append((normal * gain_ref[lanes][None, :].astype(jnp.float32) * opened).astype(jnp.bfloat16))
        gated = jnp.concatenate(gated, axis=1)
        for chip in range(NX):
            for part in range(2):
                for mine in range(2):
                    core = c if mine else 1 - c
                    lanes = pl.ds(
                        pl.multiple_of((chip * 2 + core) * width + part * wide, wide), wide
                    )
                    pool[mine * 4 + chip * 2 + part, at, :] = jnp.dot(
                        gated, wo_ref[:, lanes], preferred_element_type=jnp.float32
                    ).astype(jnp.bfloat16)
        front_core(i).start()

    def core_sum(i):
        at = pl.ds(pl.multiple_of(i * strip, strip), strip)
        front_core(i).wait_recv()
        for part in range(2):
            far, near = (1 - x) * 2 + part, x * 2 + part
            pool[8 + part, at, :] = (
                pool[4 + far, at, :].astype(jnp.float32) + core_in[far, at, :].astype(jnp.float32)
            ).astype(jnp.bfloat16)
        front_x(i).start()

    @pl.loop(0, 5)
    def _(i):
        @pl.when(i < 4)
        def _():
            gate_strip(i)

        @pl.when(i == 2)
        def _():
            y_weight(1).wait_recv()
            z_send(3)

        @pl.when(i >= 1)
        def _():
            core_sum(i - 1)

    z_forward(1, 0)
    z_forward(1, 1)
    y_weight(2).wait_recv()
    own_down.wait()
    z_down(0, 0)
    for part in range(2):
        loads["resid" + str(part)].wait()

    def piece(owner_x, owner_c, owner_y, i):
        at = pl.multiple_of(owner_y * tokens + i * strip, strip)
        lanes = pl.multiple_of((owner_x * 2 + owner_c) * width, width)
        return rows_all.at[pl.ds(at, strip), pl.ds(lanes, width)]

    def to_x(i):
        part = piece(x, c, y, i)
        return remote(part, part, (gsem.at[0, i], gsem.at[1, i]), x_next)

    def to_y(kind, i):
        part = piece(x if kind == 0 else 1 - x, c, y, i)
        return remote(part, part, (gsem.at[2 + kind, i], gsem.at[4 + kind, i]), y_next)

    def to_core(kind, i):
        part = piece(
            x if kind % 2 == 0 else 1 - x, c, y if kind // 2 == 0 else 1 - y, i
        )
        return remote(part, part, (gsem.at[6 + kind, i], gsem.at[10 + kind, i]), partner)

    @pl.loop(0, 4)
    def _(i):
        at = pl.ds(pl.multiple_of(i * strip, strip), strip)
        front_x(i).wait_recv()
        start = pl.multiple_of(y * tokens + i * strip, strip)
        for part in range(2):
            lanes = slice(part * wide, (part + 1) * wide)
            near = x * 2 + part
            total = (
                pool[4 + near, at, :].astype(jnp.float32)
                + core_in[near, at, :].astype(jnp.float32)
                + x_in[part, at, :].astype(jnp.float32)
            )
            fresh = (resid_ref[part, at, :].astype(jnp.float32) + total).astype(jnp.bfloat16)
            out_ref[at, lanes] = fresh
            columns = pl.ds(pl.multiple_of(tp * width + part * wide, wide), wide)
            rows_all[pl.ds(start, strip), columns] = fresh
        to_x(i).start()
        to_y(0, i).start()
        to_core(0, i).start()

        @pl.when(i == 1)
        def _():
            z_forward(1, 2)

    z_forward(1, 3)
    z_down(1, 0)

    @pl.loop(0, 4)
    def _(i):
        to_x(i).wait_recv()
        to_y(1, i).start()
        to_core(1, i).start()
        to_y(0, i).wait_recv()
        to_core(2, i).start()

        @pl.when(i == 1)
        def _():
            z_forward(2, 0)
            z_forward(2, 1)

    z_forward(2, 2)
    z_down(1, 1)

    short = 128

    def norm_rows(owner, kinds):
        @pl.loop(0, 4)
        def _(i):
            for kind in kinds:
                to_core(kind, i).wait_recv()

        @pl.loop(0, tokens // short)
        def _(i):
            at = pl.ds(pl.multiple_of(owner * tokens + i * short, short), short)
            wide_rows = rows_all[at, :].astype(jnp.float32)
            scale = lax.rsqrt(jnp.mean(wide_rows * wide_rows, axis=-1, keepdims=True) + EPSILON)
            rows_all[at, :] = (wide_rows * scale * fgain_ref[...][None, :].astype(jnp.float32)).astype(
                jnp.bfloat16
            )

    @pl.loop(0, 4)
    def _(i):
        to_y(1, i).wait_recv()
        to_core(3, i).start()

    z_forward(2, 3)
    z_down(2, 0)

    @pl.loop(0, 4)
    def _(i):
        for copy in (front_core(i), front_x(i), to_x(i), to_y(0, i), to_y(1, i)):
            copy.wait_send()
        for kind in range(4):
            to_core(kind, i).wait_send()

    norm_rows(y, (0, 1))
    norm_rows(1 - y, (2, 3))

    tall = 512
    plane_rows = NY * depth
    early = last * plane_rows
    early_at = jnp.where(z == last, plane_rows, 0)
    late_at = jnp.where(z == last, 0, early)

    def gate_up(i, start, size):
        at = pl.ds(pl.multiple_of(i * tall, tall), tall)
        taken = pl.ds(pl.multiple_of(start, plane_rows), size)
        return at, jnp.dot(rows_all[at, taken], gu[taken, :], preferred_element_type=jnp.float32)

    def gu_arrived(dist):
        for way in range(2):

            @pl.when(jnp.logical_and(has_origin(way, dist), jnp.logical_not(has_next(way))))
            def _():
                for chunk in range(4):
                    z_arrival(way, dist, chunk).wait_recv()

    for dist in range(1, last):
        gu_arrived(dist)

    @pl.loop(0, NY * tokens // tall)
    def _(i):
        at, product = gate_up(i, early_at, early)
        sums[at, :] = product

    gu_arrived(last)

    @pl.loop(0, NY * tokens // tall)
    def _(i):
        at, product = gate_up(i, late_at, plane_rows)
        both = sums[at, :] + product
        hid[at, :] = (jax.nn.silu(both[:, :half]) * both[:, half:]).astype(jnp.bfloat16)

    z_down(2, 1)
    z_down(2, 2)

    units = planes * NY * 2
    rows = tokens // 2

    def side_of(unit):
        return unit // 2 % NY

    def place(unit):
        step = unit // (2 * NY)
        base = jnp.where(jnp.logical_or(z == 0, z == last), step, (step + 1) % planes)
        return jnp.where(z < planes // 2, base, last - base)

    def across(unit):
        group = unit // 2
        return jnp.logical_or(group == 1, group == 4)

    def along(unit):
        return jnp.logical_not(across(unit))

    def slot(unit):
        return unit // 8 * 2 + side_of(unit)

    def kept_index(unit):
        return slot(unit) * 2 + unit % 2

    def strip_of(unit):
        return pl.ds(pl.multiple_of(unit % 2 * rows, rows), rows)

    def held(unit, top_row):
        return unit // 2 * 2 + top_row, strip_of(unit)

    def both_of(unit):
        return pool.at[pl.ds(unit // 2 * 2, 2), strip_of(unit)]

    def back_core(unit):
        kept = core_back.at[slot(unit), :, strip_of(unit)]
        return remote(both_of(unit), kept, (bsem.at[0, kept_index(unit)], bsem.at[1, kept_index(unit)]), partner)

    def back_y(unit):
        kept = y_back.at[slot(unit), strip_of(unit)]
        return remote(pool.at[held(unit, 1 - y)], kept, (bsem.at[2, kept_index(unit)], bsem.at[3, kept_index(unit)]), y_next)

    def back_x(unit):
        kept = x_back.at[side_of(unit), y, strip_of(unit)]
        return remote(pool.at[held(unit, y)], kept, (bsem.at[4, unit % 4], bsem.at[4, 4 + unit % 4]), x_next)

    def back_xx(unit):
        kept = x_back.at[side_of(unit), :, strip_of(unit)]
        return remote(both_of(unit), kept, (bsem.at[4, unit % 4], bsem.at[4, 4 + unit % 4]), x_next)

    def keeps(unit):
        return place(unit) % 2 == c

    def owns(unit):
        return place(unit) == tp

    def passes(unit):
        return jnp.logical_and(keeps(unit), place(unit) // 2 != x)

    def add(unit, top_row, other):
        at = held(unit, top_row)
        pool[at] = (pool[at].astype(jnp.float32) + other.astype(jnp.float32)).astype(jnp.bfloat16)

    def down_part(unit):
        step, side = unit // (2 * NY), side_of(unit)
        ends = jnp.logical_or(z == 0, z == last)

        @pl.when(jnp.logical_and(jnp.logical_and(step > 0, unit % 2 == 0), ends))
        def _():
            way = jnp.where(z == 0, 1, 0)
            part = dn.at[place(unit) * NY + side]
            remote(part, part, (zs.at[way, 0, 4 + side], zr.at[way, step - 1, 4 + side]), on_plane(z)).wait_recv()

        weight = dn[place(unit) * NY + side]
        for top_row in (1 - y, y):
            start = pl.multiple_of(top_row * tokens + unit % 2 * rows, rows)
            pool[held(unit, top_row)] = jnp.dot(
                hid[pl.ds(start, rows), :], weight, preferred_element_type=jnp.float32
            ).astype(jnp.bfloat16)

        @pl.when(jnp.logical_not(keeps(unit)))
        def _():
            back_core(unit).start()

    def after_core(unit):
        @pl.when(keeps(unit))
        def _():
            back_core(unit).wait_recv()
            for top_row in (1 - y, y):
                add(unit, top_row, core_back[slot(unit), top_row, strip_of(unit)])

        @pl.when(jnp.logical_and(keeps(unit), along(unit)))
        def _():
            back_y(unit).start()

        @pl.when(jnp.logical_and(passes(unit), across(unit)))
        def _():
            back_xx(unit).start()

    def after_xx(unit):
        @pl.when(owns(unit))
        def _():
            back_xx(unit).wait_recv()
            for top_row in (1 - y, y):
                add(unit, top_row, x_back[side_of(unit), top_row, strip_of(unit)])
            back_y(unit).start()

    def after_y(unit):
        @pl.when(keeps(unit))
        def _():
            back_y(unit).wait_recv()
            add(unit, y, y_back[slot(unit), strip_of(unit)])

        @pl.when(passes(unit))
        def _():
            back_x(unit).start()

    def finish(unit, other):
        at = strip_of(unit)
        lanes = pl.ds(pl.multiple_of(side_of(unit) * wide, wide), wide)
        total = pool[held(unit, y)].astype(jnp.float32) + other.astype(jnp.float32)
        out_ref[at, lanes] = (out_ref[at, lanes].astype(jnp.float32) + 0.5 * total).astype(out_ref.dtype)

    def after_all(unit):
        @pl.when(jnp.logical_and(owns(unit), along(unit)))
        def _():
            back_x(unit).wait_recv()
            finish(unit, x_back[side_of(unit), y, strip_of(unit)])

        @pl.when(jnp.logical_and(owns(unit), across(unit)))
        def _():
            back_y(unit).wait_recv()
            finish(unit, y_back[slot(unit), strip_of(unit)])

    def run(low, high):
        @pl.loop(low, high + 1)
        def _(i):
            @pl.when(i < high)
            def _():
                down_part(i)

            @pl.when(i > low)
            def _():
                after_core(i - 1)

    def each(stage, low, high):
        @pl.loop(low, high)
        def _(i):
            stage(i)


    def at_ends(low, high):
        @pl.when(ends)
        def _():
            run(low, high)

    run(0, 8)

    @pl.when(jnp.logical_not(ends))
    def _():
        run(8, units)

    each(after_y, 0, 2)
    each(after_xx, 2, 4)
    at_ends(8, 10)
    each(after_y, 4, 8)
    at_ends(10, 12)
    each(after_xx, 8, 9)
    at_ends(12, 14)
    each(after_y, 10, 12)
    at_ends(14, units)
    each(after_xx, 9, 10)
    each(after_y, 12, units)
    each(after_all, 0, units)

    @pl.loop(0, units)
    def _(i):
        @pl.when(jnp.logical_not(keeps(i)))
        def _():
            back_core(i).wait_send()

        @pl.when(jnp.logical_and(keeps(i), jnp.logical_or(along(i), owns(i))))
        def _():
            back_y(i).wait_send()

        @pl.when(jnp.logical_and(passes(i), along(i)))
        def _():
            back_x(i).wait_send()

        @pl.when(jnp.logical_and(passes(i), across(i)))
        def _():
            back_xx(i).wait_send()

    for chunk in range(3):
        y_weight(chunk).wait_send()
    for copy in state_y:
        copy.wait_send()
    @pl.when(z == 0)
    def _():
        for copy in state_z(1, 0):
            copy.wait_send()

    @pl.when(jnp.logical_and(z > 0, z < last))
    def _():
        for copy in state_z(1, 1):
            copy.wait_send()

    for way in range(2):
        for dist in range(planes - 1):

            @pl.when(jnp.logical_and(has_origin(way, dist), has_next(way)))
            def _():
                for chunk in range(6):
                    z_copy(way, dist, chunk).wait_send()


def plane_layer(
    planes,
    queries,
    cell_key_rows,
    cell_value_rows,
    output_gate_logits,
    input_gate_logits,
    forget_gate_logits,
    forget_extra_term,
    residual,
    head_norm_gain,
    cell_output_weight,
    feedforward_norm_gain,
    gate_projection_weight,
    up_projection_weight,
    down_projection_weight,
):
    tokens, heads = queries.shape[0], input_gate_logits.shape[0]
    width = residual.shape[1]
    model = cell_output_weight.shape[1]
    depth, hidden = gate_projection_weight.shape
    half = hidden // NY
    dk, dv = queries.shape[1] // heads, cell_value_rows.shape[1] // heads
    bf16, f32 = jnp.bfloat16, jnp.float32
    vmem, dma = pltpu.VMEM, pltpu.SemaphoreType.DMA
    scratch = [
        vmem((depth, hidden), bf16),
        vmem((depth, hidden), bf16),
        vmem((heads * dv, model), bf16),
        vmem((8, tokens), f32),
        vmem((tokens, 8), f32),
        vmem((8, dv), f32),
        vmem((model, hidden), bf16),
        vmem((planes * NY, half, depth), bf16),
        vmem((NY * tokens, 2 * NX * width), bf16),
        vmem((NY * tokens, half), bf16),
        vmem((NY * tokens, hidden), f32),
        vmem((depth, hidden), bf16),
        vmem((tokens, heads * dv), f32),
        vmem((heads, dk, dv), f32),
        vmem((heads, dk, dv), bf16),
        vmem((heads, dk, dv), bf16),
        vmem((heads, dk, dv), bf16),
        vmem((heads, dk, dv), bf16),
        vmem((heads, dk, dv), bf16),
        vmem((8, dv), f32),
        vmem((8, dv), f32),
        vmem((8, dv), f32),
        vmem((8, dv), f32),
        vmem((2, 8, dv), f32),
        vmem((2 * planes * NY, tokens, width // 2), bf16),
        vmem((4, tokens, width // 2), bf16),
        vmem((2, tokens, width // 2), bf16),
        vmem((planes * NY // 2, 2, tokens, width // 2), bf16),
        vmem((planes * NY // 2, tokens, width // 2), bf16),
        vmem((2, 2, tokens, width // 2), bf16),
        dma((2, planes - 1, 6)),
        dma((2, planes - 1, 6)),
        dma((2, 3)),
        dma((8,)),
        dma((4, 4)),
        dma((14, 4)),
        dma((5, planes * NY)),
        dma((12,)),
    ]
    whole = pl.BlockSpec(memory_space=pltpu.VMEM)
    far = pl.BlockSpec(memory_space=pl.ANY)
    return pl.pallas_call(
        functools.partial(block_body, planes),
        out_shape=pltpu.VMEM((tokens, width), bf16),
        in_specs=[far] * 4 + [whole] * 3 + [far, whole, far, whole] + [far] * 3,
        out_specs=whole,
        scratch_shapes=scratch,
        compiler_params=pltpu.CompilerParams(
            collective_id=0, has_side_effects=True, vmem_limit_bytes=65000000
        ),
        cost_estimate=pl.CostEstimate(flops=22 * 10**9, bytes_accessed=10**7, transcendentals=0),
        name="block",
    )(
        queries,
        cell_key_rows,
        cell_value_rows,
        output_gate_logits,
        input_gate_logits,
        forget_gate_logits,
        forget_extra_term,
        residual,
        head_norm_gain,
        cell_output_weight,
        feedforward_norm_gain,
        gate_projection_weight,
        up_projection_weight,
        down_projection_weight,
    )


def layer(rows, columns, *arrays):
    if columns == 2 * NX and rows == 4 * NY:
        return plane_layer(rows // NY, *arrays)
    return general(*arrays)


def solution(mesh):
    placed = (
        P("sp", "tp"),
        P("sp", "tp"),
        P("sp", "tp"),
        P("sp", "tp"),
        P("tp", "sp"),
        P("tp", "sp"),
        P("tp", "sp"),
        P("sp", "tp"),
        P("tp"),
        P("tp", None),
        P(),
        P("sp", "tp"),
        P("sp", "tp"),
        P("tp", "sp"),
    )
    return jax.shard_map(
        functools.partial(layer, mesh.shape["sp"], mesh.shape["tp"]), mesh=mesh, in_specs=placed, out_specs=P("sp", "tp"), check_vma=False
    )
```

```python
import functools

import jax
import jax.numpy as jnp
from jax import lax
from jax.experimental import pallas as pl
from jax.experimental.pallas import tpu as pltpu
from jax.sharding import PartitionSpec as P

LOWEST_LOG = -1e30
EPSILON = 1e-06


def shift_pairs(length, step):
    return [(source, source + step) for source in range(length - step)]


def entering_state(state, top, total):
    length, index = lax.axis_size("sp"), lax.axis_index("sp")
    heads, key_width, value_width = state.shape

    def pack(s, t, f):
        tail = jnp.zeros((heads, 8, value_width), jnp.float32)
        tail = tail.at[:, 0, :].set(t[:, None]).at[:, 1, :].set(f[:, None])
        return jnp.concatenate([s, tail], axis=1)

    def unpack(p, valid):
        s = p[:, :key_width, :]
        t = jnp.where(valid, p[:, key_width, 0], LOWEST_LOG)
        f = jnp.where(valid, p[:, key_width + 1, 0], 0.0)
        return jnp.where(valid, s, 0.0), t, f

    moved = lax.ppermute(pack(state, top, total), "sp", shift_pairs(length, 1))
    s, t, f = unpack(moved, index >= 1)
    step = 1
    while step < length - 1:
        moved = lax.ppermute(pack(s, t, f), "sp", shift_pairs(length, step))
        s0, t0, f0 = unpack(moved, index >= step)
        from_top = t0 + f
        new_top = jnp.maximum(from_top, t)
        s = (
            jnp.exp(from_top - new_top)[:, None, None] * s0
            + jnp.exp(t - new_top)[:, None, None] * s
        )
        t, f = new_top, f0 + f
        step *= 2
    return s, t


def cell_kernel(q_ref, k_ref, v_ref, a_ref, m_ref, c_ref, state_ref, open_ref, gain_ref, o_ref, *, scale):
    block = q_ref.shape[0]
    length = k_ref.shape[0]
    q = q_ref[...]
    first = pl.program_id(1) * block
    scores = lax.dot_general(
        q, k_ref[...], (((1,), (1,)), ((), ())), preferred_element_type=jnp.float32
    )
    rows = first + lax.broadcasted_iota(jnp.int32, (block, length), 0)
    cols = lax.broadcasted_iota(jnp.int32, (block, length), 1)
    weight = jnp.where(cols <= rows, jnp.exp(jnp.minimum(a_ref[0] - m_ref[0], 0.0)), 0.0)
    numer = jnp.dot(
        (scores * weight).astype(jnp.bfloat16), v_ref[...], preferred_element_type=jnp.float32
    )
    before = jnp.dot(q, state_ref[0].astype(jnp.bfloat16), preferred_element_type=jnp.float32)
    memory = (numer + c_ref[0] * before) * scale
    normal = memory * lax.rsqrt(jnp.mean(memory * memory, axis=-1, keepdims=True) + EPSILON)
    gate_open = jax.nn.sigmoid(open_ref[...].astype(jnp.float32))
    o_ref[...] = (normal * gain_ref[...].astype(jnp.float32) * gate_open).astype(o_ref.dtype)


def cell(queries, keys, values, a_log, m_col, c_col, state, open_logits, gain):
    heads, length = a_log.shape
    dk, dv = queries.shape[1] // heads, values.shape[1] // heads
    block = min(length, 256)
    return pl.pallas_call(
        lambda *refs: cell_kernel(*refs, scale=dk ** (-0.5)),
        grid=(heads, length // block),
        in_specs=[
            pl.BlockSpec((block, dk), lambda h, i: (i, h)),
            pl.BlockSpec((length, dk), lambda h, i: (0, h)),
            pl.BlockSpec((length, dv), lambda h, i: (0, h)),
            pl.BlockSpec((1, 1, length), lambda h, i: (h, 0, 0)),
            pl.BlockSpec((1, block, 1), lambda h, i: (h, i, 0)),
            pl.BlockSpec((1, block, 1), lambda h, i: (h, i, 0)),
            pl.BlockSpec((1, dk, dv), lambda h, i: (h, 0, 0)),
            pl.BlockSpec((block, dv), lambda h, i: (i, h)),
            pl.BlockSpec((1, dv), lambda h, i: (0, h)),
        ],
        out_specs=pl.BlockSpec((block, dv), lambda h, i: (i, h)),
        out_shape=jax.ShapeDtypeStruct((length, heads * dv), jnp.bfloat16),
        cost_estimate=pl.CostEstimate(
            flops=8 * heads * length * length * dv, bytes_accessed=6 * length * heads * dv, transcendentals=0
        ),
        name="cell",
    )(queries, keys, values, a_log[:, None, :], m_col[:, :, None], c_col[:, :, None], state, open_logits, gain)


def partner_pairs(count):
    return [(i, i ^ 1) for i in range(count)]


def ring_pairs(count, step):
    return [(i, (i + 2 * step) % count) for i in range(count)]


def product_scattered(rows, weight):
    count, index = lax.axis_size("tp"), lax.axis_index("tp")
    chips, core, chip = count // 2, index % 2, index // 2
    width = weight.shape[1] // count

    def product(block):
        columns = lax.dynamic_slice_in_dim(weight, block * width, width, 1)
        return jnp.dot(rows, columns, preferred_element_type=jnp.float32)

    def chip_sum(to):
        given = product(2 * to + 1 - core).astype(jnp.bfloat16)
        got = lax.ppermute(given, "tp", partner_pairs(count))
        return product(2 * to + core) + got.astype(jnp.float32)

    moved = []
    for step in range(1, chips):
        sent = chip_sum((chip + step) % chips).astype(jnp.bfloat16)
        moved.append(lax.ppermute(sent, "tp", ring_pairs(count, step)))
    total = chip_sum(chip)
    for part in moved:
        total = total + part.astype(jnp.float32)
    return total


def columns_gathered(block):
    count, index = lax.axis_size("tp"), lax.axis_index("tp")
    chips, core, chip = count // 2, index % 2, index // 2
    width = block.shape[1]
    whole = jnp.zeros((block.shape[0], count * width), block.dtype)
    held = [(chip, block)]
    for step in range(1, chips):
        moved = lax.ppermute(block, "tp", ring_pairs(count, step))
        held.append(((chip - step) % chips, moved))
    for place, piece in held:
        other = lax.ppermute(piece, "tp", partner_pairs(count))
        whole = lax.dynamic_update_slice(whole, piece, (0, (2 * place + core) * width))
        whole = lax.dynamic_update_slice(whole, other, (0, (2 * place + 1 - core) * width))
    return whole


def general(
    queries,
    cell_key_rows,
    cell_value_rows,
    output_gate_logits,
    input_gate_logits,
    forget_gate_logits,
    forget_extra_term,
    residual,
    head_norm_gain,
    cell_output_weight,
    feedforward_norm_gain,
    gate_projection_weight,
    up_projection_weight,
    down_projection_weight,
):
    whole_gate = lax.all_gather(gate_projection_weight, "sp", axis=0, tiled=True)
    whole_up = lax.all_gather(up_projection_weight, "sp", axis=0, tiled=True)
    length = queries.shape[0]
    heads = input_gate_logits.shape[0]
    dk, dv = queries.shape[1] // heads, cell_value_rows.shape[1] // heads
    log_forget = jax.nn.log_sigmoid(forget_gate_logits.astype(jnp.float32)) + forget_extra_term
    running = jnp.cumsum(log_forget, axis=-1)
    a_log = input_gate_logits.astype(jnp.float32) - running
    m_log = lax.cummax(a_log, axis=1)
    a_top, total = m_log[:, -1], running[:, -1]
    decay = jnp.exp(a_log - a_top[:, None])
    weighed = (
        cell_key_rows.reshape(length, heads, dk).astype(jnp.float32) * decay.T[:, :, None]
    ).astype(jnp.bfloat16)
    state = jnp.stack(
        [
            lax.dot_general(
                weighed[:, h],
                cell_value_rows[:, h * dv : (h + 1) * dv],
                (((0,), (0,)), ((), ())),
                preferred_element_type=jnp.float32,
            )
            for h in range(heads)
        ]
    )
    carried, carried_top = entering_state(state, a_top + total, total)
    m_all = jnp.maximum(m_log, carried_top[:, None])
    coefficient = jnp.exp(carried_top[:, None] - m_all)
    gated = cell(
        queries,
        cell_key_rows,
        cell_value_rows,
        a_log,
        m_all,
        coefficient,
        carried,
        output_gate_logits,
        head_norm_gain[None, :],
    )
    summed = product_scattered(gated, cell_output_weight)
    stream = (residual.astype(jnp.float32) + summed).astype(jnp.bfloat16)
    down_late, stream = lax.optimization_barrier((down_projection_weight, stream))
    whole_down = lax.all_gather(down_late, "sp", axis=1, tiled=True)
    wide = columns_gathered(stream).astype(jnp.float32)
    scale = lax.rsqrt(jnp.mean(wide * wide, axis=-1, keepdims=True) + EPSILON)
    normed = (wide * scale * feedforward_norm_gain.astype(jnp.float32)[None, :]).astype(jnp.bfloat16)
    gate_value = jnp.dot(normed, whole_gate, preferred_element_type=jnp.float32)
    lifted = jnp.dot(normed, whole_up, preferred_element_type=jnp.float32)
    hidden = (jax.nn.silu(gate_value) * lifted).astype(jnp.bfloat16)
    channel_total = product_scattered(hidden, whole_down)
    return (stream.astype(jnp.float32) + 0.5 * channel_total).astype(jnp.bfloat16)


NX, NY = 2, 2
PIECES = 4
BY_NAME = pl.DeviceIdType.MESH


def block_body(
    planes,
    q_in,
    k_in,
    v_in,
    open_in,
    input_in,
    forget_in,
    extra_in,
    resid_in,
    gain_ref,
    wo_in,
    fgain_ref,
    gate_in,
    up_in,
    down_ref,
    out_ref,
    gate_ref,
    up_ref,
    wo_ref,
    a_ref,
    cols_ref,
    meta_ref,
    gu,
    dn,
    rows_all,
    hid,
    sums,
    gu_out,
    num,
    ent,
    st_own,
    st_y,
    st_sum,
    st_pre,
    st_z,
    meta_y,
    meta_sum,
    meta_pre,
    meta_z,
    lw_ref,
    pool,
    core_in,
    x_in,
    core_back,
    y_back,
    x_back,
    zs,
    zr,
    ysem,
    ssem,
    fsem,
    gsem,
    bsem,
    lsem,
):
    sp, tp = lax.axis_index("sp"), lax.axis_index("tp")
    z, y, x, c = sp // NY, sp % NY, tp // 2, tp % 2
    tokens, heads = q_in.shape[0], input_in.shape[0]
    dk, dv = q_in.shape[1] // heads, v_in.shape[1] // heads
    width = resid_in.shape[1]
    depth, hidden = gate_ref.shape
    half = hidden // NY
    count = 2 * NX
    last = planes - 1
    strip = tokens // 4
    wide = width // 2
    part_rows = depth // 2

    partner = {"tp": tp + 1 - 2 * c}
    x_next = {"tp": (1 - x) * 2 + c}
    y_next = {"sp": z * NY + 1 - y}

    def on_plane(at):
        return {"sp": at * NY + y}

    def remote(src, dst, sems, to):
        return pltpu.make_async_remote_copy(
            src_ref=src, dst_ref=dst, send_sem=sems[0], recv_sem=sems[1], device_id=to, device_id_type=BY_NAME
        )

    q_ref, k_ref = core_back.at[0, 0], core_back.at[0, 1]
    v_ref, open_ref, resid_ref = core_back.at[1], core_back.at[2], core_back.at[3]
    loads = {}
    wanted = [("gate", gate_in, gate_ref), ("up", up_in, up_ref), ("k", k_in, k_ref)]
    for name, source, kept in (("v", v_in, v_ref), ("q", q_in, q_ref), ("open", open_in, open_ref)):
        if name == "q":
            wanted.append((name, source, kept))
        else:
            for part in range(2):
                wanted.append((name + str(part), source.at[:, part * wide : (part + 1) * wide], kept.at[part]))
    wanted.append(("wo", wo_in, wo_ref))
    for part in range(2):
        wanted.append(("resid" + str(part), resid_in.at[:, part * wide : (part + 1) * wide], resid_ref.at[part]))
    for index, (name, source, kept) in enumerate(wanted):
        loads[name] = pltpu.make_async_copy(source, kept, lsem.at[index + 1])
        loads[name].start()

    barrier = pltpu.get_barrier_semaphore()
    for to in (partner, x_next, y_next):
        pl.semaphore_signal(barrier, inc=1, device_id=to, device_id_type=BY_NAME)
    for ok, at in ((z > 0, z - 1), (z < last, z + 1)):

        @pl.when(ok)
        def _():
            pl.semaphore_signal(barrier, inc=1, device_id=on_plane(at), device_id_type=BY_NAME)

    ends = jnp.logical_or(z == 0, z == last)
    pl.semaphore_wait(barrier, 5 - jnp.where(ends, 1, 0))

    loads["gate"].wait()
    loads["up"].wait()

    for mine in range(NY):

        @pl.when(y == mine)
        def _():
            own = pl.ds(pl.multiple_of(sp * depth, depth), depth)
            here, there = mine * half, (1 - mine) * half
            gu_out[:, 0:half] = gate_ref[:, there : there + half]
            gu_out[:, half : 2 * half] = up_ref[:, there : there + half]
            gu[own, 0:half] = gate_ref[:, here : here + half]
            gu[own, half : 2 * half] = up_ref[:, here : here + half]

    def gu_rows(at, chunk):
        side = (y + chunk // 2) % 2
        start = (at * NY + side) * depth + (chunk % 2) * part_rows
        return pl.ds(pl.multiple_of(start, part_rows), part_rows)

    def z_copy(way, dist, chunk):
        at = z - dist if way == 0 else z + dist
        to = z + 1 if way == 0 else z - 1
        sems = (zs.at[way, dist, chunk // 4], zr.at[way, dist, chunk])
        if chunk < 4:
            part = gu.at[gu_rows(at, chunk), :]
        else:
            part = dn.at[at * NY + chunk - 4]
        return remote(part, part, sems, on_plane(to))

    def z_arrival(way, dist, chunk):
        at = z - dist if way == 0 else z + dist
        sems = (zs.at[way, 0, 0], zr.at[way, dist - 1, chunk])
        if chunk < 4:
            part = gu.at[gu_rows(at, chunk), :]
        else:
            part = dn.at[at * NY + chunk - 4]
        return remote(part, part, sems, on_plane(z))

    def has_next(way):
        return z < last if way == 0 else z > 0

    def has_origin(way, dist):
        return z >= dist if way == 0 else z + dist <= last

    def z_send(chunk, ways=((0, True), (1, True))):
        for way, also in ways:

            @pl.when(jnp.logical_and(has_next(way), also))
            def _():
                z_copy(way, 0, chunk).start()

    def z_forward(dist, chunk):
        for way in range(2):

            @pl.when(jnp.logical_and(has_origin(way, dist), has_next(way)))
            def _():
                z_arrival(way, dist, chunk).wait_recv()
                z_copy(way, dist, chunk).start()

    def z_down(rank, dist):
        for way in range(2):

            @pl.when(z == (rank if way == 0 else last - rank))
            def _():
                for chunk in (4, 5):
                    if dist:
                        z_arrival(way, dist, chunk).wait_recv()
                    z_copy(way, dist, chunk).start()

    def y_rows(owner, chunk):
        start = (z * NY + owner) * depth + chunk * part_rows
        return pl.ds(pl.multiple_of(start, part_rows), part_rows)

    def y_weight(chunk):
        sems = (ysem.at[0, chunk], ysem.at[1, chunk])
        if chunk < 2:
            return remote(
                gu_out.at[pl.ds(chunk * part_rows, part_rows), :], gu.at[y_rows(y, chunk), :], sems, y_next
            )
        start = pl.multiple_of((1 - y) * half, half)
        return remote(down_ref.at[pl.ds(start, half), :], dn.at[sp], sems, y_next)

    own_down = pltpu.make_async_copy(
        down_ref.at[pl.ds(pl.multiple_of(y * half, half), half), :], dn.at[sp], lsem.at[0]
    )
    z_send(0)

    def padded(rows):
        return jnp.concatenate([rows, jnp.zeros((8 - heads, tokens), jnp.float32)], axis=0)

    lane = lax.broadcasted_iota(jnp.int32, (8, tokens), 1)
    logits = forget_in[...].astype(jnp.float32)
    running = padded(
        jnp.minimum(logits, 0.0) - jnp.log1p(jnp.exp(-jnp.abs(logits))) + extra_in[...]
    )
    step = 1
    while step < tokens:
        running = running + jnp.where(lane >= step, pltpu.roll(running, step, 1), 0.0)
        step *= 2
    a_log = padded(input_in[...].astype(jnp.float32)) - running
    m_log = a_log
    step = 1
    while step < tokens:
        m_log = jnp.maximum(m_log, jnp.where(lane >= step, pltpu.roll(m_log, step, 1), LOWEST_LOG))
        step *= 2
    a_ref[...] = a_log
    a_top, total = m_log[:, tokens - 1 :], running[:, tokens - 1 :]
    decay = jnp.exp(a_log - a_top)
    cols_ref[...] = jnp.concatenate(
        [decay[0:heads], m_log[0:heads], jnp.zeros((8 - 2 * heads, tokens), jnp.float32)], axis=0
    ).T
    meta_ref[...] = jnp.zeros_like(meta_ref)
    meta_ref[0:heads, :] = jnp.broadcast_to((a_top + total)[0:heads], (heads, meta_ref.shape[1]))
    meta_ref[heads : 2 * heads, :] = jnp.broadcast_to(total[0:heads], (heads, meta_ref.shape[1]))
    for name in ("k", "v0", "v1"):
        loads[name].wait()

    for h in range(heads):
        weighed = (
            k_ref[:, h * dk : (h + 1) * dk].astype(jnp.float32) * cols_ref[:, h : h + 1]
        ).astype(jnp.bfloat16)
        st_own[h] = lax.dot_general(
            weighed,
            v_ref[h],
            (((0,), (0,)), ((), ())),
            preferred_element_type=jnp.float32,
        ).astype(jnp.bfloat16)

    state_y = [
        remote(st_own, st_y, (ssem.at[0], ssem.at[1]), y_next),
        remote(meta_ref, meta_y, (ssem.at[2], ssem.at[3]), y_next),
    ]
    for copy in state_y:
        copy.start()
    for chunk in range(3):
        y_weight(chunk).start()
    own_down.start()
    loads["q"].wait()

    def attend(h, i):
        span = (i + 1) * strip
        at = pl.ds(i * strip, strip)
        scores = lax.dot_general(
            q_ref[at, h * dk : (h + 1) * dk],
            k_ref[0:span, h * dk : (h + 1) * dk],
            (((1,), (1,)), ((), ())),
            preferred_element_type=jnp.float32,
        )
        log_weight = a_ref[h : h + 1, 0:span] - cols_ref[at, heads + h : heads + h + 1]
        row = i * strip + lax.broadcasted_iota(jnp.int32, (strip, span), 0)
        col = lax.broadcasted_iota(jnp.int32, (strip, span), 1)
        weight = jnp.where(col <= row, jnp.exp(jnp.minimum(log_weight, 0.0)), 0.0)
        num[at, h * dv : (h + 1) * dv] = jnp.dot(
            (scores * weight).astype(jnp.bfloat16),
            v_ref[h, 0:span, :],
            preferred_element_type=jnp.float32,
        )

    for h in range(heads):
        attend(h, 0)

    for copy in state_y:
        copy.wait_recv()
    first = y == 0
    meta_own, meta_other = meta_ref[...], meta_y[...]
    meta_0 = jnp.where(first, meta_own, meta_other)
    meta_1 = jnp.where(first, meta_other, meta_own)
    top_0 = meta_0[0:heads] + meta_1[heads : 2 * heads]
    top_1 = meta_1[0:heads]
    top = jnp.maximum(top_0, top_1)
    scale_0, scale_1 = jnp.exp(top_0 - top), jnp.exp(top_1 - top)
    scale_own = jnp.where(first, scale_0, scale_1)
    scale_other = jnp.where(first, scale_1, scale_0)
    meta_sum[...] = jnp.zeros_like(meta_sum)
    meta_sum[0:heads, :] = top
    meta_sum[heads : 2 * heads, :] = meta_0[heads : 2 * heads] + meta_1[heads : 2 * heads]
    for h in range(heads):
        st_sum[h] = (
            st_own[h].astype(jnp.float32) * scale_own[h : h + 1]
            + st_y[h].astype(jnp.float32) * scale_other[h : h + 1]
        ).astype(jnp.bfloat16)

    def state_z(step, summed):
        state, meta = (st_pre, meta_pre) if summed else (st_sum, meta_sum)
        to = on_plane(z + step)
        return [
            remote(state, st_z, (ssem.at[4], ssem.at[5]), to),
            remote(meta, meta_z, (ssem.at[6], ssem.at[7]), to),
        ]

    @pl.when(z == 0)
    def _():
        for copy in state_z(1, 0):
            copy.start()

    def hop():
        for copy in state_z(0, 0):
            copy.wait_recv()
        before, own = meta_z[0:heads, :] + meta_sum[heads : 2 * heads, :], meta_sum[0:heads, :]
        joint = jnp.maximum(before, own)
        meta_pre[...] = jnp.zeros_like(meta_pre)
        meta_pre[0:heads, :] = joint
        meta_pre[heads : 2 * heads, :] = meta_z[heads : 2 * heads, :] + meta_sum[heads : 2 * heads, :]
        scale_before, scale_own = jnp.exp(before - joint), jnp.exp(own - joint)
        for h in range(heads):
            st_pre[h] = (
                st_z[h].astype(jnp.float32) * scale_before[h : h + 1]
                + st_sum[h].astype(jnp.float32) * scale_own[h : h + 1]
            ).astype(jnp.bfloat16)
        for copy in state_z(1, 1):
            copy.start()

    z_send(1, ((0, z != 1), (1, True)))
    for h in range(heads):
        for i in range(1, 4):
            attend(h, i)

    pl.when(z == 1)(hop)
    z_send(1, ((0, z == 1),))

    def z_half(part):
        short_part = part_rows // 2
        start = pl.multiple_of((z * NY + 1 - y) * depth + part * short_part, short_part)
        piece = gu.at[pl.ds(start, short_part), :]
        return remote(piece, piece, (zs.at[0, 0, 0], zr.at[0, 0, 2]), on_plane(z + 1))

    y_weight(0).wait_recv()
    z_send(2, ((0, z < 2), (1, True)))

    @pl.when(z == 2)
    def _():
        z_half(0).start()
        hop()
        z_half(1).start()

    low = jnp.full((heads, meta_ref.shape[1]), LOWEST_LOG, jnp.float32)
    later = jnp.where(y == 1, meta_y[heads : 2 * heads, :], 0.0)
    lw_ref[1, 0:heads, :] = jnp.where(y == 1, meta_y[0:heads, :], low)

    @pl.when(z == last)
    def _():
        for copy in state_z(0, 0):
            copy.wait_recv()

    lw_ref[0, 0:heads, :] = jnp.where(z > 0, meta_z[0:heads, :] + later, low)
    ctop = jnp.maximum(lw_ref[0, 0:heads, :], lw_ref[1, 0:heads, :])
    ent[...] = jnp.zeros_like(ent)
    for source, valid in ((0, z > 0), (1, y == 1)):

        @pl.when(valid)
        def _():
            scale = jnp.exp(lw_ref[source, 0:heads, :] - ctop)
            for h in range(heads):
                part = st_y[h] if source else st_z[h]
                ent[h] += part.astype(jnp.float32) * scale[h : h + 1]

    for name in ("open0", "open1", "wo"):
        loads[name].wait()

    def front_core(i):
        at = pl.ds(pl.multiple_of(i * strip, strip), strip)
        return remote(
            pool.at[0:4, at, :], core_in.at[:, at, :], (fsem.at[8], fsem.at[i]), partner
        )

    def front_x(i):
        at = pl.ds(pl.multiple_of(i * strip, strip), strip)
        return remote(
            pool.at[8:10, at, :], x_in.at[:, at, :], (fsem.at[9], fsem.at[4 + i]), x_next
        )

    def gate_strip(i):
        at = pl.ds(pl.multiple_of(i * strip, strip), strip)
        gated = []
        for h in range(heads):
            lanes = slice(h * dv, (h + 1) * dv)
            before = jnp.dot(
                q_ref[at, h * dk : (h + 1) * dk],
                ent[h].astype(jnp.bfloat16),
                preferred_element_type=jnp.float32,
            )
            m_log = cols_ref[at, heads + h : heads + h + 1]
            m_all = jnp.maximum(m_log, ctop[h : h + 1, 0:1])
            memory = (
                num[at, lanes] * jnp.exp(m_log - m_all)
                + jnp.exp(ctop[h : h + 1, 0:1] - m_all) * before
            ) * dk ** (-0.5)
            normal = memory * lax.rsqrt(jnp.mean(memory * memory, axis=-1, keepdims=True) + EPSILON)
            opened = jax.nn.sigmoid(open_ref[h, at, :].astype(jnp.float32))
            gated.append((normal * gain_ref[lanes][None, :].astype(jnp.float32) * opened).astype(jnp.bfloat16))
        gated = jnp.concatenate(gated, axis=1)
        for chip in range(NX):
            for part in range(2):
                for mine in range(2):
                    core = c if mine else 1 - c
                    lanes = pl.ds(
                        pl.multiple_of((chip * 2 + core) * width + part * wide, wide), wide
                    )
                    pool[mine * 4 + chip * 2 + part, at, :] = jnp.dot(
                        gated, wo_ref[:, lanes], preferred_element_type=jnp.float32
                    ).astype(jnp.bfloat16)
        front_core(i).start()

    def core_sum(i):
        at = pl.ds(pl.multiple_of(i * strip, strip), strip)
        front_core(i).wait_recv()
        for part in range(2):
            far, near = (1 - x) * 2 + part, x * 2 + part
            pool[8 + part, at, :] = (
                pool[4 + far, at, :].astype(jnp.float32) + core_in[far, at, :].astype(jnp.float32)
            ).astype(jnp.bfloat16)
        front_x(i).start()

    @pl.loop(0, 5)
    def _(i):
        @pl.when(i < 4)
        def _():
            gate_strip(i)

        @pl.when(i == 2)
        def _():
            y_weight(1).wait_recv()
            z_send(3)

        @pl.when(i >= 1)
        def _():
            core_sum(i - 1)

    z_forward(1, 0)
    z_forward(1, 1)
    y_weight(2).wait_recv()
    own_down.wait()
    z_down(0, 0)
    for part in range(2):
        loads["resid" + str(part)].wait()

    def piece(owner_x, owner_c, owner_y, i):
        at = pl.multiple_of(owner_y * tokens + i * strip, strip)
        lanes = pl.multiple_of((owner_x * 2 + owner_c) * width, width)
        return rows_all.at[pl.ds(at, strip), pl.ds(lanes, width)]

    def to_x(i):
        part = piece(x, c, y, i)
        return remote(part, part, (gsem.at[28], gsem.at[i]), x_next)

    def to_y(kind, i):
        part = piece(x if kind == 0 else 1 - x, c, y, i)
        return remote(part, part, (gsem.at[29 + kind], gsem.at[4 + kind * 4 + i]), y_next)

    def to_core(kind, i):
        part = piece(
            x if kind % 2 == 0 else 1 - x, c, y if kind // 2 == 0 else 1 - y, i
        )
        return remote(part, part, (gsem.at[31 + kind], gsem.at[12 + kind * 4 + i]), partner)

    @pl.loop(0, 4)
    def _(i):
        at = pl.ds(pl.multiple_of(i * strip, strip), strip)
        front_x(i).wait_recv()
        start = pl.multiple_of(y * tokens + i * strip, strip)
        for part in range(2):
            lanes = slice(part * wide, (part + 1) * wide)
            near = x * 2 + part
            total = (
                pool[4 + near, at, :].astype(jnp.float32)
                + core_in[near, at, :].astype(jnp.float32)
                + x_in[part, at, :].astype(jnp.float32)
            )
            fresh = (resid_ref[part, at, :].astype(jnp.float32) + total).astype(jnp.bfloat16)
            out_ref[at, lanes] = fresh
            columns = pl.ds(pl.multiple_of(tp * width + part * wide, wide), wide)
            rows_all[pl.ds(start, strip), columns] = fresh
        to_x(i).start()
        to_y(0, i).start()
        to_core(0, i).start()

        @pl.when(i == 1)
        def _():
            z_forward(1, 2)

    z_forward(1, 3)
    z_down(1, 0)

    @pl.loop(0, 4)
    def _(i):
        to_x(i).wait_recv()
        to_y(1, i).start()
        to_core(1, i).start()
        to_y(0, i).wait_recv()
        to_core(2, i).start()

        @pl.when(i == 1)
        def _():
            z_forward(2, 0)
            z_forward(2, 1)

    z_forward(2, 2)
    z_down(1, 1)

    short = 128

    def norm_rows(owner, kinds):
        @pl.loop(0, 4)
        def _(i):
            for kind in kinds:
                to_core(kind, i).wait_recv()

        @pl.loop(0, tokens // short)
        def _(i):
            at = pl.ds(pl.multiple_of(owner * tokens + i * short, short), short)
            wide_rows = rows_all[at, :].astype(jnp.float32)
            scale = lax.rsqrt(jnp.mean(wide_rows * wide_rows, axis=-1, keepdims=True) + EPSILON)
            rows_all[at, :] = (wide_rows * scale * fgain_ref[...][None, :].astype(jnp.float32)).astype(
                jnp.bfloat16
            )

    @pl.loop(0, 4)
    def _(i):
        to_y(1, i).wait_recv()
        to_core(3, i).start()

    z_forward(2, 3)

    whole_strip = rows_all.at[pl.ds(0, tokens), pl.ds(0, width)]
    remote(pool.at[0:4], pool.at[0:4], (fsem.at[8], fsem.at[0]), partner).wait_send()
    remote(pool.at[8:10], pool.at[8:10], (fsem.at[9], fsem.at[4]), x_next).wait_send()
    for index in range(28, 35):
        remote(whole_strip, whole_strip, (gsem.at[index], gsem.at[0]), partner).wait_send()

    norm_rows(y, (0, 1))
    norm_rows(1 - y, (2, 3))

    tall = 512
    plane_rows = NY * depth
    early = last * plane_rows
    early_at = jnp.where(z == last, plane_rows, 0)
    late_at = jnp.where(z == last, 0, early)

    def gate_up(i, start, size):
        at = pl.ds(pl.multiple_of(i * tall, tall), tall)
        taken = pl.ds(pl.multiple_of(start, plane_rows), size)
        return at, jnp.dot(rows_all[at, taken], gu[taken, :], preferred_element_type=jnp.float32)

    def gu_arrived(dist):
        for way in range(2):

            @pl.when(jnp.logical_and(has_origin(way, dist), jnp.logical_not(has_next(way))))
            def _():
                for chunk in range(4):
                    z_arrival(way, dist, chunk).wait_recv()

    for dist in range(1, last):
        gu_arrived(dist)

    @pl.loop(0, NY * tokens // tall)
    def _(i):
        at, product = gate_up(i, early_at, early)
        sums[at, :] = product

    z_down(2, 1)
    z_down(2, 0)
    gu_arrived(last)

    def finish_hidden(i):
        at, product = gate_up(i, late_at, plane_rows)
        both = sums[at, :] + product
        hid[at, :] = (jax.nn.silu(both[:, :half]) * both[:, half:]).astype(jnp.bfloat16)

    @pl.loop(0, NY)
    def _(i):
        finish_hidden(i * (tokens // tall))


    units = planes * NY * PIECES
    rows = tokens // PIECES

    def side_of(unit):
        return unit // PIECES % NY

    def place(unit):
        step = unit // (PIECES * NY)
        return (z // 2 + step % 2) % 2 * 2 + (z % 2 + step // 2) % 2

    def slot(unit):
        return unit // (PIECES * NY) % 2 * 2 + side_of(unit)

    def kept_index(unit):
        return slot(unit) * PIECES + unit % PIECES

    def strip_of(unit):
        return pl.ds(pl.multiple_of(unit % PIECES * rows, rows), rows)

    def held(unit, top_row):
        return unit // PIECES * 2 + top_row, strip_of(unit)

    def both_of(unit):
        return pool.at[pl.ds(unit // PIECES * 2, 2), strip_of(unit)]

    def back_core(unit):
        kept = core_back.at[slot(unit), :, strip_of(unit)]
        return remote(both_of(unit), kept, (bsem.at[0], bsem.at[3 + kept_index(unit)]), partner)

    def back_y(unit):
        kept = y_back.at[slot(unit), strip_of(unit)]
        return remote(pool.at[held(unit, 1 - y)], kept, (bsem.at[1], bsem.at[3 + 4 * PIECES + kept_index(unit)]), y_next)

    def back_x(unit):
        kept = x_back.at[side_of(unit), strip_of(unit)]
        return remote(pool.at[held(unit, y)], kept, (bsem.at[2], bsem.at[3 + 8 * PIECES + unit % (2 * PIECES)]), x_next)

    def keeps(unit):
        return place(unit) % 2 == c

    def owns(unit):
        return place(unit) == tp

    def passes(unit):
        return jnp.logical_and(keeps(unit), place(unit) // 2 != x)

    def add(unit, top_row, other):
        at = held(unit, top_row)
        pool[at] = (pool[at].astype(jnp.float32) + other.astype(jnp.float32)).astype(jnp.bfloat16)

    def down_part(unit):
        step, side = unit // (PIECES * NY), side_of(unit)
        ends = jnp.logical_or(z == 0, z == last)

        @pl.when(jnp.logical_and(jnp.logical_and(step > 0, unit % PIECES == 0), ends))
        def _():
            at = place(unit)
            way = jnp.where(z == 0, 1, 0)
            dist = jnp.where(z == 0, at, z - at)
            part = dn.at[at * NY + side]
            remote(part, part, (zs.at[way, 0, 0], zr.at[way, dist - 1, 4 + side]), on_plane(z)).wait_recv()

        weight = dn[place(unit) * NY + side]
        for top_row in (1 - y, y):
            start = pl.multiple_of(top_row * tokens + unit % PIECES * rows, rows)
            pool[held(unit, top_row)] = jnp.dot(
                hid[pl.ds(start, rows), :], weight, preferred_element_type=jnp.float32
            ).astype(jnp.bfloat16)

        @pl.when(jnp.logical_not(keeps(unit)))
        def _():
            back_core(unit).start()

    def after_core(unit):
        @pl.when(keeps(unit))
        def _():
            back_core(unit).wait_recv()
            for top_row in (1 - y, y):
                add(unit, top_row, core_back[slot(unit), top_row, strip_of(unit)])
            back_y(unit).start()

    def after_y(unit):
        @pl.when(keeps(unit))
        def _():
            back_y(unit).wait_recv()
            add(unit, y, y_back[slot(unit), strip_of(unit)])

        @pl.when(passes(unit))
        def _():
            back_x(unit).start()

    def finish(unit, other):
        at = strip_of(unit)
        lanes = pl.ds(pl.multiple_of(side_of(unit) * wide, wide), wide)
        total = pool[held(unit, y)].astype(jnp.float32) + other.astype(jnp.float32)
        out_ref[at, lanes] = (out_ref[at, lanes].astype(jnp.float32) + 0.5 * total).astype(out_ref.dtype)

    def after_x(unit):
        @pl.when(owns(unit))
        def _():
            back_x(unit).wait_recv()
            finish(unit, x_back[side_of(unit), strip_of(unit)])

    def run(low, high, begun=0, trail=0):
        @pl.loop(low, high + 1)
        def _(i):
            @pl.when(jnp.logical_and(i >= begun, i < high))
            def _():
                down_part(i)

            @pl.when(i > low)
            def _():
                after_core(i - 1)

            if trail:

                @pl.when(i < high - 1)
                def _():
                    after_y(i - trail)

    def each(stage, low, high):
        @pl.loop(low, high)
        def _(i):
            stage(i)


    def at_ends(low, high):
        @pl.when(ends)
        def _():
            run(low, high)

    begun = tall // rows

    @pl.loop(0, begun)
    def _(i):
        down_part(i)

    @pl.loop(0, NY)
    def _(i):
        finish_hidden(i * (tokens // tall) + 1)

    run(0, 8, begun)
    z_down(2, 2)
    run(8, 16)

    @pl.when(jnp.logical_not(ends))
    def _():
        run(16, units)

    each(after_y, 0, 8)
    at_ends(16, 20)
    each(after_y, 8, 12)
    at_ends(20, 24)
    each(after_y, 12, 20)
    at_ends(24, 28)
    each(after_y, 20, 24)
    each(after_y, units - 2 * PIECES, units - 2 * PIECES + 1)

    @pl.when(ends)
    def _():
        run(units - PIECES, units, 0, PIECES - 1)

    @pl.when(jnp.logical_not(ends))
    def _():
        each(after_y, units - 2 * PIECES + 1, units - PIECES)

    each(after_y, units - PIECES, units)
    def sent(part, sem, to):
        remote(part, part, (sem, zr.at[0, 0, 0]), to).wait_send()

    sent(core_back, bsem.at[0], partner)
    sent(y_back, bsem.at[1], y_next)
    sent(x_back, bsem.at[2], x_next)
    for chunk in range(3):
        y_weight(chunk).wait_send()
    for copy in state_y:
        copy.wait_send()

    @pl.when(z == 0)
    def _():
        for copy in state_z(1, 0):
            copy.wait_send()

    @pl.when(jnp.logical_and(z > 0, z < last))
    def _():
        for copy in state_z(1, 1):
            copy.wait_send()

    for way in range(2):
        for dist in range(planes - 1):

            @pl.when(jnp.logical_and(has_origin(way, dist), has_next(way)))
            def _():
                sent(gu.at[pl.ds(0, plane_rows), :], zs.at[way, dist, 0], partner)
                sent(dn.at[pl.ds(0, NY)], zs.at[way, dist, 1], partner)

    each(after_x, 0, units)


def plane_layer(
    planes,
    queries,
    cell_key_rows,
    cell_value_rows,
    output_gate_logits,
    input_gate_logits,
    forget_gate_logits,
    forget_extra_term,
    residual,
    head_norm_gain,
    cell_output_weight,
    feedforward_norm_gain,
    gate_projection_weight,
    up_projection_weight,
    down_projection_weight,
):
    tokens, heads = queries.shape[0], input_gate_logits.shape[0]
    width = residual.shape[1]
    model = cell_output_weight.shape[1]
    depth, hidden = gate_projection_weight.shape
    half = hidden // NY
    dk, dv = queries.shape[1] // heads, cell_value_rows.shape[1] // heads
    bf16, f32 = jnp.bfloat16, jnp.float32
    vmem, dma = pltpu.VMEM, pltpu.SemaphoreType.DMA
    scratch = [
        vmem((depth, hidden), bf16),
        vmem((depth, hidden), bf16),
        vmem((heads * dv, model), bf16),
        vmem((8, tokens), f32),
        vmem((tokens, 8), f32),
        vmem((8, dv), f32),
        vmem((model, hidden), bf16),
        vmem((planes * NY, half, depth), bf16),
        vmem((NY * tokens, 2 * NX * width), bf16),
        vmem((NY * tokens, half), bf16),
        vmem((NY * tokens, hidden), f32),
        vmem((depth, hidden), bf16),
        vmem((tokens, heads * dv), f32),
        vmem((heads, dk, dv), f32),
        vmem((heads, dk, dv), bf16),
        vmem((heads, dk, dv), bf16),
        vmem((heads, dk, dv), bf16),
        vmem((heads, dk, dv), bf16),
        vmem((heads, dk, dv), bf16),
        vmem((8, dv), f32),
        vmem((8, dv), f32),
        vmem((8, dv), f32),
        vmem((8, dv), f32),
        vmem((2, 8, dv), f32),
        vmem((2 * planes * NY, tokens, width // 2), bf16),
        vmem((4, tokens, width // 2), bf16),
        vmem((2, tokens, width // 2), bf16),
        vmem((planes * NY // 2, 2, tokens, width // 2), bf16),
        vmem((planes * NY // 2, tokens, width // 2), bf16),
        vmem((2, tokens, width // 2), bf16),
        dma((2, planes - 1, 2)),
        dma((2, planes - 1, 6)),
        dma((2, 3)),
        dma((8,)),
        dma((10,)),
        dma((35,)),
        dma((3 + 10 * PIECES,)),
        dma((12,)),
    ]
    whole = pl.BlockSpec(memory_space=pltpu.VMEM)
    far = pl.BlockSpec(memory_space=pl.ANY)
    return pl.pallas_call(
        functools.partial(block_body, planes),
        out_shape=pltpu.VMEM((tokens, width), bf16),
        in_specs=[far] * 4 + [whole] * 3 + [far, whole, far, whole] + [far] * 3,
        out_specs=whole,
        scratch_shapes=scratch,
        compiler_params=pltpu.CompilerParams(
            collective_id=0, has_side_effects=True, vmem_limit_bytes=65000000
        ),
        cost_estimate=pl.CostEstimate(flops=22 * 10**9, bytes_accessed=10**7, transcendentals=0),
        name="block",
    )(
        queries,
        cell_key_rows,
        cell_value_rows,
        output_gate_logits,
        input_gate_logits,
        forget_gate_logits,
        forget_extra_term,
        residual,
        head_norm_gain,
        cell_output_weight,
        feedforward_norm_gain,
        gate_projection_weight,
        up_projection_weight,
        down_projection_weight,
    )


def layer(rows, columns, *arrays):
    if columns == 2 * NX and rows == 4 * NY:
        return plane_layer(rows // NY, *arrays)
    return general(*arrays)


def solution(mesh):
    placed = (
        P("sp", "tp"),
        P("sp", "tp"),
        P("sp", "tp"),
        P("sp", "tp"),
        P("tp", "sp"),
        P("tp", "sp"),
        P("tp", "sp"),
        P("sp", "tp"),
        P("tp"),
        P("tp", None),
        P(),
        P("sp", "tp"),
        P("sp", "tp"),
        P("tp", "sp"),
    )
    return jax.shard_map(
        functools.partial(layer, mesh.shape["sp"], mesh.shape["tp"]), mesh=mesh, in_specs=placed, out_specs=P("sp", "tp"), check_vma=False
    )
```

```python
import functools

import jax
import jax.numpy as jnp
from jax import lax
from jax.experimental import pallas as pl
from jax.experimental.pallas import tpu as pltpu
from jax.sharding import PartitionSpec as P

LOWEST_LOG = -1e30
EPSILON = 1e-06


def shift_pairs(length, step):
    return [(source, source + step) for source in range(length - step)]


def entering_state(state, top, total):
    length, index = lax.axis_size("sp"), lax.axis_index("sp")
    heads, key_width, value_width = state.shape

    def pack(s, t, f):
        tail = jnp.zeros((heads, 8, value_width), jnp.float32)
        tail = tail.at[:, 0, :].set(t[:, None]).at[:, 1, :].set(f[:, None])
        return jnp.concatenate([s, tail], axis=1)

    def unpack(p, valid):
        s = p[:, :key_width, :]
        t = jnp.where(valid, p[:, key_width, 0], LOWEST_LOG)
        f = jnp.where(valid, p[:, key_width + 1, 0], 0.0)
        return jnp.where(valid, s, 0.0), t, f

    moved = lax.ppermute(pack(state, top, total), "sp", shift_pairs(length, 1))
    s, t, f = unpack(moved, index >= 1)
    step = 1
    while step < length - 1:
        moved = lax.ppermute(pack(s, t, f), "sp", shift_pairs(length, step))
        s0, t0, f0 = unpack(moved, index >= step)
        from_top = t0 + f
        new_top = jnp.maximum(from_top, t)
        s = (
            jnp.exp(from_top - new_top)[:, None, None] * s0
            + jnp.exp(t - new_top)[:, None, None] * s
        )
        t, f = new_top, f0 + f
        step *= 2
    return s, t


def cell_kernel(q_ref, k_ref, v_ref, a_ref, m_ref, c_ref, state_ref, open_ref, gain_ref, o_ref, *, scale):
    block = q_ref.shape[0]
    length = k_ref.shape[0]
    q = q_ref[...]
    first = pl.program_id(1) * block
    scores = lax.dot_general(
        q, k_ref[...], (((1,), (1,)), ((), ())), preferred_element_type=jnp.float32
    )
    rows = first + lax.broadcasted_iota(jnp.int32, (block, length), 0)
    cols = lax.broadcasted_iota(jnp.int32, (block, length), 1)
    weight = jnp.where(cols <= rows, jnp.exp(jnp.minimum(a_ref[0] - m_ref[0], 0.0)), 0.0)
    numer = jnp.dot(
        (scores * weight).astype(jnp.bfloat16), v_ref[...], preferred_element_type=jnp.float32
    )
    before = jnp.dot(q, state_ref[0].astype(jnp.bfloat16), preferred_element_type=jnp.float32)
    memory = (numer + c_ref[0] * before) * scale
    normal = memory * lax.rsqrt(jnp.mean(memory * memory, axis=-1, keepdims=True) + EPSILON)
    gate_open = jax.nn.sigmoid(open_ref[...].astype(jnp.float32))
    o_ref[...] = (normal * gain_ref[...].astype(jnp.float32) * gate_open).astype(o_ref.dtype)


def cell(queries, keys, values, a_log, m_col, c_col, state, open_logits, gain):
    heads, length = a_log.shape
    dk, dv = queries.shape[1] // heads, values.shape[1] // heads
    block = min(length, 256)
    return pl.pallas_call(
        lambda *refs: cell_kernel(*refs, scale=dk ** (-0.5)),
        grid=(heads, length // block),
        in_specs=[
            pl.BlockSpec((block, dk), lambda h, i: (i, h)),
            pl.BlockSpec((length, dk), lambda h, i: (0, h)),
            pl.BlockSpec((length, dv), lambda h, i: (0, h)),
            pl.BlockSpec((1, 1, length), lambda h, i: (h, 0, 0)),
            pl.BlockSpec((1, block, 1), lambda h, i: (h, i, 0)),
            pl.BlockSpec((1, block, 1), lambda h, i: (h, i, 0)),
            pl.BlockSpec((1, dk, dv), lambda h, i: (h, 0, 0)),
            pl.BlockSpec((block, dv), lambda h, i: (i, h)),
            pl.BlockSpec((1, dv), lambda h, i: (0, h)),
        ],
        out_specs=pl.BlockSpec((block, dv), lambda h, i: (i, h)),
        out_shape=jax.ShapeDtypeStruct((length, heads * dv), jnp.bfloat16),
        cost_estimate=pl.CostEstimate(
            flops=8 * heads * length * length * dv, bytes_accessed=6 * length * heads * dv, transcendentals=0
        ),
        name="cell",
    )(queries, keys, values, a_log[:, None, :], m_col[:, :, None], c_col[:, :, None], state, open_logits, gain)


def partner_pairs(count):
    return [(i, i ^ 1) for i in range(count)]


def ring_pairs(count, step):
    return [(i, (i + 2 * step) % count) for i in range(count)]


def product_scattered(rows, weight):
    count, index = lax.axis_size("tp"), lax.axis_index("tp")
    chips, core, chip = count // 2, index % 2, index // 2
    width = weight.shape[1] // count

    def product(block):
        columns = lax.dynamic_slice_in_dim(weight, block * width, width, 1)
        return jnp.dot(rows, columns, preferred_element_type=jnp.float32)

    def chip_sum(to):
        given = product(2 * to + 1 - core).astype(jnp.bfloat16)
        got = lax.ppermute(given, "tp", partner_pairs(count))
        return product(2 * to + core) + got.astype(jnp.float32)

    moved = []
    for step in range(1, chips):
        sent = chip_sum((chip + step) % chips).astype(jnp.bfloat16)
        moved.append(lax.ppermute(sent, "tp", ring_pairs(count, step)))
    total = chip_sum(chip)
    for part in moved:
        total = total + part.astype(jnp.float32)
    return total


def columns_gathered(block):
    count, index = lax.axis_size("tp"), lax.axis_index("tp")
    chips, core, chip = count // 2, index % 2, index // 2
    width = block.shape[1]
    whole = jnp.zeros((block.shape[0], count * width), block.dtype)
    held = [(chip, block)]
    for step in range(1, chips):
        moved = lax.ppermute(block, "tp", ring_pairs(count, step))
        held.append(((chip - step) % chips, moved))
    for place, piece in held:
        other = lax.ppermute(piece, "tp", partner_pairs(count))
        whole = lax.dynamic_update_slice(whole, piece, (0, (2 * place + core) * width))
        whole = lax.dynamic_update_slice(whole, other, (0, (2 * place + 1 - core) * width))
    return whole


def general(
    queries,
    cell_key_rows,
    cell_value_rows,
    output_gate_logits,
    input_gate_logits,
    forget_gate_logits,
    forget_extra_term,
    residual,
    head_norm_gain,
    cell_output_weight,
    feedforward_norm_gain,
    gate_projection_weight,
    up_projection_weight,
    down_projection_weight,
):
    whole_gate = lax.all_gather(gate_projection_weight, "sp", axis=0, tiled=True)
    whole_up = lax.all_gather(up_projection_weight, "sp", axis=0, tiled=True)
    length = queries.shape[0]
    heads = input_gate_logits.shape[0]
    dk, dv = queries.shape[1] // heads, cell_value_rows.shape[1] // heads
    log_forget = jax.nn.log_sigmoid(forget_gate_logits.astype(jnp.float32)) + forget_extra_term
    running = jnp.cumsum(log_forget, axis=-1)
    a_log = input_gate_logits.astype(jnp.float32) - running
    m_log = lax.cummax(a_log, axis=1)
    a_top, total = m_log[:, -1], running[:, -1]
    decay = jnp.exp(a_log - a_top[:, None])
    weighed = (
        cell_key_rows.reshape(length, heads, dk).astype(jnp.float32) * decay.T[:, :, None]
    ).astype(jnp.bfloat16)
    state = jnp.stack(
        [
            lax.dot_general(
                weighed[:, h],
                cell_value_rows[:, h * dv : (h + 1) * dv],
                (((0,), (0,)), ((), ())),
                preferred_element_type=jnp.float32,
            )
            for h in range(heads)
        ]
    )
    carried, carried_top = entering_state(state, a_top + total, total)
    m_all = jnp.maximum(m_log, carried_top[:, None])
    coefficient = jnp.exp(carried_top[:, None] - m_all)
    gated = cell(
        queries,
        cell_key_rows,
        cell_value_rows,
        a_log,
        m_all,
        coefficient,
        carried,
        output_gate_logits,
        head_norm_gain[None, :],
    )
    summed = product_scattered(gated, cell_output_weight)
    stream = (residual.astype(jnp.float32) + summed).astype(jnp.bfloat16)
    down_late, stream = lax.optimization_barrier((down_projection_weight, stream))
    whole_down = lax.all_gather(down_late, "sp", axis=1, tiled=True)
    wide = columns_gathered(stream).astype(jnp.float32)
    scale = lax.rsqrt(jnp.mean(wide * wide, axis=-1, keepdims=True) + EPSILON)
    normed = (wide * scale * feedforward_norm_gain.astype(jnp.float32)[None, :]).astype(jnp.bfloat16)
    gate_value = jnp.dot(normed, whole_gate, preferred_element_type=jnp.float32)
    lifted = jnp.dot(normed, whole_up, preferred_element_type=jnp.float32)
    hidden = (jax.nn.silu(gate_value) * lifted).astype(jnp.bfloat16)
    channel_total = product_scattered(hidden, whole_down)
    return (stream.astype(jnp.float32) + 0.5 * channel_total).astype(jnp.bfloat16)


NX, NY = 2, 2
PIECES = 4
BY_NAME = pl.DeviceIdType.MESH


def block_body(
    planes,
    q_in,
    k_in,
    v_in,
    open_in,
    input_far,
    forget_far,
    extra_far,
    resid_in,
    gain_far,
    wo_in,
    fgain_far,
    gate_in,
    up_in,
    down_ref,
    out_ref,
    input_in,
    forget_in,
    extra_in,
    gain_ref,
    fgain_ref,
    gate_ref,
    up_ref,
    wo_ref,
    a_ref,
    cols_ref,
    meta_ref,
    gu,
    dn,
    rows_all,
    hid,
    sums,
    gu_out,
    num,
    ent,
    st_own,
    st_y,
    st_sum,
    st_pre,
    st_z,
    meta_y,
    meta_sum,
    meta_pre,
    meta_z,
    lw_ref,
    pool,
    core_in,
    x_in,
    core_back,
    y_back,
    x_back,
    zs,
    zr,
    ysem,
    ssem,
    fsem,
    gsem,
    bsem,
    lsem,
):
    sp, tp = lax.axis_index("sp"), lax.axis_index("tp")
    z, y, x, c = sp // NY, sp % NY, tp // 2, tp % 2
    tokens, heads = q_in.shape[0], input_in.shape[0]
    dk, dv = q_in.shape[1] // heads, v_in.shape[1] // heads
    width = resid_in.shape[1]
    depth, hidden = gate_ref.shape
    half = hidden // NY
    count = 2 * NX
    last = planes - 1
    strip = tokens // 4
    wide = width // 2
    part_rows = depth // 2

    partner = {"tp": tp + 1 - 2 * c}
    x_next = {"tp": (1 - x) * 2 + c}
    y_next = {"sp": z * NY + 1 - y}

    def on_plane(at):
        return {"sp": at * NY + y}

    def remote(src, dst, sems, to):
        return pltpu.make_async_remote_copy(
            src_ref=src, dst_ref=dst, send_sem=sems[0], recv_sem=sems[1], device_id=to, device_id_type=BY_NAME
        )

    q_ref, k_ref = core_back.at[0, 0], core_back.at[0, 1]
    v_ref, open_ref, resid_ref = core_back.at[1], core_back.at[2], core_back.at[3]
    loads = {}
    wanted = [
        ("gate", gate_in, gate_ref),
        ("up", up_in, up_ref),
        ("forget", forget_far, forget_in),
        ("extra", extra_far, extra_in),
        ("input", input_far, input_in),
        ("gain", gain_far, gain_ref),
        ("fgain", fgain_far, fgain_ref),
        ("k", k_in, k_ref),
    ]
    for name, source, kept in (("v", v_in, v_ref), ("q", q_in, q_ref), ("open", open_in, open_ref)):
        if name == "q":
            wanted.append((name, source, kept))
        else:
            for part in range(2):
                wanted.append((name + str(part), source.at[:, part * wide : (part + 1) * wide], kept.at[part]))
    wanted.append(("wo", wo_in, wo_ref))
    for part in range(2):
        wanted.append(("resid" + str(part), resid_in.at[:, part * wide : (part + 1) * wide], resid_ref.at[part]))
    for index, (name, source, kept) in enumerate(wanted):
        loads[name] = pltpu.make_async_copy(source, kept, lsem.at[index + 1])
        loads[name].start()

    barrier = pltpu.get_barrier_semaphore()
    for to in (partner, x_next, y_next):
        pl.semaphore_signal(barrier, inc=1, device_id=to, device_id_type=BY_NAME)
    for ok, at in ((z > 0, z - 1), (z < last, z + 1)):

        @pl.when(ok)
        def _():
            pl.semaphore_signal(barrier, inc=1, device_id=on_plane(at), device_id_type=BY_NAME)

    ends = jnp.logical_or(z == 0, z == last)
    pl.semaphore_wait(barrier, 5 - jnp.where(ends, 1, 0))

    loads["gate"].wait()
    loads["up"].wait()

    for mine in range(NY):

        @pl.when(y == mine)
        def _():
            own = pl.ds(pl.multiple_of(sp * depth, depth), depth)
            here, there = mine * half, (1 - mine) * half
            gu_out[:, 0:half] = gate_ref[:, there : there + half]
            gu_out[:, half : 2 * half] = up_ref[:, there : there + half]
            gu[own, 0:half] = gate_ref[:, here : here + half]
            gu[own, half : 2 * half] = up_ref[:, here : here + half]

    def gu_rows(at, chunk):
        side = (y + chunk // 2) % 2
        start = (at * NY + side) * depth + (chunk % 2) * part_rows
        return pl.ds(pl.multiple_of(start, part_rows), part_rows)

    def z_copy(way, dist, chunk):
        at = z - dist if way == 0 else z + dist
        to = z + 1 if way == 0 else z - 1
        sems = (zs.at[way, dist, chunk // 4], zr.at[way, dist, chunk])
        if chunk < 4:
            part = gu.at[gu_rows(at, chunk), :]
        else:
            part = dn.at[at * NY + chunk - 4]
        return remote(part, part, sems, on_plane(to))

    def z_arrival(way, dist, chunk):
        at = z - dist if way == 0 else z + dist
        sems = (zs.at[way, 0, 0], zr.at[way, dist - 1, chunk])
        if chunk < 4:
            part = gu.at[gu_rows(at, chunk), :]
        else:
            part = dn.at[at * NY + chunk - 4]
        return remote(part, part, sems, on_plane(z))

    def has_next(way):
        return z < last if way == 0 else z > 0

    def has_origin(way, dist):
        return z >= dist if way == 0 else z + dist <= last

    def z_send(chunk, ways=((0, True), (1, True))):
        for way, also in ways:

            @pl.when(jnp.logical_and(has_next(way), also))
            def _():
                z_copy(way, 0, chunk).start()

    def z_forward(dist, chunk):
        for way in range(2):

            @pl.when(jnp.logical_and(has_origin(way, dist), has_next(way)))
            def _():
                z_arrival(way, dist, chunk).wait_recv()
                z_copy(way, dist, chunk).start()

    def z_down(rank, dist):
        for way in range(2):

            @pl.when(z == (rank if way == 0 else last - rank))
            def _():
                for chunk in (4, 5):
                    if dist:
                        z_arrival(way, dist, chunk).wait_recv()
                    z_copy(way, dist, chunk).start()

    def y_rows(owner, chunk):
        start = (z * NY + owner) * depth + chunk * part_rows
        return pl.ds(pl.multiple_of(start, part_rows), part_rows)

    def y_weight(chunk):
        sems = (ysem.at[0, chunk], ysem.at[1, chunk])
        if chunk < 2:
            return remote(
                gu_out.at[pl.ds(chunk * part_rows, part_rows), :], gu.at[y_rows(y, chunk), :], sems, y_next
            )
        start = pl.multiple_of((1 - y) * half, half)
        return remote(down_ref.at[pl.ds(start, half), :], dn.at[sp], sems, y_next)

    own_down = pltpu.make_async_copy(
        down_ref.at[pl.ds(pl.multiple_of(y * half, half), half), :], dn.at[sp], lsem.at[0]
    )
    z_send(0)

    def padded(rows):
        return jnp.concatenate([rows, jnp.zeros((8 - heads, tokens), jnp.float32)], axis=0)

    for name in ("forget", "extra", "input", "gain", "fgain"):
        loads[name].wait()
    lane = lax.broadcasted_iota(jnp.int32, (8, tokens), 1)
    logits = forget_in[...].astype(jnp.float32)
    running = padded(
        jnp.minimum(logits, 0.0) - jnp.log1p(jnp.exp(-jnp.abs(logits))) + extra_in[...]
    )
    step = 1
    while step < tokens:
        running = running + jnp.where(lane >= step, pltpu.roll(running, step, 1), 0.0)
        step *= 2
    a_log = padded(input_in[...].astype(jnp.float32)) - running
    m_log = a_log
    step = 1
    while step < tokens:
        m_log = jnp.maximum(m_log, jnp.where(lane >= step, pltpu.roll(m_log, step, 1), LOWEST_LOG))
        step *= 2
    a_ref[...] = a_log
    a_top, total = m_log[:, tokens - 1 :], running[:, tokens - 1 :]
    decay = jnp.exp(a_log - a_top)
    cols_ref[...] = jnp.concatenate(
        [decay[0:heads], m_log[0:heads], jnp.zeros((8 - 2 * heads, tokens), jnp.float32)], axis=0
    ).T
    meta_ref[...] = jnp.zeros_like(meta_ref)
    meta_ref[0:heads, :] = jnp.broadcast_to((a_top + total)[0:heads], (heads, meta_ref.shape[1]))
    meta_ref[heads : 2 * heads, :] = jnp.broadcast_to(total[0:heads], (heads, meta_ref.shape[1]))
    for name in ("k", "v0", "v1"):
        loads[name].wait()

    for h in range(heads):
        weighed = (
            k_ref[:, h * dk : (h + 1) * dk].astype(jnp.float32) * cols_ref[:, h : h + 1]
        ).astype(jnp.bfloat16)
        st_own[h] = lax.dot_general(
            weighed,
            v_ref[h],
            (((0,), (0,)), ((), ())),
            preferred_element_type=jnp.float32,
        ).astype(jnp.bfloat16)

    state_y = [
        remote(st_own, st_y, (ssem.at[0], ssem.at[1]), y_next),
        remote(meta_ref, meta_y, (ssem.at[2], ssem.at[3]), y_next),
    ]
    for copy in state_y:
        copy.start()
    for chunk in range(3):
        y_weight(chunk).start()
    own_down.start()
    loads["q"].wait()

    def attend(h, i):
        span = (i + 1) * strip
        at = pl.ds(i * strip, strip)
        scores = lax.dot_general(
            q_ref[at, h * dk : (h + 1) * dk],
            k_ref[0:span, h * dk : (h + 1) * dk],
            (((1,), (1,)), ((), ())),
            preferred_element_type=jnp.float32,
        )
        log_weight = a_ref[h : h + 1, 0:span] - cols_ref[at, heads + h : heads + h + 1]
        row = i * strip + lax.broadcasted_iota(jnp.int32, (strip, span), 0)
        col = lax.broadcasted_iota(jnp.int32, (strip, span), 1)
        weight = jnp.where(col <= row, jnp.exp(jnp.minimum(log_weight, 0.0)), 0.0)
        num[at, h * dv : (h + 1) * dv] = jnp.dot(
            (scores * weight).astype(jnp.bfloat16),
            v_ref[h, 0:span, :],
            preferred_element_type=jnp.float32,
        )

    for h in range(heads):
        attend(h, 0)

    for copy in state_y:
        copy.wait_recv()
    first = y == 0
    meta_own, meta_other = meta_ref[...], meta_y[...]
    meta_0 = jnp.where(first, meta_own, meta_other)
    meta_1 = jnp.where(first, meta_other, meta_own)
    top_0 = meta_0[0:heads] + meta_1[heads : 2 * heads]
    top_1 = meta_1[0:heads]
    top = jnp.maximum(top_0, top_1)
    scale_0, scale_1 = jnp.exp(top_0 - top), jnp.exp(top_1 - top)
    scale_own = jnp.where(first, scale_0, scale_1)
    scale_other = jnp.where(first, scale_1, scale_0)
    meta_sum[...] = jnp.zeros_like(meta_sum)
    meta_sum[0:heads, :] = top
    meta_sum[heads : 2 * heads, :] = meta_0[heads : 2 * heads] + meta_1[heads : 2 * heads]
    for h in range(heads):
        st_sum[h] = (
            st_own[h].astype(jnp.float32) * scale_own[h : h + 1]
            + st_y[h].astype(jnp.float32) * scale_other[h : h + 1]
        ).astype(jnp.bfloat16)

    def state_z(step, summed):
        state, meta = (st_pre, meta_pre) if summed else (st_sum, meta_sum)
        to = on_plane(z + step)
        return [
            remote(state, st_z, (ssem.at[4], ssem.at[5]), to),
            remote(meta, meta_z, (ssem.at[6], ssem.at[7]), to),
        ]

    @pl.when(z == 0)
    def _():
        for copy in state_z(1, 0):
            copy.start()

    def hop():
        for copy in state_z(0, 0):
            copy.wait_recv()
        before, own = meta_z[0:heads, :] + meta_sum[heads : 2 * heads, :], meta_sum[0:heads, :]
        joint = jnp.maximum(before, own)
        meta_pre[...] = jnp.zeros_like(meta_pre)
        meta_pre[0:heads, :] = joint
        meta_pre[heads : 2 * heads, :] = meta_z[heads : 2 * heads, :] + meta_sum[heads : 2 * heads, :]
        scale_before, scale_own = jnp.exp(before - joint), jnp.exp(own - joint)
        for h in range(heads):
            st_pre[h] = (
                st_z[h].astype(jnp.float32) * scale_before[h : h + 1]
                + st_sum[h].astype(jnp.float32) * scale_own[h : h + 1]
            ).astype(jnp.bfloat16)
        for copy in state_z(1, 1):
            copy.start()

    z_send(1, ((0, z != 1), (1, True)))
    for h in range(heads):
        for i in range(1, 4):
            attend(h, i)

    pl.when(z == 1)(hop)
    z_send(1, ((0, z == 1),))

    def z_half(part):
        short_part = part_rows // 2
        start = pl.multiple_of((z * NY + 1 - y) * depth + part * short_part, short_part)
        piece = gu.at[pl.ds(start, short_part), :]
        return remote(piece, piece, (zs.at[0, 0, 0], zr.at[0, 0, 2]), on_plane(z + 1))

    y_weight(0).wait_recv()
    z_send(2, ((0, z < 2), (1, True)))

    @pl.when(z == 2)
    def _():
        z_half(0).start()
        hop()
        z_half(1).start()

    low = jnp.full((heads, meta_ref.shape[1]), LOWEST_LOG, jnp.float32)
    later = jnp.where(y == 1, meta_y[heads : 2 * heads, :], 0.0)
    lw_ref[1, 0:heads, :] = jnp.where(y == 1, meta_y[0:heads, :], low)

    @pl.when(z == last)
    def _():
        for copy in state_z(0, 0):
            copy.wait_recv()

    lw_ref[0, 0:heads, :] = jnp.where(z > 0, meta_z[0:heads, :] + later, low)
    ctop = jnp.maximum(lw_ref[0, 0:heads, :], lw_ref[1, 0:heads, :])
    ent[...] = jnp.zeros_like(ent)
    for source, valid in ((0, z > 0), (1, y == 1)):

        @pl.when(valid)
        def _():
            scale = jnp.exp(lw_ref[source, 0:heads, :] - ctop)
            for h in range(heads):
                part = st_y[h] if source else st_z[h]
                ent[h] += part.astype(jnp.float32) * scale[h : h + 1]

    for name in ("open0", "open1", "wo"):
        loads[name].wait()

    def front_core(i):
        at = pl.ds(pl.multiple_of(i * strip, strip), strip)
        return remote(
            pool.at[0:4, at, :], core_in.at[:, at, :], (fsem.at[8], fsem.at[i]), partner
        )

    def front_x(i):
        at = pl.ds(pl.multiple_of(i * strip, strip), strip)
        return remote(
            pool.at[8:10, at, :], x_in.at[:, at, :], (fsem.at[9], fsem.at[4 + i]), x_next
        )

    def gate_strip(i):
        at = pl.ds(pl.multiple_of(i * strip, strip), strip)
        gated = []
        for h in range(heads):
            lanes = slice(h * dv, (h + 1) * dv)
            before = jnp.dot(
                q_ref[at, h * dk : (h + 1) * dk],
                ent[h].astype(jnp.bfloat16),
                preferred_element_type=jnp.float32,
            )
            m_log = cols_ref[at, heads + h : heads + h + 1]
            m_all = jnp.maximum(m_log, ctop[h : h + 1, 0:1])
            memory = (
                num[at, lanes] * jnp.exp(m_log - m_all)
                + jnp.exp(ctop[h : h + 1, 0:1] - m_all) * before
            ) * dk ** (-0.5)
            normal = memory * lax.rsqrt(jnp.mean(memory * memory, axis=-1, keepdims=True) + EPSILON)
            opened = jax.nn.sigmoid(open_ref[h, at, :].astype(jnp.float32))
            gated.append((normal * gain_ref[lanes][None, :].astype(jnp.float32) * opened).astype(jnp.bfloat16))
        gated = jnp.concatenate(gated, axis=1)
        for chip in range(NX):
            for part in range(2):
                for mine in range(2):
                    core = c if mine else 1 - c
                    lanes = pl.ds(
                        pl.multiple_of((chip * 2 + core) * width + part * wide, wide), wide
                    )
                    pool[mine * 4 + chip * 2 + part, at, :] = jnp.dot(
                        gated, wo_ref[:, lanes], preferred_element_type=jnp.float32
                    ).astype(jnp.bfloat16)
        front_core(i).start()

    def core_sum(i):
        at = pl.ds(pl.multiple_of(i * strip, strip), strip)
        front_core(i).wait_recv()
        for part in range(2):
            far, near = (1 - x) * 2 + part, x * 2 + part
            pool[8 + part, at, :] = (
                pool[4 + far, at, :].astype(jnp.float32) + core_in[far, at, :].astype(jnp.float32)
            ).astype(jnp.bfloat16)
        front_x(i).start()

    @pl.loop(0, 5)
    def _(i):
        @pl.when(i < 4)
        def _():
            gate_strip(i)

        @pl.when(i == 2)
        def _():
            y_weight(1).wait_recv()
            z_send(3)

        @pl.when(i >= 1)
        def _():
            core_sum(i - 1)

    z_forward(1, 0)
    z_forward(1, 1)
    y_weight(2).wait_recv()
    own_down.wait()
    z_down(0, 0)
    for part in range(2):
        loads["resid" + str(part)].wait()

    def piece(owner_x, owner_c, owner_y, i):
        at = pl.multiple_of(owner_y * tokens + i * strip, strip)
        lanes = pl.multiple_of((owner_x * 2 + owner_c) * width, width)
        return rows_all.at[pl.ds(at, strip), pl.ds(lanes, width)]

    def to_x(i):
        part = piece(x, c, y, i)
        return remote(part, part, (gsem.at[16], gsem.at[i]), x_next)

    def to_y(kind, i):
        part = piece(x if kind == 0 else 1 - x, c, y, i)
        return remote(part, part, (gsem.at[17 + kind], gsem.at[4 + kind * 4 + i]), y_next)

    def to_core(kind, i):
        part = piece(
            x if kind % 2 == 0 else 1 - x, c, y if kind // 2 == 0 else 1 - y, i
        )
        return remote(part, part, (gsem.at[19 + kind], gsem.at[12 + kind]), partner)

    @pl.loop(0, 4)
    def _(i):
        at = pl.ds(pl.multiple_of(i * strip, strip), strip)
        front_x(i).wait_recv()
        start = pl.multiple_of(y * tokens + i * strip, strip)
        for part in range(2):
            lanes = slice(part * wide, (part + 1) * wide)
            near = x * 2 + part
            total = (
                pool[4 + near, at, :].astype(jnp.float32)
                + core_in[near, at, :].astype(jnp.float32)
                + x_in[part, at, :].astype(jnp.float32)
            )
            fresh = (resid_ref[part, at, :].astype(jnp.float32) + total).astype(jnp.bfloat16)
            out_ref[at, lanes] = fresh
            columns = pl.ds(pl.multiple_of(tp * width + part * wide, wide), wide)
            rows_all[pl.ds(start, strip), columns] = fresh
        to_x(i).start()
        to_y(0, i).start()
        to_core(0, i).start()

        @pl.when(i == 1)
        def _():
            z_forward(1, 2)

    z_forward(1, 3)
    z_down(1, 0)

    @pl.loop(0, 4)
    def _(i):
        to_x(i).wait_recv()
        to_y(1, i).start()
        to_core(1, i).start()
        to_y(0, i).wait_recv()
        to_core(2, i).start()

        @pl.when(i == 1)
        def _():
            z_forward(2, 0)
            z_forward(2, 1)

    z_forward(2, 2)
    z_down(1, 1)

    short = 128

    def norm_rows(owner, kinds):
        for kind in kinds:
            remote(whole_strip, whole_strip, (gsem.at[16], gsem.at[12 + kind]), partner).wait_recv()

        @pl.loop(0, tokens // short)
        def _(i):
            at = pl.ds(pl.multiple_of(owner * tokens + i * short, short), short)
            wide_rows = rows_all[at, :].astype(jnp.float32)
            scale = lax.rsqrt(jnp.mean(wide_rows * wide_rows, axis=-1, keepdims=True) + EPSILON)
            rows_all[at, :] = (wide_rows * scale * fgain_ref[...][None, :].astype(jnp.float32)).astype(
                jnp.bfloat16
            )

    @pl.loop(0, 4)
    def _(i):
        to_y(1, i).wait_recv()
        to_core(3, i).start()

    z_forward(2, 3)

    whole_strip = rows_all.at[pl.ds(0, tokens), pl.ds(0, width)]
    remote(pool.at[0:4], pool.at[0:4], (fsem.at[8], fsem.at[0]), partner).wait_send()
    remote(pool.at[8:10], pool.at[8:10], (fsem.at[9], fsem.at[4]), x_next).wait_send()
    for index in range(16, 23):
        remote(whole_strip, whole_strip, (gsem.at[index], gsem.at[0]), partner).wait_send()

    norm_rows(y, (0, 1))
    norm_rows(1 - y, (2, 3))

    tall = 512
    plane_rows = NY * depth
    early = last * plane_rows
    early_at = jnp.where(z == last, plane_rows, 0)
    late_at = jnp.where(z == last, 0, early)

    def gate_up(i, start, size):
        at = pl.ds(pl.multiple_of(i * tall, tall), tall)
        taken = pl.ds(pl.multiple_of(start, plane_rows), size)
        return at, jnp.dot(rows_all[at, taken], gu[taken, :], preferred_element_type=jnp.float32)

    def gu_arrived(dist):
        for way in range(2):

            @pl.when(jnp.logical_and(has_origin(way, dist), jnp.logical_not(has_next(way))))
            def _():
                for chunk in range(4):
                    z_arrival(way, dist, chunk).wait_recv()

    for dist in range(1, last):
        gu_arrived(dist)

    @pl.loop(0, NY * tokens // tall)
    def _(i):
        at, product = gate_up(i, early_at, early)
        sums[at, :] = product

    z_down(2, 1)
    z_down(2, 0)
    gu_arrived(last)

    def finish_hidden(i):
        at, product = gate_up(i, late_at, plane_rows)
        both = sums[at, :] + product
        hid[at, :] = (jax.nn.silu(both[:, :half]) * both[:, half:]).astype(jnp.bfloat16)

    @pl.loop(0, NY)
    def _(i):
        finish_hidden(i * (tokens // tall))


    units = planes * NY * PIECES
    rows = tokens // PIECES

    def side_of(unit):
        return unit // PIECES % NY

    def place(unit):
        step = unit // (PIECES * NY)
        return (z // 2 + step % 2) % 2 * 2 + (z % 2 + step // 2) % 2

    def slot(unit):
        return unit // (PIECES * NY) % 2 * 2 + side_of(unit)

    def kept_index(unit):
        return slot(unit) * PIECES + unit % PIECES

    def strip_of(unit):
        return pl.ds(pl.multiple_of(unit % PIECES * rows, rows), rows)

    def held(unit, top_row):
        return unit // PIECES * 2 + top_row, strip_of(unit)

    def both_of(unit):
        return pool.at[pl.ds(unit // PIECES * 2, 2), strip_of(unit)]

    def back_core(unit):
        kept = core_back.at[slot(unit), :, strip_of(unit)]
        return remote(both_of(unit), kept, (bsem.at[0], bsem.at[3 + kept_index(unit)]), partner)

    def back_y(unit):
        kept = y_back.at[slot(unit), strip_of(unit)]
        return remote(pool.at[held(unit, 1 - y)], kept, (bsem.at[1], bsem.at[3 + 4 * PIECES + kept_index(unit)]), y_next)

    def back_x(unit):
        kept = x_back.at[side_of(unit), strip_of(unit)]
        return remote(pool.at[held(unit, y)], kept, (bsem.at[2], bsem.at[3 + 8 * PIECES + unit % (2 * PIECES)]), x_next)

    def keeps(unit):
        return place(unit) % 2 == c

    def owns(unit):
        return place(unit) == tp

    def passes(unit):
        return jnp.logical_and(keeps(unit), place(unit) // 2 != x)

    def add(unit, top_row, other):
        at = held(unit, top_row)
        pool[at] = (pool[at].astype(jnp.float32) + other.astype(jnp.float32)).astype(jnp.bfloat16)

    def down_part(unit):
        step, side = unit // (PIECES * NY), side_of(unit)
        ends = jnp.logical_or(z == 0, z == last)

        @pl.when(jnp.logical_and(jnp.logical_and(step > 0, unit % PIECES == 0), ends))
        def _():
            at = place(unit)
            way = jnp.where(z == 0, 1, 0)
            dist = jnp.where(z == 0, at, z - at)
            part = dn.at[at * NY + side]
            remote(part, part, (zs.at[way, 0, 0], zr.at[way, dist - 1, 4 + side]), on_plane(z)).wait_recv()

        weight = dn[place(unit) * NY + side]
        for top_row in (1 - y, y):
            start = pl.multiple_of(top_row * tokens + unit % PIECES * rows, rows)
            pool[held(unit, top_row)] = jnp.dot(
                hid[pl.ds(start, rows), :], weight, preferred_element_type=jnp.float32
            ).astype(jnp.bfloat16)

        @pl.when(jnp.logical_not(keeps(unit)))
        def _():
            back_core(unit).start()

    def after_core(unit):
        @pl.when(keeps(unit))
        def _():
            back_core(unit).wait_recv()
            for top_row in (1 - y, y):
                add(unit, top_row, core_back[slot(unit), top_row, strip_of(unit)])
            back_y(unit).start()

    def after_y(unit):
        @pl.when(keeps(unit))
        def _():
            back_y(unit).wait_recv()
            add(unit, y, y_back[slot(unit), strip_of(unit)])

        @pl.when(passes(unit))
        def _():
            back_x(unit).start()

    def finish(unit, other):
        at = strip_of(unit)
        lanes = pl.ds(pl.multiple_of(side_of(unit) * wide, wide), wide)
        total = pool[held(unit, y)].astype(jnp.float32) + other.astype(jnp.float32)
        out_ref[at, lanes] = (out_ref[at, lanes].astype(jnp.float32) + 0.5 * total).astype(out_ref.dtype)

    def after_x(unit):
        @pl.when(owns(unit))
        def _():
            back_x(unit).wait_recv()
            finish(unit, x_back[side_of(unit), strip_of(unit)])

    def run(low, high, begun=0, trail=0):
        @pl.loop(low, high + 1)
        def _(i):
            @pl.when(jnp.logical_and(i >= begun, i < high))
            def _():
                down_part(i)

            @pl.when(i > low)
            def _():
                after_core(i - 1)

            if trail:

                @pl.when(i < high - 1)
                def _():
                    after_y(i - trail)

    def each(stage, low, high):
        @pl.loop(low, high)
        def _(i):
            stage(i)


    def at_ends(low, high):
        @pl.when(ends)
        def _():
            run(low, high)

    begun = tall // rows

    @pl.loop(0, begun)
    def _(i):
        down_part(i)

    @pl.loop(0, NY)
    def _(i):
        finish_hidden(i * (tokens // tall) + 1)

    run(0, 8, begun)
    z_down(2, 2)
    run(8, 16)

    @pl.when(jnp.logical_not(ends))
    def _():
        run(16, units)

    each(after_y, 0, 8)
    at_ends(16, 20)
    each(after_y, 8, 12)
    at_ends(20, 24)
    each(after_y, 12, 20)
    at_ends(24, 28)
    each(after_y, 20, 24)
    each(after_y, units - 2 * PIECES, units - 2 * PIECES + 1)

    @pl.when(ends)
    def _():
        run(units - PIECES, units, 0, PIECES - 1)

    @pl.when(jnp.logical_not(ends))
    def _():
        each(after_y, units - 2 * PIECES + 1, units - PIECES)

    each(after_y, units - PIECES, units)
    def sent(part, sem, to):
        remote(part, part, (sem, zr.at[0, 0, 0]), to).wait_send()

    sent(core_back, bsem.at[0], partner)
    sent(y_back, bsem.at[1], y_next)
    sent(x_back, bsem.at[2], x_next)
    for chunk in range(3):
        y_weight(chunk).wait_send()
    for copy in state_y:
        copy.wait_send()

    @pl.when(z == 0)
    def _():
        for copy in state_z(1, 0):
            copy.wait_send()

    @pl.when(jnp.logical_and(z > 0, z < last))
    def _():
        for copy in state_z(1, 1):
            copy.wait_send()

    for way in range(2):
        for dist in range(planes - 1):

            @pl.when(jnp.logical_and(has_origin(way, dist), has_next(way)))
            def _():
                sent(gu.at[pl.ds(0, plane_rows), :], zs.at[way, dist, 0], partner)
                sent(dn.at[pl.ds(0, NY)], zs.at[way, dist, 1], partner)

    each(after_x, 0, units)


def plane_layer(
    planes,
    queries,
    cell_key_rows,
    cell_value_rows,
    output_gate_logits,
    input_gate_logits,
    forget_gate_logits,
    forget_extra_term,
    residual,
    head_norm_gain,
    cell_output_weight,
    feedforward_norm_gain,
    gate_projection_weight,
    up_projection_weight,
    down_projection_weight,
):
    tokens, heads = queries.shape[0], input_gate_logits.shape[0]
    width = residual.shape[1]
    model = cell_output_weight.shape[1]
    depth, hidden = gate_projection_weight.shape
    half = hidden // NY
    dk, dv = queries.shape[1] // heads, cell_value_rows.shape[1] // heads
    bf16, f32 = jnp.bfloat16, jnp.float32
    vmem, dma = pltpu.VMEM, pltpu.SemaphoreType.DMA
    scratch = [
        vmem((heads, tokens), input_gate_logits.dtype),
        vmem((heads, tokens), forget_gate_logits.dtype),
        vmem((heads, tokens), forget_extra_term.dtype),
        vmem((heads * dv,), head_norm_gain.dtype),
        vmem((model,), feedforward_norm_gain.dtype),
        vmem((depth, hidden), bf16),
        vmem((depth, hidden), bf16),
        vmem((heads * dv, model), bf16),
        vmem((8, tokens), f32),
        vmem((tokens, 8), f32),
        vmem((8, dv), f32),
        vmem((model, hidden), bf16),
        vmem((planes * NY, half, depth), bf16),
        vmem((NY * tokens, 2 * NX * width), bf16),
        vmem((NY * tokens, half), bf16),
        vmem((NY * tokens, hidden), f32),
        vmem((depth, hidden), bf16),
        vmem((tokens, heads * dv), f32),
        vmem((heads, dk, dv), f32),
        vmem((heads, dk, dv), bf16),
        vmem((heads, dk, dv), bf16),
        vmem((heads, dk, dv), bf16),
        vmem((heads, dk, dv), bf16),
        vmem((heads, dk, dv), bf16),
        vmem((8, dv), f32),
        vmem((8, dv), f32),
        vmem((8, dv), f32),
        vmem((8, dv), f32),
        vmem((2, 8, dv), f32),
        vmem((2 * planes * NY, tokens, width // 2), bf16),
        vmem((4, tokens, width // 2), bf16),
        vmem((2, tokens, width // 2), bf16),
        vmem((planes * NY // 2, 2, tokens, width // 2), bf16),
        vmem((planes * NY // 2, tokens, width // 2), bf16),
        vmem((2, tokens, width // 2), bf16),
        dma((2, planes - 1, 2)),
        dma((2, planes - 1, 6)),
        dma((2, 3)),
        dma((8,)),
        dma((10,)),
        dma((23,)),
        dma((3 + 10 * PIECES,)),
        dma((17,)),
    ]
    whole = pl.BlockSpec(memory_space=pltpu.VMEM)
    far = pl.BlockSpec(memory_space=pl.ANY)
    return pl.pallas_call(
        functools.partial(block_body, planes),
        out_shape=pltpu.VMEM((tokens, width), bf16),
        in_specs=[far] * 14,
        out_specs=whole,
        scratch_shapes=scratch,
        compiler_params=pltpu.CompilerParams(
            collective_id=0, has_side_effects=True, vmem_limit_bytes=65000000
        ),
        cost_estimate=pl.CostEstimate(flops=22 * 10**9, bytes_accessed=10**7, transcendentals=0),
        name="block",
    )(
        queries,
        cell_key_rows,
        cell_value_rows,
        output_gate_logits,
        input_gate_logits,
        forget_gate_logits,
        forget_extra_term,
        residual,
        head_norm_gain,
        cell_output_weight,
        feedforward_norm_gain,
        gate_projection_weight,
        up_projection_weight,
        down_projection_weight,
    )


def layer(rows, columns, *arrays):
    if columns == 2 * NX and rows == 4 * NY:
        return plane_layer(rows // NY, *arrays)
    return general(*arrays)


def solution(mesh):
    placed = (
        P("sp", "tp"),
        P("sp", "tp"),
        P("sp", "tp"),
        P("sp", "tp"),
        P("tp", "sp"),
        P("tp", "sp"),
        P("tp", "sp"),
        P("sp", "tp"),
        P("tp"),
        P("tp", None),
        P(),
        P("sp", "tp"),
        P("sp", "tp"),
        P("tp", "sp"),
    )
    return jax.shard_map(
        functools.partial(layer, mesh.shape["sp"], mesh.shape["tp"]), mesh=mesh, in_specs=placed, out_specs=P("sp", "tp"), check_vma=False
    )
```

```python
import functools

import jax
import jax.numpy as jnp
from jax import lax
from jax.experimental import pallas as pl
from jax.experimental.pallas import tpu as pltpu
from jax.sharding import PartitionSpec as P

LOWEST_LOG = -1e30
EPSILON = 1e-06


def shift_pairs(length, step):
    return [(source, source + step) for source in range(length - step)]


def entering_state(state, top, total):
    length, index = lax.axis_size("sp"), lax.axis_index("sp")
    heads, key_width, value_width = state.shape

    def pack(s, t, f):
        tail = jnp.zeros((heads, 8, value_width), jnp.float32)
        tail = tail.at[:, 0, :].set(t[:, None]).at[:, 1, :].set(f[:, None])
        return jnp.concatenate([s, tail], axis=1)

    def unpack(p, valid):
        s = p[:, :key_width, :]
        t = jnp.where(valid, p[:, key_width, 0], LOWEST_LOG)
        f = jnp.where(valid, p[:, key_width + 1, 0], 0.0)
        return jnp.where(valid, s, 0.0), t, f

    moved = lax.ppermute(pack(state, top, total), "sp", shift_pairs(length, 1))
    s, t, f = unpack(moved, index >= 1)
    step = 1
    while step < length - 1:
        moved = lax.ppermute(pack(s, t, f), "sp", shift_pairs(length, step))
        s0, t0, f0 = unpack(moved, index >= step)
        from_top = t0 + f
        new_top = jnp.maximum(from_top, t)
        s = (
            jnp.exp(from_top - new_top)[:, None, None] * s0
            + jnp.exp(t - new_top)[:, None, None] * s
        )
        t, f = new_top, f0 + f
        step *= 2
    return s, t


def cell_kernel(q_ref, k_ref, v_ref, a_ref, m_ref, c_ref, state_ref, open_ref, gain_ref, o_ref, *, scale):
    block = q_ref.shape[0]
    length = k_ref.shape[0]
    q = q_ref[...]
    first = pl.program_id(1) * block
    scores = lax.dot_general(
        q, k_ref[...], (((1,), (1,)), ((), ())), preferred_element_type=jnp.float32
    )
    rows = first + lax.broadcasted_iota(jnp.int32, (block, length), 0)
    cols = lax.broadcasted_iota(jnp.int32, (block, length), 1)
    weight = jnp.where(cols <= rows, jnp.exp(jnp.minimum(a_ref[0] - m_ref[0], 0.0)), 0.0)
    numer = jnp.dot(
        (scores * weight).astype(jnp.bfloat16), v_ref[...], preferred_element_type=jnp.float32
    )
    before = jnp.dot(q, state_ref[0].astype(jnp.bfloat16), preferred_element_type=jnp.float32)
    memory = (numer + c_ref[0] * before) * scale
    normal = memory * lax.rsqrt(jnp.mean(memory * memory, axis=-1, keepdims=True) + EPSILON)
    gate_open = jax.nn.sigmoid(open_ref[...].astype(jnp.float32))
    o_ref[...] = (normal * gain_ref[...].astype(jnp.float32) * gate_open).astype(o_ref.dtype)


def cell(queries, keys, values, a_log, m_col, c_col, state, open_logits, gain):
    heads, length = a_log.shape
    dk, dv = queries.shape[1] // heads, values.shape[1] // heads
    block = min(length, 256)
    return pl.pallas_call(
        lambda *refs: cell_kernel(*refs, scale=dk ** (-0.5)),
        grid=(heads, length // block),
        in_specs=[
            pl.BlockSpec((block, dk), lambda h, i: (i, h)),
            pl.BlockSpec((length, dk), lambda h, i: (0, h)),
            pl.BlockSpec((length, dv), lambda h, i: (0, h)),
            pl.BlockSpec((1, 1, length), lambda h, i: (h, 0, 0)),
            pl.BlockSpec((1, block, 1), lambda h, i: (h, i, 0)),
            pl.BlockSpec((1, block, 1), lambda h, i: (h, i, 0)),
            pl.BlockSpec((1, dk, dv), lambda h, i: (h, 0, 0)),
            pl.BlockSpec((block, dv), lambda h, i: (i, h)),
            pl.BlockSpec((1, dv), lambda h, i: (0, h)),
        ],
        out_specs=pl.BlockSpec((block, dv), lambda h, i: (i, h)),
        out_shape=jax.ShapeDtypeStruct((length, heads * dv), jnp.bfloat16),
        cost_estimate=pl.CostEstimate(
            flops=8 * heads * length * length * dv, bytes_accessed=6 * length * heads * dv, transcendentals=0
        ),
        name="cell",
    )(queries, keys, values, a_log[:, None, :], m_col[:, :, None], c_col[:, :, None], state, open_logits, gain)


def partner_pairs(count):
    return [(i, i ^ 1) for i in range(count)]


def ring_pairs(count, step):
    return [(i, (i + 2 * step) % count) for i in range(count)]


def product_scattered(rows, weight):
    count, index = lax.axis_size("tp"), lax.axis_index("tp")
    chips, core, chip = count // 2, index % 2, index // 2
    width = weight.shape[1] // count

    def product(block):
        columns = lax.dynamic_slice_in_dim(weight, block * width, width, 1)
        return jnp.dot(rows, columns, preferred_element_type=jnp.float32)

    def chip_sum(to):
        given = product(2 * to + 1 - core).astype(jnp.bfloat16)
        got = lax.ppermute(given, "tp", partner_pairs(count))
        return product(2 * to + core) + got.astype(jnp.float32)

    moved = []
    for step in range(1, chips):
        sent = chip_sum((chip + step) % chips).astype(jnp.bfloat16)
        moved.append(lax.ppermute(sent, "tp", ring_pairs(count, step)))
    total = chip_sum(chip)
    for part in moved:
        total = total + part.astype(jnp.float32)
    return total


def columns_gathered(block):
    count, index = lax.axis_size("tp"), lax.axis_index("tp")
    chips, core, chip = count // 2, index % 2, index // 2
    width = block.shape[1]
    whole = jnp.zeros((block.shape[0], count * width), block.dtype)
    held = [(chip, block)]
    for step in range(1, chips):
        moved = lax.ppermute(block, "tp", ring_pairs(count, step))
        held.append(((chip - step) % chips, moved))
    for place, piece in held:
        other = lax.ppermute(piece, "tp", partner_pairs(count))
        whole = lax.dynamic_update_slice(whole, piece, (0, (2 * place + core) * width))
        whole = lax.dynamic_update_slice(whole, other, (0, (2 * place + 1 - core) * width))
    return whole


def general(
    queries,
    cell_key_rows,
    cell_value_rows,
    output_gate_logits,
    input_gate_logits,
    forget_gate_logits,
    forget_extra_term,
    residual,
    head_norm_gain,
    cell_output_weight,
    feedforward_norm_gain,
    gate_projection_weight,
    up_projection_weight,
    down_projection_weight,
):
    whole_gate = lax.all_gather(gate_projection_weight, "sp", axis=0, tiled=True)
    whole_up = lax.all_gather(up_projection_weight, "sp", axis=0, tiled=True)
    length = queries.shape[0]
    heads = input_gate_logits.shape[0]
    dk, dv = queries.shape[1] // heads, cell_value_rows.shape[1] // heads
    log_forget = jax.nn.log_sigmoid(forget_gate_logits.astype(jnp.float32)) + forget_extra_term
    running = jnp.cumsum(log_forget, axis=-1)
    a_log = input_gate_logits.astype(jnp.float32) - running
    m_log = lax.cummax(a_log, axis=1)
    a_top, total = m_log[:, -1], running[:, -1]
    decay = jnp.exp(a_log - a_top[:, None])
    weighed = (
        cell_key_rows.reshape(length, heads, dk).astype(jnp.float32) * decay.T[:, :, None]
    ).astype(jnp.bfloat16)
    state = jnp.stack(
        [
            lax.dot_general(
                weighed[:, h],
                cell_value_rows[:, h * dv : (h + 1) * dv],
                (((0,), (0,)), ((), ())),
                preferred_element_type=jnp.float32,
            )
            for h in range(heads)
        ]
    )
    carried, carried_top = entering_state(state, a_top + total, total)
    m_all = jnp.maximum(m_log, carried_top[:, None])
    coefficient = jnp.exp(carried_top[:, None] - m_all)
    gated = cell(
        queries,
        cell_key_rows,
        cell_value_rows,
        a_log,
        m_all,
        coefficient,
        carried,
        output_gate_logits,
        head_norm_gain[None, :],
    )
    summed = product_scattered(gated, cell_output_weight)
    stream = (residual.astype(jnp.float32) + summed).astype(jnp.bfloat16)
    down_late, stream = lax.optimization_barrier((down_projection_weight, stream))
    whole_down = lax.all_gather(down_late, "sp", axis=1, tiled=True)
    wide = columns_gathered(stream).astype(jnp.float32)
    scale = lax.rsqrt(jnp.mean(wide * wide, axis=-1, keepdims=True) + EPSILON)
    normed = (wide * scale * feedforward_norm_gain.astype(jnp.float32)[None, :]).astype(jnp.bfloat16)
    gate_value = jnp.dot(normed, whole_gate, preferred_element_type=jnp.float32)
    lifted = jnp.dot(normed, whole_up, preferred_element_type=jnp.float32)
    hidden = (jax.nn.silu(gate_value) * lifted).astype(jnp.bfloat16)
    channel_total = product_scattered(hidden, whole_down)
    return (stream.astype(jnp.float32) + 0.5 * channel_total).astype(jnp.bfloat16)


NX, NY = 2, 2
PIECES = 4
BY_NAME = pl.DeviceIdType.MESH


def block_body(
    planes,
    q_in,
    k_in,
    v_in,
    open_in,
    input_far,
    forget_far,
    extra_far,
    resid_in,
    gain_far,
    wo_in,
    fgain_far,
    gate_in,
    up_in,
    down_ref,
    out_ref,
    input_in,
    forget_in,
    extra_in,
    gain_ref,
    fgain_ref,
    gate_ref,
    up_ref,
    wo_ref,
    a_ref,
    cols_ref,
    meta_ref,
    gu,
    dn,
    rows_all,
    hid,
    sums,
    gu_out,
    num,
    ent,
    st_own,
    st_y,
    st_sum,
    st_pre,
    st_z,
    meta_y,
    meta_sum,
    meta_pre,
    meta_z,
    lw_ref,
    pool,
    core_in,
    x_in,
    core_back,
    y_back,
    x_back,
    zs,
    zr,
    ysem,
    ssem,
    fsem,
    gsem,
    bsem,
    lsem,
):
    sp, tp = lax.axis_index("sp"), lax.axis_index("tp")
    z, y, x, c = sp // NY, sp % NY, tp // 2, tp % 2
    tokens, heads = q_in.shape[0], input_in.shape[0]
    dk, dv = q_in.shape[1] // heads, v_in.shape[1] // heads
    width = resid_in.shape[1]
    depth, hidden = gate_ref.shape
    half = hidden // NY
    count = 2 * NX
    last = planes - 1
    strip = tokens // 4
    wide = width // 2
    part_rows = depth // 2

    partner = {"tp": tp + 1 - 2 * c}
    x_next = {"tp": (1 - x) * 2 + c}
    y_next = {"sp": z * NY + 1 - y}

    def on_plane(at):
        return {"sp": at * NY + y}

    def remote(src, dst, sems, to):
        return pltpu.make_async_remote_copy(
            src_ref=src, dst_ref=dst, send_sem=sems[0], recv_sem=sems[1], device_id=to, device_id_type=BY_NAME
        )

    q_ref, k_ref = core_back.at[0, 0], core_back.at[0, 1]
    v_ref, open_ref, resid_ref = core_back.at[1], core_back.at[2], core_back.at[3]
    loads = {}
    wanted = [
        ("gate", gate_in, gate_ref),
        ("up", up_in, up_ref),
        ("forget", forget_far, forget_in),
        ("extra", extra_far, extra_in),
        ("input", input_far, input_in),
        ("gain", gain_far, gain_ref),
        ("fgain", fgain_far, fgain_ref),
        ("k", k_in, k_ref),
    ]
    for name, source, kept in (("v", v_in, v_ref), ("q", q_in, q_ref), ("open", open_in, open_ref)):
        if name == "q":
            wanted.append((name, source, kept))
        else:
            for part in range(2):
                wanted.append((name + str(part), source.at[:, part * wide : (part + 1) * wide], kept.at[part]))
    wanted.append(("wo", wo_in, wo_ref))
    for part in range(2):
        wanted.append(("resid" + str(part), resid_in.at[:, part * wide : (part + 1) * wide], resid_ref.at[part]))
    for index, (name, source, kept) in enumerate(wanted):
        loads[name] = pltpu.make_async_copy(source, kept, lsem.at[index + 1])
        loads[name].start()

    barrier = pltpu.get_barrier_semaphore()
    for to in (partner, x_next, y_next):
        pl.semaphore_signal(barrier, inc=1, device_id=to, device_id_type=BY_NAME)
    for ok, at in ((z > 0, z - 1), (z < last, z + 1)):

        @pl.when(ok)
        def _():
            pl.semaphore_signal(barrier, inc=1, device_id=on_plane(at), device_id_type=BY_NAME)

    ends = jnp.logical_or(z == 0, z == last)
    pl.semaphore_wait(barrier, 5 - jnp.where(ends, 1, 0))

    loads["gate"].wait()
    loads["up"].wait()

    for mine in range(NY):

        @pl.when(y == mine)
        def _():
            own = pl.ds(pl.multiple_of(sp * depth, depth), depth)
            here, there = mine * half, (1 - mine) * half
            gu_out[:, 0:half] = gate_ref[:, there : there + half]
            gu_out[:, half : 2 * half] = up_ref[:, there : there + half]
            gu[own, 0:half] = gate_ref[:, here : here + half]
            gu[own, half : 2 * half] = up_ref[:, here : here + half]

    def gu_rows(at, chunk):
        side = (y + chunk // 2) % 2
        start = (at * NY + side) * depth + (chunk % 2) * part_rows
        return pl.ds(pl.multiple_of(start, part_rows), part_rows)

    def z_copy(way, dist, chunk):
        at = z - dist if way == 0 else z + dist
        to = z + 1 if way == 0 else z - 1
        sems = (zs.at[way, dist, chunk // 4], zr.at[way, dist, chunk])
        if chunk < 4:
            part = gu.at[gu_rows(at, chunk), :]
        else:
            part = dn.at[at * NY + chunk - 4]
        return remote(part, part, sems, on_plane(to))

    def z_arrival(way, dist, chunk):
        at = z - dist if way == 0 else z + dist
        sems = (zs.at[way, 0, 0], zr.at[way, dist - 1, chunk])
        if chunk < 4:
            part = gu.at[gu_rows(at, chunk), :]
        else:
            part = dn.at[at * NY + chunk - 4]
        return remote(part, part, sems, on_plane(z))

    def has_next(way):
        return z < last if way == 0 else z > 0

    def has_origin(way, dist):
        return z >= dist if way == 0 else z + dist <= last

    def z_send(chunk, ways=((0, True), (1, True))):
        for way, also in ways:

            @pl.when(jnp.logical_and(has_next(way), also))
            def _():
                z_copy(way, 0, chunk).start()

    def z_forward(dist, chunk):
        for way in range(2):

            @pl.when(jnp.logical_and(has_origin(way, dist), has_next(way)))
            def _():
                z_arrival(way, dist, chunk).wait_recv()
                z_copy(way, dist, chunk).start()

    def z_down(rank, dist):
        for way in range(2):

            @pl.when(z == (rank if way == 0 else last - rank))
            def _():
                for chunk in (4, 5):
                    if dist:
                        z_arrival(way, dist, chunk).wait_recv()
                    z_copy(way, dist, chunk).start()

    def y_rows(owner, chunk):
        start = (z * NY + owner) * depth + chunk * part_rows
        return pl.ds(pl.multiple_of(start, part_rows), part_rows)

    def y_weight(chunk):
        sems = (ysem.at[0, chunk], ysem.at[1, chunk])
        if chunk < 2:
            return remote(
                gu_out.at[pl.ds(chunk * part_rows, part_rows), :], gu.at[y_rows(y, chunk), :], sems, y_next
            )
        start = pl.multiple_of((1 - y) * half, half)
        return remote(down_ref.at[pl.ds(start, half), :], dn.at[sp], sems, y_next)

    own_down = pltpu.make_async_copy(
        down_ref.at[pl.ds(pl.multiple_of(y * half, half), half), :], dn.at[sp], lsem.at[0]
    )
    z_send(0)

    def padded(rows):
        return jnp.concatenate([rows, jnp.zeros((8 - heads, tokens), jnp.float32)], axis=0)

    for name in ("forget", "extra", "input", "gain", "fgain"):
        loads[name].wait()
    lane = lax.broadcasted_iota(jnp.int32, (8, tokens), 1)
    logits = forget_in[...].astype(jnp.float32)
    running = padded(
        jnp.minimum(logits, 0.0) - jnp.log1p(jnp.exp(-jnp.abs(logits))) + extra_in[...]
    )
    step = 1
    while step < tokens:
        running = running + jnp.where(lane >= step, pltpu.roll(running, step, 1), 0.0)
        step *= 2
    a_log = padded(input_in[...].astype(jnp.float32)) - running
    m_log = a_log
    step = 1
    while step < tokens:
        m_log = jnp.maximum(m_log, jnp.where(lane >= step, pltpu.roll(m_log, step, 1), LOWEST_LOG))
        step *= 2
    a_ref[...] = a_log
    a_top, total = m_log[:, tokens - 1 :], running[:, tokens - 1 :]
    decay = jnp.exp(a_log - a_top)
    cols_ref[...] = jnp.concatenate(
        [decay[0:heads], m_log[0:heads], jnp.zeros((8 - 2 * heads, tokens), jnp.float32)], axis=0
    ).T
    meta_ref[...] = jnp.zeros_like(meta_ref)
    meta_ref[0:heads, :] = jnp.broadcast_to((a_top + total)[0:heads], (heads, meta_ref.shape[1]))
    meta_ref[heads : 2 * heads, :] = jnp.broadcast_to(total[0:heads], (heads, meta_ref.shape[1]))
    for name in ("k", "v0", "v1"):
        loads[name].wait()

    for h in range(heads):
        weighed = (
            k_ref[:, h * dk : (h + 1) * dk].astype(jnp.float32) * cols_ref[:, h : h + 1]
        ).astype(jnp.bfloat16)
        st_own[h] = lax.dot_general(
            weighed,
            v_ref[h],
            (((0,), (0,)), ((), ())),
            preferred_element_type=jnp.float32,
        ).astype(jnp.bfloat16)

    state_y = [
        remote(st_own, st_y, (ssem.at[0], ssem.at[1]), y_next),
        remote(meta_ref, meta_y, (ssem.at[2], ssem.at[3]), y_next),
    ]
    for copy in state_y:
        copy.start()
    for chunk in range(3):
        y_weight(chunk).start()
    own_down.start()
    loads["q"].wait()

    def attend(h, i):
        span = (i + 1) * strip
        at = pl.ds(i * strip, strip)
        scores = lax.dot_general(
            q_ref[at, h * dk : (h + 1) * dk],
            k_ref[0:span, h * dk : (h + 1) * dk],
            (((1,), (1,)), ((), ())),
            preferred_element_type=jnp.float32,
        )
        log_weight = a_ref[h : h + 1, 0:span] - cols_ref[at, heads + h : heads + h + 1]
        row = i * strip + lax.broadcasted_iota(jnp.int32, (strip, span), 0)
        col = lax.broadcasted_iota(jnp.int32, (strip, span), 1)
        weight = jnp.where(col <= row, jnp.exp(jnp.minimum(log_weight, 0.0)), 0.0)
        num[at, h * dv : (h + 1) * dv] = jnp.dot(
            (scores * weight).astype(jnp.bfloat16),
            v_ref[h, 0:span, :],
            preferred_element_type=jnp.float32,
        )

    for h in range(heads):
        attend(h, 0)

    for copy in state_y:
        copy.wait_recv()
    first = y == 0
    meta_own, meta_other = meta_ref[...], meta_y[...]
    meta_0 = jnp.where(first, meta_own, meta_other)
    meta_1 = jnp.where(first, meta_other, meta_own)
    top_0 = meta_0[0:heads] + meta_1[heads : 2 * heads]
    top_1 = meta_1[0:heads]
    top = jnp.maximum(top_0, top_1)
    scale_0, scale_1 = jnp.exp(top_0 - top), jnp.exp(top_1 - top)
    scale_own = jnp.where(first, scale_0, scale_1)
    scale_other = jnp.where(first, scale_1, scale_0)
    meta_sum[...] = jnp.zeros_like(meta_sum)
    meta_sum[0:heads, :] = top
    meta_sum[heads : 2 * heads, :] = meta_0[heads : 2 * heads] + meta_1[heads : 2 * heads]
    for h in range(heads):
        st_sum[h] = (
            st_own[h].astype(jnp.float32) * scale_own[h : h + 1]
            + st_y[h].astype(jnp.float32) * scale_other[h : h + 1]
        ).astype(jnp.bfloat16)

    def state_z(step, summed):
        state, meta = (st_pre, meta_pre) if summed else (st_sum, meta_sum)
        to = on_plane(z + step)
        return [
            remote(state, st_z, (ssem.at[4], ssem.at[5]), to),
            remote(meta, meta_z, (ssem.at[6], ssem.at[7]), to),
        ]

    @pl.when(z == 0)
    def _():
        for copy in state_z(1, 0):
            copy.start()

    def hop():
        for copy in state_z(0, 0):
            copy.wait_recv()
        before, own = meta_z[0:heads, :] + meta_sum[heads : 2 * heads, :], meta_sum[0:heads, :]
        joint = jnp.maximum(before, own)
        meta_pre[...] = jnp.zeros_like(meta_pre)
        meta_pre[0:heads, :] = joint
        meta_pre[heads : 2 * heads, :] = meta_z[heads : 2 * heads, :] + meta_sum[heads : 2 * heads, :]
        scale_before, scale_own = jnp.exp(before - joint), jnp.exp(own - joint)
        for h in range(heads):
            st_pre[h] = (
                st_z[h].astype(jnp.float32) * scale_before[h : h + 1]
                + st_sum[h].astype(jnp.float32) * scale_own[h : h + 1]
            ).astype(jnp.bfloat16)
        for copy in state_z(1, 1):
            copy.start()

    z_send(1, ((0, z != 1), (1, True)))
    for h in range(heads):
        for i in range(1, 4):
            attend(h, i)

    pl.when(z == 1)(hop)
    z_send(1, ((0, z == 1),))

    def z_half(part):
        short_part = part_rows // 2
        start = pl.multiple_of((z * NY + 1 - y) * depth + part * short_part, short_part)
        piece = gu.at[pl.ds(start, short_part), :]
        return remote(piece, piece, (zs.at[0, 0, 0], zr.at[0, 0, 2]), on_plane(z + 1))

    y_weight(0).wait_recv()
    z_send(2, ((0, z < 2), (1, True)))

    @pl.when(z == 2)
    def _():
        z_half(0).start()
        hop()
        z_half(1).start()

    low = jnp.full((heads, meta_ref.shape[1]), LOWEST_LOG, jnp.float32)
    later = jnp.where(y == 1, meta_y[heads : 2 * heads, :], 0.0)
    lw_ref[1, 0:heads, :] = jnp.where(y == 1, meta_y[0:heads, :], low)

    @pl.when(z == last)
    def _():
        for copy in state_z(0, 0):
            copy.wait_recv()

    lw_ref[0, 0:heads, :] = jnp.where(z > 0, meta_z[0:heads, :] + later, low)
    ctop = jnp.maximum(lw_ref[0, 0:heads, :], lw_ref[1, 0:heads, :])
    ent[...] = jnp.zeros_like(ent)
    for source, valid in ((0, z > 0), (1, y == 1)):

        @pl.when(valid)
        def _():
            scale = jnp.exp(lw_ref[source, 0:heads, :] - ctop)
            for h in range(heads):
                part = st_y[h] if source else st_z[h]
                ent[h] += part.astype(jnp.float32) * scale[h : h + 1]

    for name in ("open0", "open1", "wo"):
        loads[name].wait()

    def front_core(i):
        at = pl.ds(pl.multiple_of(i * strip, strip), strip)
        return remote(
            pool.at[0:4, at, :], core_in.at[:, at, :], (fsem.at[8], fsem.at[i]), partner
        )

    def front_x(i):
        at = pl.ds(pl.multiple_of(i * strip, strip), strip)
        return remote(
            pool.at[8:10, at, :], x_in.at[:, at, :], (fsem.at[9], fsem.at[4 + i]), x_next
        )

    def gate_strip(i):
        at = pl.ds(pl.multiple_of(i * strip, strip), strip)
        gated = []
        for h in range(heads):
            lanes = slice(h * dv, (h + 1) * dv)
            before = jnp.dot(
                q_ref[at, h * dk : (h + 1) * dk],
                ent[h].astype(jnp.bfloat16),
                preferred_element_type=jnp.float32,
            )
            m_log = cols_ref[at, heads + h : heads + h + 1]
            m_all = jnp.maximum(m_log, ctop[h : h + 1, 0:1])
            memory = (
                num[at, lanes] * jnp.exp(m_log - m_all)
                + jnp.exp(ctop[h : h + 1, 0:1] - m_all) * before
            ) * dk ** (-0.5)
            normal = memory * lax.rsqrt(jnp.mean(memory * memory, axis=-1, keepdims=True) + EPSILON)
            opened = jax.nn.sigmoid(open_ref[h, at, :].astype(jnp.float32))
            gated.append((normal * gain_ref[lanes][None, :].astype(jnp.float32) * opened).astype(jnp.bfloat16))
        gated = jnp.concatenate(gated, axis=1)
        for chip in range(NX):
            for part in range(2):
                for mine in range(2):
                    core = c if mine else 1 - c
                    lanes = pl.ds(
                        pl.multiple_of((chip * 2 + core) * width + part * wide, wide), wide
                    )
                    pool[mine * 4 + chip * 2 + part, at, :] = jnp.dot(
                        gated, wo_ref[:, lanes], preferred_element_type=jnp.float32
                    ).astype(jnp.bfloat16)
        front_core(i).start()

    def core_sum(i):
        at = pl.ds(pl.multiple_of(i * strip, strip), strip)
        front_core(i).wait_recv()
        for part in range(2):
            far, near = (1 - x) * 2 + part, x * 2 + part
            pool[8 + part, at, :] = (
                pool[4 + far, at, :].astype(jnp.float32) + core_in[far, at, :].astype(jnp.float32)
            ).astype(jnp.bfloat16)
        front_x(i).start()

    @pl.loop(0, 5)
    def _(i):
        @pl.when(i < 4)
        def _():
            gate_strip(i)

        @pl.when(i == 2)
        def _():
            y_weight(1).wait_recv()
            z_send(3)

        @pl.when(i >= 1)
        def _():
            core_sum(i - 1)

    z_forward(1, 0)
    z_forward(1, 1)
    y_weight(2).wait_recv()
    own_down.wait()
    z_down(0, 0)
    for part in range(2):
        loads["resid" + str(part)].wait()

    def piece(owner_x, owner_c, owner_y, i):
        at = pl.multiple_of(owner_y * tokens + i * strip, strip)
        lanes = pl.multiple_of((owner_x * 2 + owner_c) * width, width)
        return rows_all.at[pl.ds(at, strip), pl.ds(lanes, width)]

    def to_x(i):
        part = piece(x, c, y, i)
        return remote(part, part, (gsem.at[16], gsem.at[i]), x_next)

    def to_y(kind, i):
        part = piece(x if kind == 0 else 1 - x, c, y, i)
        return remote(part, part, (gsem.at[17 + kind], gsem.at[4 + kind * 4 + i]), y_next)

    def to_core(kind, i):
        part = piece(
            x if kind % 2 == 0 else 1 - x, c, y if kind // 2 == 0 else 1 - y, i
        )
        return remote(part, part, (gsem.at[19 + kind], gsem.at[12 + kind]), partner)

    @pl.loop(0, 4)
    def _(i):
        at = pl.ds(pl.multiple_of(i * strip, strip), strip)
        front_x(i).wait_recv()
        start = pl.multiple_of(y * tokens + i * strip, strip)
        for part in range(2):
            lanes = slice(part * wide, (part + 1) * wide)
            near = x * 2 + part
            total = (
                pool[4 + near, at, :].astype(jnp.float32)
                + core_in[near, at, :].astype(jnp.float32)
                + x_in[part, at, :].astype(jnp.float32)
            )
            fresh = (resid_ref[part, at, :].astype(jnp.float32) + total).astype(jnp.bfloat16)
            out_ref[at, lanes] = fresh
            columns = pl.ds(pl.multiple_of(tp * width + part * wide, wide), wide)
            rows_all[pl.ds(start, strip), columns] = fresh
        to_x(i).start()
        to_y(0, i).start()
        to_core(0, i).start()

        @pl.when(i == 1)
        def _():
            z_forward(1, 2)

    z_forward(1, 3)
    z_down(1, 0)

    @pl.loop(0, 4)
    def _(i):
        to_x(i).wait_recv()
        to_y(1, i).start()
        to_core(1, i).start()
        to_y(0, i).wait_recv()
        to_core(2, i).start()

        @pl.when(i == 1)
        def _():
            z_forward(2, 0)
            z_forward(2, 1)

    z_forward(2, 2)
    z_down(1, 1)

    short = 256

    def norm_rows(owner, kinds):
        for kind in kinds:
            remote(whole_strip, whole_strip, (gsem.at[16], gsem.at[12 + kind]), partner).wait_recv()

        @pl.loop(0, tokens // short)
        def _(i):
            at = pl.ds(pl.multiple_of(owner * tokens + i * short, short), short)
            wide_rows = rows_all[at, :].astype(jnp.float32)
            scale = lax.rsqrt(jnp.mean(wide_rows * wide_rows, axis=-1, keepdims=True) + EPSILON)
            rows_all[at, :] = (wide_rows * scale * fgain_ref[...][None, :].astype(jnp.float32)).astype(
                jnp.bfloat16
            )

    @pl.loop(0, 4)
    def _(i):
        to_y(1, i).wait_recv()
        to_core(3, i).start()

    z_forward(2, 3)

    whole_strip = rows_all.at[pl.ds(0, tokens), pl.ds(0, width)]
    remote(pool.at[0:4], pool.at[0:4], (fsem.at[8], fsem.at[0]), partner).wait_send()
    remote(pool.at[8:10], pool.at[8:10], (fsem.at[9], fsem.at[4]), x_next).wait_send()
    for index in range(16, 23):
        remote(whole_strip, whole_strip, (gsem.at[index], gsem.at[0]), partner).wait_send()

    norm_rows(y, (0, 1))
    norm_rows(1 - y, (2, 3))

    tall = 512
    plane_rows = NY * depth
    early = last * plane_rows
    early_at = jnp.where(z == last, plane_rows, 0)
    late_at = jnp.where(z == last, 0, early)

    def gate_up(i, start, size):
        at = pl.ds(pl.multiple_of(i * tall, tall), tall)
        taken = pl.ds(pl.multiple_of(start, plane_rows), size)
        return at, jnp.dot(rows_all[at, taken], gu[taken, :], preferred_element_type=jnp.float32)

    def gu_arrived(dist):
        for way in range(2):

            @pl.when(jnp.logical_and(has_origin(way, dist), jnp.logical_not(has_next(way))))
            def _():
                for chunk in range(4):
                    z_arrival(way, dist, chunk).wait_recv()

    for dist in range(1, last):
        gu_arrived(dist)

    @pl.loop(0, NY * tokens // tall)
    def _(i):
        at, product = gate_up(i, early_at, early)
        sums[at, :] = product

    z_down(2, 1)
    z_down(2, 0)
    gu_arrived(last)

    def finish_hidden(i):
        at, product = gate_up(i, late_at, plane_rows)
        both = sums[at, :] + product
        hid[at, :] = (jax.nn.silu(both[:, :half]) * both[:, half:]).astype(jnp.bfloat16)

    @pl.loop(0, NY)
    def _(i):
        finish_hidden(i * (tokens // tall))


    units = planes * NY * PIECES
    rows = tokens // PIECES

    def side_of(unit):
        return unit // PIECES % NY

    def place(unit):
        step = unit // (PIECES * NY)
        return (z // 2 + step % 2) % 2 * 2 + (z % 2 + step // 2) % 2

    def slot(unit):
        return unit // (PIECES * NY) % 2 * 2 + side_of(unit)

    def kept_index(unit):
        return slot(unit) * PIECES + unit % PIECES

    def strip_of(unit):
        return pl.ds(pl.multiple_of(unit % PIECES * rows, rows), rows)

    def held(unit, top_row):
        return unit // PIECES * 2 + top_row, strip_of(unit)

    def both_of(unit):
        return pool.at[pl.ds(unit // PIECES * 2, 2), strip_of(unit)]

    def back_core(unit):
        kept = core_back.at[slot(unit), :, strip_of(unit)]
        return remote(both_of(unit), kept, (bsem.at[0], bsem.at[3 + kept_index(unit)]), partner)

    def back_y(unit):
        kept = y_back.at[slot(unit), strip_of(unit)]
        return remote(pool.at[held(unit, 1 - y)], kept, (bsem.at[1], bsem.at[3 + 4 * PIECES + kept_index(unit)]), y_next)

    def back_x(unit):
        kept = x_back.at[side_of(unit), strip_of(unit)]
        return remote(pool.at[held(unit, y)], kept, (bsem.at[2], bsem.at[3 + 8 * PIECES + unit % (2 * PIECES)]), x_next)

    def keeps(unit):
        return place(unit) % 2 == c

    def owns(unit):
        return place(unit) == tp

    def passes(unit):
        return jnp.logical_and(keeps(unit), place(unit) // 2 != x)

    def add(unit, top_row, other):
        at = held(unit, top_row)
        pool[at] = (pool[at].astype(jnp.float32) + other.astype(jnp.float32)).astype(jnp.bfloat16)

    def down_part(unit):
        step, side = unit // (PIECES * NY), side_of(unit)
        ends = jnp.logical_or(z == 0, z == last)

        @pl.when(jnp.logical_and(jnp.logical_and(step > 0, unit % PIECES == 0), ends))
        def _():
            at = place(unit)
            way = jnp.where(z == 0, 1, 0)
            dist = jnp.where(z == 0, at, z - at)
            part = dn.at[at * NY + side]
            remote(part, part, (zs.at[way, 0, 0], zr.at[way, dist - 1, 4 + side]), on_plane(z)).wait_recv()

        weight = dn[place(unit) * NY + side]
        for top_row in (1 - y, y):
            start = pl.multiple_of(top_row * tokens + unit % PIECES * rows, rows)
            pool[held(unit, top_row)] = jnp.dot(
                hid[pl.ds(start, rows), :], weight, preferred_element_type=jnp.float32
            ).astype(jnp.bfloat16)

        @pl.when(jnp.logical_not(keeps(unit)))
        def _():
            back_core(unit).start()

    def after_core(unit):
        @pl.when(keeps(unit))
        def _():
            back_core(unit).wait_recv()
            for top_row in (1 - y, y):
                add(unit, top_row, core_back[slot(unit), top_row, strip_of(unit)])
            back_y(unit).start()

    def after_y(unit):
        @pl.when(keeps(unit))
        def _():
            back_y(unit).wait_recv()
            add(unit, y, y_back[slot(unit), strip_of(unit)])

        @pl.when(passes(unit))
        def _():
            back_x(unit).start()

    def finish(unit, other):
        at = strip_of(unit)
        lanes = pl.ds(pl.multiple_of(side_of(unit) * wide, wide), wide)
        total = pool[held(unit, y)].astype(jnp.float32) + other.astype(jnp.float32)
        out_ref[at, lanes] = (out_ref[at, lanes].astype(jnp.float32) + 0.5 * total).astype(out_ref.dtype)

    def after_x(unit):
        @pl.when(owns(unit))
        def _():
            back_x(unit).wait_recv()
            finish(unit, x_back[side_of(unit), strip_of(unit)])

    def run(low, high, begun=0, trail=0):
        @pl.loop(low, high + 1)
        def _(i):
            @pl.when(jnp.logical_and(i >= begun, i < high))
            def _():
                down_part(i)

            @pl.when(i > low)
            def _():
                after_core(i - 1)

            if trail:

                @pl.when(i < high - 1)
                def _():
                    after_y(i - trail)

    def each(stage, low, high):
        @pl.loop(low, high)
        def _(i):
            stage(i)


    def at_ends(low, high):
        @pl.when(ends)
        def _():
            run(low, high)

    begun = tall // rows

    @pl.loop(0, begun)
    def _(i):
        down_part(i)

    @pl.loop(0, NY)
    def _(i):
        finish_hidden(i * (tokens // tall) + 1)

    run(0, 8, begun)
    z_down(2, 2)
    run(8, 16)

    @pl.when(jnp.logical_not(ends))
    def _():
        run(16, units)

    each(after_y, 0, 8)
    at_ends(16, 20)
    each(after_y, 8, 12)
    at_ends(20, 24)
    each(after_y, 12, 20)
    at_ends(24, 28)
    each(after_y, 20, 24)
    each(after_y, units - 2 * PIECES, units - 2 * PIECES + 1)

    @pl.when(ends)
    def _():
        run(units - PIECES, units, 0, PIECES - 1)

    @pl.when(jnp.logical_not(ends))
    def _():
        each(after_y, units - 2 * PIECES + 1, units - PIECES)

    each(after_y, units - PIECES, units)
    def sent(part, sem, to):
        remote(part, part, (sem, zr.at[0, 0, 0]), to).wait_send()

    sent(core_back, bsem.at[0], partner)
    sent(y_back, bsem.at[1], y_next)
    sent(x_back, bsem.at[2], x_next)
    for chunk in range(3):
        y_weight(chunk).wait_send()
    for copy in state_y:
        copy.wait_send()

    @pl.when(z == 0)
    def _():
        for copy in state_z(1, 0):
            copy.wait_send()

    @pl.when(jnp.logical_and(z > 0, z < last))
    def _():
        for copy in state_z(1, 1):
            copy.wait_send()

    for way in range(2):
        for dist in range(planes - 1):

            @pl.when(jnp.logical_and(has_origin(way, dist), has_next(way)))
            def _():
                sent(gu.at[pl.ds(0, plane_rows), :], zs.at[way, dist, 0], partner)
                sent(dn.at[pl.ds(0, NY)], zs.at[way, dist, 1], partner)

    each(after_x, 0, units)


def plane_layer(
    planes,
    queries,
    cell_key_rows,
    cell_value_rows,
    output_gate_logits,
    input_gate_logits,
    forget_gate_logits,
    forget_extra_term,
    residual,
    head_norm_gain,
    cell_output_weight,
    feedforward_norm_gain,
    gate_projection_weight,
    up_projection_weight,
    down_projection_weight,
):
    tokens, heads = queries.shape[0], input_gate_logits.shape[0]
    width = residual.shape[1]
    model = cell_output_weight.shape[1]
    depth, hidden = gate_projection_weight.shape
    half = hidden // NY
    dk, dv = queries.shape[1] // heads, cell_value_rows.shape[1] // heads
    bf16, f32 = jnp.bfloat16, jnp.float32
    vmem, dma = pltpu.VMEM, pltpu.SemaphoreType.DMA
    scratch = [
        vmem((heads, tokens), input_gate_logits.dtype),
        vmem((heads, tokens), forget_gate_logits.dtype),
        vmem((heads, tokens), forget_extra_term.dtype),
        vmem((heads * dv,), head_norm_gain.dtype),
        vmem((model,), feedforward_norm_gain.dtype),
        vmem((depth, hidden), bf16),
        vmem((depth, hidden), bf16),
        vmem((heads * dv, model), bf16),
        vmem((8, tokens), f32),
        vmem((tokens, 8), f32),
        vmem((8, dv), f32),
        vmem((model, hidden), bf16),
        vmem((planes * NY, half, depth), bf16),
        vmem((NY * tokens, 2 * NX * width), bf16),
        vmem((NY * tokens, half), bf16),
        vmem((NY * tokens, hidden), f32),
        vmem((depth, hidden), bf16),
        vmem((tokens, heads * dv), f32),
        vmem((heads, dk, dv), f32),
        vmem((heads, dk, dv), bf16),
        vmem((heads, dk, dv), bf16),
        vmem((heads, dk, dv), bf16),
        vmem((heads, dk, dv), bf16),
        vmem((heads, dk, dv), bf16),
        vmem((8, dv), f32),
        vmem((8, dv), f32),
        vmem((8, dv), f32),
        vmem((8, dv), f32),
        vmem((2, 8, dv), f32),
        vmem((2 * planes * NY, tokens, width // 2), bf16),
        vmem((4, tokens, width // 2), bf16),
        vmem((2, tokens, width // 2), bf16),
        vmem((planes * NY // 2, 2, tokens, width // 2), bf16),
        vmem((planes * NY // 2, tokens, width // 2), bf16),
        vmem((2, tokens, width // 2), bf16),
        dma((2, planes - 1, 2)),
        dma((2, planes - 1, 6)),
        dma((2, 3)),
        dma((8,)),
        dma((10,)),
        dma((23,)),
        dma((3 + 10 * PIECES,)),
        dma((17,)),
    ]
    whole = pl.BlockSpec(memory_space=pltpu.VMEM)
    far = pl.BlockSpec(memory_space=pl.ANY)
    return pl.pallas_call(
        functools.partial(block_body, planes),
        out_shape=pltpu.VMEM((tokens, width), bf16),
        in_specs=[far] * 14,
        out_specs=whole,
        scratch_shapes=scratch,
        compiler_params=pltpu.CompilerParams(
            collective_id=0, has_side_effects=True, vmem_limit_bytes=65000000
        ),
        cost_estimate=pl.CostEstimate(flops=22 * 10**9, bytes_accessed=10**7, transcendentals=0),
        name="block",
    )(
        queries,
        cell_key_rows,
        cell_value_rows,
        output_gate_logits,
        input_gate_logits,
        forget_gate_logits,
        forget_extra_term,
        residual,
        head_norm_gain,
        cell_output_weight,
        feedforward_norm_gain,
        gate_projection_weight,
        up_projection_weight,
        down_projection_weight,
    )


def layer(rows, columns, *arrays):
    if columns == 2 * NX and rows == 4 * NY:
        return plane_layer(rows // NY, *arrays)
    return general(*arrays)


def solution(mesh):
    placed = (
        P("sp", "tp"),
        P("sp", "tp"),
        P("sp", "tp"),
        P("sp", "tp"),
        P("tp", "sp"),
        P("tp", "sp"),
        P("tp", "sp"),
        P("sp", "tp"),
        P("tp"),
        P("tp", None),
        P(),
        P("sp", "tp"),
        P("sp", "tp"),
        P("tp", "sp"),
    )
    return jax.shard_map(
        functools.partial(layer, mesh.shape["sp"], mesh.shape["tp"]), mesh=mesh, in_specs=placed, out_specs=P("sp", "tp"), check_vma=False
    )
```
